256 devices in a mesh: sp: 32 (over z, x), tp: 4 (over y), dp: 2 (over core).
Axes of the slice: x: 4, y: 4, z: 8, core: 2. Of those that a mesh axis runs over, the one named last changes fastest.
Arguments:
- latent: bfloat16 [2, 16384, 2048], P('dp', ('sp', 'tp')), may hold values from -6 to 6
- condition: float32 [2, 2048], P('dp'), may hold values from -6 to 6
- context: bfloat16 [2, 1024, 2048], P('dp', 'sp'), may hold values from -6 to 6
- context_cond: float32 [2048], replicated, may hold values from -6 to 6
- shift_matrix: bfloat16 [2048, 2048], P(('sp', 'tp')), may hold values from -0.125 to 0.125
- scale_matrix: bfloat16 [2048, 2048], P(('sp', 'tp')), may hold values from -0.125 to 0.125
- gate_matrix: bfloat16 [2048, 2048], P(('sp', 'tp')), may hold values from -0.125 to 0.125
- value_proj: bfloat16 [2048, 2048], P(None, 'tp'), may hold values from -0.125 to 0.125
- gate_proj: bfloat16 [2048, 2048], P(None, 'tp'), may hold values from -0.125 to 0.125
- write_proj: bfloat16 [2048, 1024], P(None, 'tp'), may hold values from -0.125 to 0.125
- read_proj: bfloat16 [2048, 1024], P(None, 'tp'), may hold values from -0.125 to 0.125
- step_proj: bfloat16 [2048, 2, 32], replicated, may hold values from -0.125 to 0.125
- decay_rate: float32 [2, 32], replicated, may hold values from 3.0456543e-05 to 0.0601
- pacing: float32 [2, 16384], P('dp'), may hold values from 0.2 to 4.3
- value_taps: float32 [5, 2048], replicated, may hold values from -2.5 to 2.5
- write_taps: float32 [5, 1024], replicated, may hold values from -2.5 to 2.5
- read_taps: float32 [5, 1024], replicated, may hold values from -2.5 to 2.5
- norm_gain: float32 [2048], replicated, may hold values from 0.1 to 1.9
- out_proj: bfloat16 [2048, 2048], P('tp'), may hold values from -0.125 to 0.125
Outputs:
- updated: bfloat16 [2, 16384, 2048], P('dp', ('sp', 'tp'))
The draws below stay inside these ranges and needn't reach their ends.
All inputs are finite; a program needn't handle non-finite values.
Results may differ from the reference program's by a relative error of at most 0.006.
Values may be sent and summed in bfloat16 or wider, within the bound.
A program may use at most 128 MiB of HBM per device.

```python
import math
import jax
import jax.numpy as jnp
from jax import lax

D = 2048
WIDTH = 2048
HEAD = 64
GROUPS = 8
STATE = 128
CONV = 5
ROW = 64
BLOCK = 128
TOK_DEV = 512
CTX = 1024
SAMPLES = 2
TOKENS = 16384
HEADS = 32
CHANNEL_BLOCK = 512


def draw_latent(key, part):
    noise_key, scale_key, direction_key, strength_key = jax.random.split(key, 4)
    span_rows = TOK_DEV // 2
    span_count = TOKENS // span_rows
    noise = jax.random.normal(noise_key, (SAMPLES, TOKENS, D), jnp.float32)
    directions = jax.random.normal(direction_key, (SAMPLES, span_count, D), jnp.float32)
    strength = jax.random.uniform(strength_key, (SAMPLES, span_count, 1), jnp.float32, 1.0, 2.0)
    offsets = jnp.repeat(directions * strength, span_rows, axis=1)
    return jnp.clip(noise + offsets, -6.0, 6.0).astype(jnp.bfloat16)


def draw_decay_rate(key, part):
    pick_key, slow_key, quick_key = jax.random.split(key, 3)
    quick_mask = jax.random.randint(pick_key, (2, HEADS), 0, 2) == 0
    slow_rate = jnp.exp(jax.random.uniform(slow_key, (2, HEADS), jnp.float32, math.log(0.5), math.log(2.0))) / TOKENS
    quick_rate = jnp.exp(jax.random.uniform(quick_key, (2, HEADS), jnp.float32, math.log(0.02), math.log(0.06)))
    return jnp.where(quick_mask, quick_rate, slow_rate).astype(jnp.float32)


def draw_pacing(key, part):
    span_key, token_key = jax.random.split(key)
    span_rows = TOK_DEV // 2
    span_count = TOKENS // span_rows
    span_factor = jnp.exp(jax.random.uniform(span_key, (SAMPLES, span_count), jnp.float32, math.log(0.35), math.log(2.8)))
    token_factor = jax.random.uniform(token_key, (SAMPLES, TOKENS), jnp.float32, 0.6, 1.5)
    return (jnp.repeat(span_factor, span_rows, axis=1) * token_factor).astype(jnp.float32)


def block_levels(stream_key, dims, cuts, least, high):
    factor_of, own = 1.0, jax.random.fold_in(stream_key, 6)
    for axis_at, blocks in cuts:
        draws = jnp.exp(jax.random.uniform(jax.random.fold_in(own, axis_at), (blocks,), jnp.float32, least / len(cuts), high / len(cuts)))
        factor_of = factor_of * jnp.repeat(draws, dims[axis_at] // blocks).reshape([-1 if axis == axis_at else 1 for axis in range(len(dims))])
    return factor_of


def gaussian(stream_key, dims, scale, limit, cuts=(), kind=jnp.bfloat16):
    level = block_levels(stream_key, dims, cuts, -0.22, 0.18) if cuts else 1.0
    entries = jax.random.normal(stream_key, dims, jnp.float32) * scale * level
    return jnp.minimum(jnp.maximum(entries, -limit), limit).astype(kind)


def setup_inputs(seed: int = 0) -> dict:
    key_list = jax.random.split(jax.random.key(seed), 20)
    return {
        "latent": draw_latent(jax.random.fold_in(key_list[19], 71), 0),
        "condition": gaussian(key_list[1], (SAMPLES, D), 1.0, 6.0, ((0, 2),), jnp.float32),
        "context": gaussian(key_list[2], (SAMPLES, CTX, D), 1.0, 6.0, ((0, 2), (1, 32))),
        "context_cond": gaussian(key_list[3], (D,), 1.0, 6.0, (), jnp.float32),
        "shift_matrix": gaussian(key_list[4], (D, D), D ** -0.5, 0.125, ((0, 128),)),
        "scale_matrix": gaussian(key_list[5], (D, D), D ** -0.5, 0.125, ((0, 128),)),
        "gate_matrix": gaussian(key_list[6], (D, D), D ** -0.5, 0.125, ((0, 128),)),
        "value_proj": gaussian(key_list[7], (D, WIDTH), D ** -0.5, 0.125, ((1, 4),)),
        "gate_proj": gaussian(key_list[8], (D, WIDTH), D ** -0.5, 0.125, ((1, 4),)),
        "write_proj": gaussian(key_list[9], (D, GROUPS * STATE), D ** -0.5, 0.125, ((1, 4),)),
        "read_proj": gaussian(key_list[10], (D, GROUPS * STATE), D ** -0.5, 0.125, ((1, 4),)),
        "step_proj": gaussian(key_list[11], (D, 2, HEADS), D ** -0.5, 0.125),
        "decay_rate": draw_decay_rate(jax.random.fold_in(key_list[19], 71), 0),
        "pacing": draw_pacing(jax.random.fold_in(key_list[19], 71), 0),
        "value_taps": gaussian(key_list[14], (CONV, WIDTH), CONV ** -0.5, 2.5, (), jnp.float32),
        "write_taps": gaussian(key_list[15], (CONV, GROUPS * STATE), CONV ** -0.5, 2.5, (), jnp.float32),
        "read_taps": gaussian(key_list[16], (CONV, GROUPS * STATE), CONV ** -0.5, 2.5, (), jnp.float32),
        "norm_gain": jnp.clip(1.0 + 0.18 * jax.random.normal(key_list[17], (WIDTH,), jnp.float32), 0.1, 1.9),
        "out_proj": gaussian(key_list[18], (WIDTH, D), WIDTH ** -0.5, 0.125, ((0, 4),)),
    }


NORM_FLOOR = 1e-05
GATED_FLOOR = 1e-06
FINEST = lax.Precision.HIGHEST

def masked_exp(exponent, allowed):
    return jnp.where(allowed, jnp.exp(jnp.where(allowed, exponent, 0.0)), 0.0)

def modulate(row_block, shift_row, scale_row):
    values = row_block.astype(jnp.float32)
    center = lax.optimization_barrier(jnp.mean(values, -1, keepdims=True))
    spread = lax.optimization_barrier(jnp.mean(jnp.square(values - center), -1, keepdims=True))
    normed = (values - center) * lax.rsqrt(spread + NORM_FLOOR)
    return (normed * (1.0 + shift_row * 0.0 + scale_row) + shift_row).astype(jnp.bfloat16)

def convolve(values, kernel, run_count):
    length, channels = values.shape
    tap_count = kernel.shape[0]
    margin = tap_count // 2
    stretch = length // run_count
    blocked = values.astype(jnp.float32).reshape(run_count, stretch, channels)
    padded = jnp.pad(blocked, ((0, 0), (margin, margin), (0, 0)))
    summed = jnp.zeros_like(blocked)
    for offset in range(tap_count):
        summed = summed + padded[:, offset:offset + stretch] * kernel[offset]
    return jax.nn.silu(summed).reshape(length, channels).astype(jnp.bfloat16)

def context_state(values, writes, weight, groups):
    length = values.shape[0]
    per_group = weight.shape[1] // groups
    scaled = (writes.reshape(length, groups, 1, STATE) * weight.reshape(length, groups, per_group, 1)).astype(jnp.bfloat16)
    head_values = values.reshape(length, groups, per_group, HEAD)
    return jnp.einsum('lgrn,lgrp->grnp', scaled.astype(jnp.float32), head_values.astype(jnp.float32))

def block_sweep(values, writes, reads, decays, steps, start):
    length = values.shape[0]
    groups = writes.shape[1] // STATE
    per_group = decays.shape[1] // groups
    blocks = length // BLOCK
    head_values = values.reshape(blocks, BLOCK, groups, per_group, HEAD).astype(jnp.float32)
    write_rows = writes.reshape(blocks, BLOCK, groups, STATE)
    read_rows = reads.reshape(blocks, BLOCK, groups, STATE).astype(jnp.float32)
    cumulative = jnp.cumsum(decays.reshape(blocks, BLOCK, groups, per_group), axis=1)
    step_rows = steps.reshape(blocks, BLOCK, groups, per_group)
    lower_mask = jnp.tril(jnp.ones((BLOCK, BLOCK), bool))[:, :, None, None]

    def advance(carry_state, inputs):
        block_values, block_writes, block_reads, block_cumul, block_steps = inputs
        affinity = jnp.einsum('tgn,sgn->tsg', block_reads, block_writes.astype(jnp.float32))
        exponent = block_cumul[:, None] - block_cumul[None, :]
        mixing = (affinity[..., None] * masked_exp(exponent, lower_mask) * block_steps[None]).astype(jnp.bfloat16)
        within = jnp.einsum('tsgr,sgrp->tgrp', mixing.astype(jnp.float32), block_values)
        carried = jnp.einsum('tgn,grnp->tgrp', block_reads, carry_state, precision=FINEST) * jnp.exp(block_cumul)[..., None]
        weight = jnp.exp(block_cumul[-1:] - block_cumul) * block_steps
        scaled = (block_writes[:, :, None, :] * weight[..., None]).astype(jnp.bfloat16)
        increment = jnp.einsum('sgrn,sgrp->grnp', scaled.astype(jnp.float32), block_values)
        carry_state = jnp.exp(block_cumul[-1])[..., None, None] * carry_state + increment
        return (carry_state, within + carried)
    final_state, outputs = lax.scan(advance, start, (head_values, write_rows, read_rows, cumulative, step_rows))
    return outputs.reshape(length, groups * per_group * HEAD)

def reference(latent, condition, context, context_cond, shift_matrix, scale_matrix, gate_matrix, value_proj, gate_proj, write_proj, read_proj, step_proj, decay_rate, pacing, value_taps, write_taps, read_taps, norm_gain, out_proj):
    model_width = latent.shape[2]
    results = []
    for sample in range(latent.shape[0]):
        activated = jax.nn.silu(jnp.stack([condition[sample], context_cond])).astype(jnp.bfloat16)
        shifts = jnp.dot(activated, shift_matrix, preferred_element_type=jnp.float32)
        scales = jnp.dot(activated, scale_matrix, preferred_element_type=jnp.float32)
        gate_row = jnp.dot(activated[:1], gate_matrix, preferred_element_type=jnp.float32)
        hidden = modulate(latent[sample], shifts[0], scales[0])
        run_count = TOKENS // ROW
        values = convolve(jnp.dot(hidden, value_proj, preferred_element_type=jnp.float32).astype(jnp.bfloat16), value_taps, run_count)
        writes = convolve(jnp.dot(hidden, write_proj, preferred_element_type=jnp.float32).astype(jnp.bfloat16), write_taps, run_count)
        read_rows = convolve(jnp.dot(hidden, read_proj, preferred_element_type=jnp.float32).astype(jnp.bfloat16), read_taps, run_count)
        gate_pre = jnp.dot(hidden, gate_proj, preferred_element_type=jnp.float32).astype(jnp.bfloat16)
        step_raw = jnp.dot(hidden, step_proj.reshape(model_width, 2 * HEADS), preferred_element_type=jnp.float32).astype(jnp.bfloat16)
        step_raw = lax.optimization_barrier(step_raw).astype(jnp.float32).reshape(TOKENS, 2, HEADS)
        context_hidden = modulate(context[sample], shifts[1], scales[1])
        ctx_values = convolve(jnp.dot(context_hidden, value_proj, preferred_element_type=jnp.float32).astype(jnp.bfloat16), value_taps, 1)
        ctx_writes = convolve(jnp.dot(context_hidden, write_proj, preferred_element_type=jnp.float32).astype(jnp.bfloat16), write_taps, 1)
        ctx_raw = jnp.dot(context_hidden, step_proj.reshape(model_width, 2 * HEADS), preferred_element_type=jnp.float32).astype(jnp.bfloat16)
        ctx_raw = lax.optimization_barrier(ctx_raw).astype(jnp.float32).reshape(CTX, 2, HEADS)
        ctx_fwd_step = jax.nn.softplus(ctx_raw[:, 0])
        ctx_fwd_decay = -decay_rate[0][None, :] * ctx_fwd_step
        ctx_cumul = jnp.cumsum(ctx_fwd_decay, axis=0)
        ctx_forward = context_state(ctx_values, ctx_writes, jnp.exp(ctx_cumul[-1:] - ctx_cumul) * ctx_fwd_step, GROUPS)
        ctx_bwd_step = jax.nn.softplus(ctx_raw[:, 1])
        ctx_bwd_decay = -decay_rate[1][None, :] * ctx_bwd_step
        ctx_back_cumul = jnp.cumsum(ctx_bwd_decay, axis=0)
        ctx_backward = context_state(ctx_values, ctx_writes, jnp.exp(ctx_back_cumul - ctx_bwd_decay) * ctx_bwd_step, GROUPS)
        forward_step = jax.nn.softplus(step_raw[:, 0]) * pacing[sample][:, None]
        forward_decay = -decay_rate[0][None, :] * forward_step
        backward_step = jax.nn.softplus(step_raw[:, 1]) * pacing[sample][:, None]
        backward_decay = -decay_rate[1][None, :] * backward_step
        forward_out = block_sweep(values, writes, read_rows, forward_decay, forward_step, ctx_forward)
        backward_out = block_sweep(values[::-1], writes[::-1], read_rows[::-1], backward_decay[::-1], backward_step[::-1], ctx_backward)[::-1]
        gated_heads = (forward_out + backward_out) * jax.nn.silu(gate_pre.astype(jnp.float32))
        grouped = gated_heads.reshape(TOKENS, GROUPS, -1)
        grouped = grouped * lax.rsqrt(lax.optimization_barrier(jnp.mean(grouped * grouped, -1, keepdims=True)) + GATED_FLOOR)
        inner_rows = (grouped.reshape(TOKENS, WIDTH) * norm_gain).astype(jnp.bfloat16)
        summed = jnp.zeros((TOKENS, model_width), jnp.float32)
        for column_block in range(WIDTH // CHANNEL_BLOCK):
            lower_edge = column_block * CHANNEL_BLOCK
            portion = jnp.dot(inner_rows[:, lower_edge:lower_edge + CHANNEL_BLOCK], out_proj[lower_edge:lower_edge + CHANNEL_BLOCK], preferred_element_type=jnp.float32).astype(jnp.bfloat16)
            summed = summed + lax.optimization_barrier(portion).astype(jnp.float32)
        mixed = lax.optimization_barrier(summed.astype(jnp.bfloat16))
        results.append((latent[sample].astype(jnp.float32) + gate_row[0] * mixed.astype(jnp.float32)).astype(jnp.bfloat16))
    return jnp.stack(results)
```

```python
import functools

import jax
import jax.numpy as jnp
from jax import lax
from jax.experimental import pallas as pl
from jax.experimental.pallas import tpu as pltpu
from jax.sharding import Mesh
from jax.sharding import PartitionSpec as P

HEAD = 64
STATE = 128
ROW = 64
BLOCK = 128
HALO = 16
SP = ("sp_0", "sp_1")
SP_TP = ("sp_0", "sp_1", "tp")
NZ, NX, NY = 8, 4, 4
NS = NZ * NX

NORM_FLOOR = 1e-05
GATED_FLOOR = 1e-06
MESH = pl.DeviceIdType.MESH
F32 = jnp.float32
BF16 = jnp.bfloat16
HIGHEST = lax.Precision.HIGHEST
VMEM = pl.BlockSpec(memory_space=pltpu.VMEM)
ANY = pl.BlockSpec(memory_space=pl.ANY)


def silu(v):
    return v / (1.0 + jnp.exp(-v))


def remote(src, dst, send, recv, **where):
    return pltpu.make_async_remote_copy(
        src_ref=src, dst_ref=dst, send_sem=send, recv_sem=recv, device_id=where, device_id_type=MESH
    )


def position():
    return lax.axis_index("sp_0"), lax.axis_index("sp_1"), lax.axis_index("tp")


def lanes(start, size):
    return pl.ds(pl.multiple_of(start, 128), size)


def rows(start, size):
    return pl.ds(pl.multiple_of(start, 16), size)


def gather_kernel(
    lat, ctx, cond, ccond, shift_m, scale_m, gate_m,
    gat, ctx_ext, mod,
    part, ybuf, summed, zbuf, qbuf, xbuf, fbuf, mbuf,
    y_send, y_recv, z_send, z_recv, x_send, x_recv, g_send, g_recv,
    l_send, l_recv, f_send, f_recv, h_send, h_recv,
):
    z, x, y = position()
    s = z * NX + x
    rank = s * NY + y
    nxt, prv = lax.rem(s + 1, NS), lax.rem(s + NS - 1, NS)
    nxt_at = {"sp_0": nxt // NX, "sp_1": lax.rem(nxt, NX)}
    prv_at = {"sp_0": prv // NX, "sp_1": lax.rem(prv, NX)}
    right, left = lax.rem(y + 1, NY), lax.rem(y + NY - 1, NY)

    barrier = pltpu.get_barrier_semaphore()
    for d in range(1, NY):
        pl.semaphore_signal(
            barrier, inc=1, device_id={"tp": lax.rem(y + d, NY)}, device_id_type=MESH
        )
    for d in range(1, NZ):
        pl.semaphore_signal(
            barrier, inc=1, device_id={"sp_0": lax.rem(z + d, NZ)}, device_id_type=MESH
        )
    for d in range(1, NX):
        pl.semaphore_signal(
            barrier, inc=1, device_id={"sp_1": lax.rem(x + d, NX)}, device_id_type=MESH
        )
    pl.semaphore_signal(barrier, inc=1, device_id=nxt_at, device_id_type=MESH)
    pl.semaphore_signal(barrier, inc=1, device_id=prv_at, device_id_type=MESH)

    vec_row, vec_off = rank // 8, lax.rem(rank, 8) * 16
    lane = lax.broadcasted_iota(jnp.int32, (8, 128), 1)
    window = (lane >= vec_off) & (lane < vec_off + 16)
    own = cond[pl.ds(vec_row, 1), :]
    shared = ccond[pl.ds(vec_row, 1), :]
    line = lax.broadcasted_iota(jnp.int32, (8, 128), 0)
    both = jnp.where(
        line == 0, jnp.broadcast_to(own, (8, 128)), jnp.broadcast_to(shared, (8, 128))
    )
    acts = jnp.where(window, silu(both), 0.0).astype(BF16)

    def product(matrix):
        tall = jnp.concatenate([matrix[...]] * 8, axis=0)
        return jnp.dot(acts, tall, preferred_element_type=F32)

    part[0:2, :] = product(shift_m)[0:2]
    part[2:4, :] = product(scale_m)[0:2]
    part[4:8, :] = product(gate_m)[0:4]
    pl.semaphore_wait(barrier, NY + NZ + NX - 3 + 2)

    y_copies = []
    for d in range(1, NY):
        copy = remote(
            part, ybuf.at[d - 1], y_send.at[d - 1], y_recv.at[d - 1], tp=lax.rem(y + d, NY)
        )
        copy.start()
        y_copies.append(copy)
    l_copies = {}
    for side, half in ((0, 0), (1, 1), (0, 1), (1, 0)):
        copy = remote(
            lat.at[pl.ds(half * 64, 64)],
            gat.at[rows(y * 128 + half * 64, 64)],
            l_send.at[side * 2 + half],
            l_recv.at[side * 2 + half],
            tp=right if side == 0 else left,
        )
        copy.start()
        l_copies[side, half] = copy
    halo_next = remote(
        ctx.at[pl.ds(HALO, HALO)], ctx_ext.at[pl.ds(0, HALO)], h_send.at[0], h_recv.at[0], **nxt_at
    )
    halo_prev = remote(
        ctx.at[pl.ds(0, HALO)],
        ctx_ext.at[pl.ds(3 * HALO, HALO)],
        h_send.at[1],
        h_recv.at[1],
        **prv_at,
    )
    halo_next.start()
    halo_prev.start()

    for copy in y_copies:
        copy.wait()
    summed[...] = (part[...] + ybuf[0]) + (ybuf[1] + ybuf[2])

    z_copies = []
    for d in range(1, NZ):
        to = lax.rem(z + d, NZ)
        copy = remote(
            summed.at[:, lanes(to * 256, 256)],
            zbuf.at[d - 1],
            z_send.at[d - 1],
            z_recv.at[d - 1],
            sp_0=to,
        )
        copy.start()
        z_copies.append(copy)
    total = summed[:, lanes(z * 256, 256)]
    gat[rows(y * 128, 128), :] = lat[...]
    ctx_ext[pl.ds(HALO, 2 * HALO), :] = ctx[...]
    for d, copy in enumerate(z_copies):
        copy.wait()
        total = total + zbuf[d]
    qbuf[...] = total
    x_copies = []
    for d in range(1, NX):
        copy = remote(
            qbuf, xbuf.at[d - 1], x_send.at[d - 1], x_recv.at[d - 1], sp_1=lax.rem(x + d, NX)
        )
        copy.start()
        x_copies.append(copy)

    l_copies[0, 0].wait_recv()
    ahead = remote(
        gat.at[rows(left * 128, 64)],
        gat.at[rows(left * 128, 64)],
        f_send.at[0],
        f_recv.at[0],
        tp=right,
    )
    ahead.start()
    l_copies[1, 1].wait_recv()
    back = remote(
        gat.at[rows(right * 128 + 64, 64)],
        gat.at[rows(right * 128 + 64, 64)],
        f_send.at[1],
        f_recv.at[1],
        tp=left,
    )
    back.start()

    for copy in x_copies:
        copy.wait()
    fbuf[...] = (qbuf[...] + xbuf[0]) + (xbuf[1] + xbuf[2])
    g_copies = []
    for d in range(1, NZ):
        copy = remote(
            fbuf,
            mbuf.at[:, lanes(z * 256, 256)],
            g_send.at[d - 1],
            g_recv.at[d - 1],
            sp_0=lax.rem(z + d, NZ),
        )
        copy.start()
        g_copies.append(copy)
    mbuf[:, lanes(z * 256, 256)] = fbuf[...]
    for copy in g_copies:
        copy.wait()
    mod[...] = mbuf[...]
    halo_next.wait()
    halo_prev.wait()
    for side, half in ((0, 0), (1, 1)):
        l_copies[side, half].wait_send()
    for side, half in ((0, 1), (1, 0)):
        l_copies[side, half].wait()
    ahead.wait()
    back.wait()


def gather_call(lat, ctx, cond, ccond, shift_m, scale_m, gate_m):
    width = lat.shape[1]
    dma = pltpu.SemaphoreType.DMA
    return pl.pallas_call(
        gather_kernel,
        out_shape=(
            jax.ShapeDtypeStruct((NY * 128, width), BF16),
            jax.ShapeDtypeStruct((4 * HALO, width), BF16),
            jax.ShapeDtypeStruct((8, width), F32),
        ),
        in_specs=[VMEM] * 7,
        out_specs=(VMEM, VMEM, VMEM),
        scratch_shapes=[
            pltpu.VMEM((8, width), F32),
            pltpu.VMEM((NY - 1, 8, width), F32),
            pltpu.VMEM((8, width), F32),
            pltpu.VMEM((NZ - 1, 8, 256), F32),
            pltpu.VMEM((8, 256), F32),
            pltpu.VMEM((NX - 1, 8, 256), F32),
            pltpu.VMEM((8, 256), F32),
            pltpu.VMEM((8, width), F32),
            dma((NY - 1,)), dma((NY - 1,)),
            dma((NZ - 1,)), dma((NZ - 1,)),
            dma((NX - 1,)), dma((NX - 1,)),
            dma((NZ - 1,)), dma((NZ - 1,)),
            dma((4,)), dma((4,)),
            dma((2,)), dma((2,)),
            dma((2,)), dma((2,)),
        ],
        compiler_params=pltpu.CompilerParams(
            collective_id=0, has_side_effects=True, vmem_limit_bytes=16 << 20
        ),
        name="gather",
    )(lat, ctx, cond, ccond, shift_m, scale_m, gate_m)


def normed_rows(block, shift, scale):
    values = block.astype(F32)
    center = jnp.mean(values, -1, keepdims=True)
    off = values - center
    spread = jnp.mean(off * off, -1, keepdims=True)
    return (off * lax.rsqrt(spread + NORM_FLOOR) * (1.0 + scale) + shift).astype(BF16)


def conv_rows(pre, taps, run):
    length = pre.shape[0]
    at = lax.rem(lax.broadcasted_iota(jnp.int32, pre.shape, 0), run)
    total = pre * taps[2:3]
    for k in (0, 1, 3, 4):
        moved = pltpu.roll(pre, (2 - k) % length, 0)
        inside = (at + (k - 2) >= 0) & (at + (k - 2) < run)
        total = total + jnp.where(inside, moved, 0.0) * taps[k : k + 1]
    return silu(total)


def split2(v):
    high = v.astype(BF16)
    return high, (v - high.astype(F32)).astype(BF16)


def expand(v, spread):
    high, low = split2(v)
    return jnp.dot(high, spread, preferred_element_type=F32) + jnp.dot(
        low, spread, preferred_element_type=F32
    )


def softplus(v):
    return jnp.maximum(v, 0.0) + jnp.log1p(jnp.exp(-jnp.abs(v)))


def spread_matrix(spread):
    shape = spread.shape
    row = lax.broadcasted_iota(jnp.int32, shape, 0)
    col = lax.broadcasted_iota(jnp.int32, shape, 1)
    spread[...] = jnp.where(row == col // HEAD, 1.0, 0.0).astype(BF16)


def compute_kernel(
    gat, ctx_ext, mod, w_value, w_gate, w_write, w_read, w_step, rates, pace,
    t_value, t_write, t_read,
    ends, totals, local, reads, gates, carry_decay,
    hid, val, wri, cum, stp, spread, inc, before, etot, tot,
):
    z, x, y = position()
    s = z * NX + x
    heads = 8
    spread_matrix(spread)
    row64 = lax.broadcasted_iota(jnp.int32, (64, 128), 0)
    col64 = lax.broadcasted_iota(jnp.int32, (64, 128), 1)
    wanted = jnp.where(col64 < heads, y * heads + col64, 32 + y * heads + col64 - heads)
    pick = jnp.where((row64 == wanted) & (col64 < 2 * heads), 1.0, 0.0)
    pick16 = pick.astype(BF16)
    rate_row = jnp.dot(
        jnp.broadcast_to(rates[...], (8, 64)), pick, precision=HIGHEST, preferred_element_type=F32
    )[0:1]
    value_taps = t_value[:, lanes(y * 512, 512)]
    write_taps = t_write[:, lanes(y * 256, 256)]
    read_taps = t_read[:, lanes(y * 256, 256)]
    row = lax.broadcasted_iota(jnp.int32, (BLOCK, BLOCK), 0)
    col = lax.broadcasted_iota(jnp.int32, (BLOCK, BLOCK), 1)
    lower = jnp.where(col <= row, 1.0, 0.0)
    upper = jnp.where(col >= row, 1.0, 0.0)
    forward_lane = col < heads

    def mix_dot(a, b, ca, cb):
        return lax.dot_general(a, b, (((ca,), (cb,)), ((), ())), preferred_element_type=F32)

    def steps_of(hidden, count):
        raw = jnp.dot(hidden, w_step[...], preferred_element_type=F32).astype(BF16)
        return softplus(jnp.dot(raw, pick16, preferred_element_type=F32))

    for part in range(4):
        rs = pl.ds(part * HALO, HALO)
        hid[rs, :] = normed_rows(ctx_ext[rs, :], mod[1:2, :], mod[3:4, :])
    hidden = hid[0 : 4 * HALO, :]
    at = lax.broadcasted_iota(jnp.int32, (4 * HALO, 1), 0)
    first = jnp.where(s == 0, HALO, 0)
    last = jnp.where(s == NS - 1, 3 * HALO, 4 * HALO)
    present = (at >= first) & (at < last)
    cv = jnp.dot(hidden, w_value[...], preferred_element_type=F32).astype(BF16).astype(F32)
    cw = jnp.dot(hidden, w_write[...], preferred_element_type=F32).astype(BF16).astype(F32)
    cv = conv_rows(jnp.where(present, cv, 0.0), value_taps, 4 * HALO)[HALO : 3 * HALO].astype(BF16)
    cw = conv_rows(jnp.where(present, cw, 0.0), write_taps, 4 * HALO)[HALO : 3 * HALO].astype(BF16)
    cstep = steps_of(hidden, 4 * HALO)[HALO : 3 * HALO]
    cdecay = -rate_row * cstep
    r32 = lax.broadcasted_iota(jnp.int32, (2 * HALO, 2 * HALO), 0)
    c32 = lax.broadcasted_iota(jnp.int32, (2 * HALO, 2 * HALO), 1)
    later = jnp.dot(
        jnp.where(c32 > r32, 1.0, 0.0), cdecay, precision=HIGHEST, preferred_element_type=F32
    )
    earlier = jnp.dot(
        jnp.where(c32 < r32, 1.0, 0.0), cdecay, precision=HIGHEST, preferred_element_type=F32
    )
    f32lane = lax.broadcasted_iota(jnp.int32, (2 * HALO, 128), 1) < heads
    cweight = jnp.exp(jnp.where(f32lane, later, earlier)) * cstep
    cvf = cv.astype(F32)
    cscaled = (jnp.concatenate([cvf, cvf], axis=1) * expand(cweight, spread[...])).astype(BF16)
    for g in range(2):
        wg = cw[:, g * 128 : (g + 1) * 128]
        for d in range(2):
            lg = d * 2 + g
            got = mix_dot(wg, cscaled[:, lg * 256 : (lg + 1) * 256], 0, 0)
            ends[:, lg * 512 + 256 : lg * 512 + 512] = got.astype(BF16)
    ctotal = jnp.exp(jnp.sum(cdecay, axis=0, keepdims=True))

    def project(b, none):
        for part in range(4):
            rs = pl.ds(part * 32, 32)
            hid[rs, :] = normed_rows(gat[rows(b * 128 + part * 32, 32), :], mod[0:1, :], mod[2:3, :])
        hidden = hid[...]
        at_b = rows(b * 128, 128)
        pre = jnp.dot(hidden, w_value[...], preferred_element_type=F32).astype(BF16).astype(F32)
        v = conv_rows(pre, value_taps, ROW)
        vb = v.astype(BF16)
        val[at_b, :] = vb
        pre = jnp.dot(hidden, w_write[...], preferred_element_type=F32).astype(BF16).astype(F32)
        w = conv_rows(pre, write_taps, ROW).astype(BF16)
        wri[at_b, :] = w
        pre = jnp.dot(hidden, w_read[...], preferred_element_type=F32).astype(BF16).astype(F32)
        reads[at_b, :] = conv_rows(pre, read_taps, ROW).astype(BF16)
        gates[at_b, :] = jnp.dot(hidden, w_gate[...], preferred_element_type=F32).astype(BF16)
        pace_row = pace[pl.ds(s * 4 + b, 1), :]
        pace_col = jnp.transpose(jnp.broadcast_to(pace_row, (128, 128)))
        step = steps_of(hidden, 128) * pace_col
        decay = -rate_row * step
        down = jnp.dot(lower, decay, precision=HIGHEST, preferred_element_type=F32)
        up = jnp.dot(upper, decay, precision=HIGHEST, preferred_element_type=F32)
        cums = jnp.where(forward_lane, down, up)
        total = jnp.where(forward_lane[0:1], down[127:128], up[0:1])
        cum[at_b, :] = cums
        stp[at_b, :] = step
        weight = jnp.exp(total - cums) * step
        vf = vb.astype(F32)
        scaled = (jnp.concatenate([vf, vf], axis=1) * expand(weight, spread[...])).astype(BF16)
        for g in range(2):
            wg = w[:, g * 128 : (g + 1) * 128]
            for d in range(2):
                lg = d * 2 + g
                inc[b, :, lg * 256 : (lg + 1) * 256] = mix_dot(
                    wg, scaled[:, lg * 256 : (lg + 1) * 256], 0, 0
                )
        tot[pl.ds(b, 1), :] = total
        return none

    lax.fori_loop(0, 4, project, 0)

    t0, t1, t2, t3 = (tot[b : b + 1, :] for b in range(4))
    zero = jnp.zeros_like(t0)
    fl = forward_lane[0:1]
    since = [
        jnp.where(fl, zero, t1 + t2 + t3),
        jnp.where(fl, t0, t2 + t3),
        jnp.where(fl, t0 + t1, t3),
        jnp.where(fl, t0 + t1 + t2, zero),
    ]
    stack = jnp.concatenate(
        [jnp.exp(t0), jnp.exp(t1), jnp.exp(t2), jnp.exp(t3), jnp.exp(t0 + t1 + t2 + t3), ctotal,
         zero, zero], axis=0,
    )
    high = stack.astype(BF16)
    rest = stack - high.astype(F32)
    etot[...] = jnp.dot(high, spread[...], preferred_element_type=F32) + expand(rest, spread[...])
    totals[...] = etot[4:6, :]
    for b in range(4):
        tot[b : b + 1, :] = since[b]
    for d, order in ((0, (0, 1, 2, 3)), (1, (3, 2, 1, 0))):
        for g in range(2):
            lg = d * 2 + g
            ls = slice(lg * 256, (lg + 1) * 256)
            state = jnp.zeros((STATE, 256), F32)
            for b in order:
                before[b, :, ls] = state.astype(BF16)
                state = etot[b : b + 1, ls] * state + inc[b, :, ls]
            ends[:, lg * 512 : lg * 512 + 256] = state.astype(BF16)

    def within(b, none):
        at_b = rows(b * 128, 128)
        cums = cum[at_b, :]
        step = stp[at_b, :]
        cums_t = jnp.transpose(cums)
        step_t = jnp.transpose(step)
        carry_decay[at_b, :] = jnp.exp(cums + tot[pl.ds(b, 1), :])
        grown = expand(jnp.exp(cums), spread[...])
        for g in range(2):
            r = reads[at_b, g * 128 : (g + 1) * 128]
            w = wri[at_b, g * 128 : (g + 1) * 128]
            affinity = mix_dot(r, w, 1, 1)
            carried = jnp.zeros((128, 256), F32)
            for d in range(2):
                ls = slice((d * 2 + g) * 256, (d * 2 + g + 1) * 256)
                carried = carried + (
                    jnp.dot(r, before[b, :, ls], preferred_element_type=F32) * grown[:, ls]
                )
            for q in range(2):
                mixes = []
                for h in (g * 4 + q * 2, g * 4 + q * 2 + 1):
                    exponent = jnp.where(
                        col <= row,
                        cums[:, h : h + 1] - cums_t[h : h + 1, :],
                        cums[:, 8 + h : 9 + h] - cums_t[8 + h : 9 + h, :],
                    )
                    sf, sb = step_t[h : h + 1, :], step_t[8 + h : 9 + h, :]
                    amount = jnp.where(col < row, sf, jnp.where(col > row, sb, sf + sb))
                    mixes.append((affinity * jnp.exp(exponent) * amount).astype(BF16))
                ls = slice((g * 2 + q) * 128, (g * 2 + q + 1) * 128)
                pair = val[at_b, ls]
                none16 = jnp.zeros_like(pair)
                tall = jnp.concatenate(
                    [jnp.where(col < HEAD, pair, none16), jnp.where(col >= HEAD, pair, none16)],
                    axis=0,
                )
                got = jnp.dot(
                    jnp.concatenate(mixes, axis=1), tall, preferred_element_type=F32
                )
                local[at_b, ls] = got + carried[:, q * 128 : (q + 1) * 128]
        return none

    lax.fori_loop(0, 4, within, 0)


def compute_call(*args):
    tokens = args[0].shape[0]
    return pl.pallas_call(
        compute_kernel,
        out_shape=(
            jax.ShapeDtypeStruct((STATE, 2048), BF16),
            jax.ShapeDtypeStruct((2, 1024), F32),
            jax.ShapeDtypeStruct((tokens, 512), F32),
            jax.ShapeDtypeStruct((tokens, 256), BF16),
            jax.ShapeDtypeStruct((tokens, 512), BF16),
            jax.ShapeDtypeStruct((tokens, 128), F32),
        ),
        in_specs=[VMEM] * 13,
        out_specs=(VMEM,) * 6,
        scratch_shapes=[
            pltpu.VMEM((128, 2048), BF16),
            pltpu.VMEM((tokens, 512), BF16),
            pltpu.VMEM((tokens, 256), BF16),
            pltpu.VMEM((tokens, 128), F32),
            pltpu.VMEM((tokens, 128), F32),
            pltpu.VMEM((128, 1024), BF16),
            pltpu.VMEM((4, STATE, 1024), F32),
            pltpu.VMEM((4, STATE, 1024), BF16),
            pltpu.VMEM((8, 1024), F32),
            pltpu.VMEM((8, 128), F32),
        ],
        compiler_params=pltpu.CompilerParams(vmem_limit_bytes=48 << 20),
        name="compute",
    )(*args)


def state_kernel(
    ends, totals, start,
    got, got_tot, sent, landing,
    a_send, a_recv, t_send, t_recv, b_send, b_recv,
):
    z, x, y = position()
    s = z * NX + x

    def at(t):
        return {"sp_0": t // NX, "sp_1": lax.rem(t, NX)}

    barrier = pltpu.get_barrier_semaphore()

    def greet(p, none):
        pl.semaphore_signal(
            barrier, inc=1, device_id=at(lax.rem(s + p, NS)), device_id_type=MESH
        )
        return none

    lax.fori_loop(1, NS, greet, 0)
    pl.semaphore_wait(barrier, NS - 1)

    def out_copy(p):
        t = lax.rem(s + p, NS)
        return (
            remote(
                ends.at[rows((t // NX) * 16, 16), lanes(lax.rem(t, NX) * 512, 512)],
                got.at[s],
                a_send.at[t],
                a_recv.at[s],
                **at(t),
            ),
            remote(
                totals.at[:, lanes(lax.rem(t, NX) * 256, 256)],
                got_tot.at[s],
                t_send.at[t],
                t_recv.at[s],
                **at(t),
            ),
        )

    def send_out(p, none):
        for copy in out_copy(p):
            copy.start()
        return none

    lax.fori_loop(1, NS, send_out, 0)
    got[s] = ends[rows(z * 16, 16), lanes(x * 512, 512)]
    got_tot[s] = totals[:, lanes(x * 256, 256)]

    def take_in(p, none):
        f = lax.rem(s + NS - p, NS)
        remote(got.at[f], got.at[f], a_send.at[f], a_recv.at[f], **at(f)).wait_recv()
        remote(got_tot.at[f], got_tot.at[f], t_send.at[f], t_recv.at[f], **at(f)).wait_recv()
        return none

    lax.fori_loop(1, NS, take_in, 0)

    turned = x // 2

    def order(k):
        return k + turned * (NS - 1 - 2 * k)

    def context(k, state):
        j = order(k)
        return got_tot[j, 1:2, :] * state + got[j, :, 256:512].astype(F32)

    state = lax.fori_loop(0, NS, context, jnp.zeros((16, 256), F32))

    def back_copy(j):
        return remote(
            sent.at[j],
            landing.at[rows(z * 16, 16), lanes(x * 256, 256)],
            b_send.at[j],
            b_recv.at[s],
            **at(j),
        )

    def latent(k, state):
        j = order(k)
        sent[j] = state.astype(BF16)

        @pl.when(j != s)
        def _():
            back_copy(j).start()

        return got_tot[j, 0:1, :] * state + got[j, :, 0:256].astype(F32)

    lax.fori_loop(0, NS, latent, state)
    landing[rows(z * 16, 16), lanes(x * 256, 256)] = sent[s]

    def finish(p, none):
        f = lax.rem(s + NS - p, NS)
        piece = landing.at[rows((f // NX) * 16, 16), lanes(lax.rem(f, NX) * 256, 256)]
        remote(piece, piece, b_send.at[f], b_recv.at[f], **at(f)).wait_recv()
        t = lax.rem(s + p, NS)
        for copy in out_copy(p):
            copy.wait_send()
        back_copy(t).wait_send()
        return none

    lax.fori_loop(1, NS, finish, 0)
    start[...] = landing[...]


def state_call(ends, totals):
    dma = pltpu.SemaphoreType.DMA
    return pl.pallas_call(
        state_kernel,
        out_shape=jax.ShapeDtypeStruct((STATE, 1024), BF16),
        in_specs=[VMEM] * 2,
        out_specs=VMEM,
        scratch_shapes=[
            pltpu.VMEM((NS, 16, 512), BF16),
            pltpu.VMEM((NS, 2, 256), F32),
            pltpu.VMEM((NS, 16, 256), BF16),
            pltpu.VMEM((STATE, 1024), BF16),
        ]
        + [dma((NS,))] * 6,
        compiler_params=pltpu.CompilerParams(
            collective_id=1, has_side_effects=True, vmem_limit_bytes=16 << 20
        ),
        name="state",
    )(ends, totals)


def output_kernel(
    start, local, reads, gates, carry_decay, gain, w_out, mod, lat,
    out,
    spread, inner, far, near_r, near_l, mine, got_far, got_r, got_l,
    s1, r1, s2, r2,
):
    z, x, y = position()
    right, left = lax.rem(y + 1, NY), lax.rem(y + NY - 1, NY)
    opposite = lax.rem(y + 2, NY)
    barrier = pltpu.get_barrier_semaphore()
    pl.semaphore_signal(barrier, inc=1, device_id={"tp": right}, device_id_type=MESH)
    pl.semaphore_signal(barrier, inc=1, device_id={"tp": left}, device_id_type=MESH)
    spread_matrix(spread)
    gains = gain[:, lanes(y * 512, 512)]
    half = w_out.shape[1] // 2

    def make_inner(b):
        at_b = rows(b * 128, 128)
        grown = expand(carry_decay[at_b, :], spread[...])
        for g in range(2):
            r = reads[at_b, g * 128 : (g + 1) * 128]
            ch = slice(g * 256, (g + 1) * 256)
            total = local[at_b, ch]
            for d in range(2):
                ls = slice((d * 2 + g) * 256, (d * 2 + g + 1) * 256)
                total = total + jnp.dot(r, start[:, ls], preferred_element_type=F32) * grown[:, ls]
            gated = total * silu(gates[at_b, ch].astype(F32))
            power = jnp.mean(gated * gated, -1, keepdims=True)
            inner[:, ch] = (gated * lax.rsqrt(power + GATED_FLOOR) * gains[:, ch]).astype(BF16)

    def product(side):
        return jnp.dot(
            inner[...], w_out[:, side * half : (side + 1) * half], preferred_element_type=F32
        ).astype(BF16)

    make_inner(opposite)
    far[0] = product(0)
    pl.semaphore_wait(barrier, 2)
    far_r = remote(far.at[0], got_far.at[0], s1.at[0], r1.at[0], tp=right)
    far_r.start()
    far[1] = product(1)
    far_l = remote(far.at[1], got_far.at[1], s1.at[1], r1.at[1], tp=left)
    far_l.start()
    make_inner(right)
    near_r[1] = product(1)
    raw_r = remote(near_r.at[1], got_r.at[1], s2.at[0], r2.at[0], tp=right)
    raw_r.start()
    near_r[0] = product(0)
    make_inner(left)
    near_l[0] = product(0)
    raw_l = remote(near_l.at[0], got_l.at[0], s2.at[1], r2.at[1], tp=left)
    raw_l.start()
    near_l[1] = product(1)
    far_r.wait_recv()
    near_r[0] = (near_r[0].astype(F32) + got_far[0].astype(F32)).astype(BF16)
    sum_r = remote(near_r.at[0], got_r.at[0], s2.at[2], r2.at[2], tp=right)
    sum_r.start()
    far_l.wait_recv()
    near_l[1] = (near_l[1].astype(F32) + got_far[1].astype(F32)).astype(BF16)
    sum_l = remote(near_l.at[1], got_l.at[1], s2.at[3], r2.at[3], tp=left)
    sum_l.start()
    make_inner(y)
    mine[0] = product(0)
    mine[1] = product(1)

    def close(side):
        cs = slice(side * half, (side + 1) * half)
        mixed = (
            mine[side].astype(F32) + got_r[side].astype(F32) + got_l[side].astype(F32)
        ).astype(BF16)
        out[:, cs] = (lat[:, cs].astype(F32) + mod[4:5, cs] * mixed.astype(F32)).astype(BF16)

    raw_r.wait_recv()
    raw_l.wait_recv()
    sum_r.wait_recv()
    sum_l.wait_recv()
    close(0)
    close(1)
    far_r.wait_send()
    far_l.wait_send()
    raw_r.wait_send()
    raw_l.wait_send()
    sum_r.wait_send()
    sum_l.wait_send()


def output_call(*args):
    width = args[6].shape[1]
    dma = pltpu.SemaphoreType.DMA
    piece = pltpu.VMEM((2, 128, width // 2), BF16)
    return pl.pallas_call(
        output_kernel,
        out_shape=jax.ShapeDtypeStruct((128, width), BF16),
        in_specs=[VMEM] * 9,
        out_specs=VMEM,
        scratch_shapes=[
            pltpu.VMEM((128, 1024), BF16),
            pltpu.VMEM((128, 512), BF16),
        ]
        + [piece] * 7
        + [dma((2,)), dma((2,)), dma((4,)), dma((4,))],
        compiler_params=pltpu.CompilerParams(
            collective_id=2, has_side_effects=True, vmem_limit_bytes=32 << 20
        ),
        name="output",
    )(*args)


def per_device(
    latent, condition, context, context_cond, shift_matrix, scale_matrix, gate_matrix,
    value_proj, gate_proj, write_proj, read_proj, step_proj, decay_rate, pacing,
    value_taps, write_taps, read_taps, norm_gain, out_proj,
):
    width = latent.shape[2]
    gathered, ctx_ext, mod = gather_call(
        latent[0],
        context[0],
        condition.reshape(width // 128, 128),
        context_cond.reshape(width // 128, 128),
        shift_matrix,
        scale_matrix,
        gate_matrix,
    )
    ends, totals, local, reads, gates, carry_decay = compute_call(
        gathered, ctx_ext, mod, value_proj, gate_proj, write_proj, read_proj,
        step_proj.reshape(width, 64), decay_rate.reshape(1, 64),
        pacing.reshape(128, 128), value_taps, write_taps, read_taps,
    )
    start = state_call(ends, totals)
    updated = output_call(
        start, local, reads, gates, carry_decay, norm_gain.reshape(1, -1), out_proj, mod, latent[0]
    )
    return updated[None]


def solution(mesh):
    torus = Mesh(
        mesh.devices.reshape(NZ, NX, mesh.shape["tp"], mesh.shape["dp"]),
        ("sp_0", "sp_1", "tp", "dp"),
    )
    placed = (
        P("dp", SP_TP, None), P("dp", None), P("dp", SP, None), P(),
        P(SP_TP, None), P(SP_TP, None), P(SP_TP, None),
        P(None, "tp"), P(None, "tp"), P(None, "tp"), P(None, "tp"),
        P(), P(), P("dp", None), P(), P(), P(), P(), P("tp", None),
    )
    return jax.shard_map(
        per_device, mesh=torus, in_specs=placed, out_specs=P("dp", SP_TP, None), check_vma=False
    )
```

```python
import jax
import jax.numpy as jnp
from jax import lax
from jax.experimental import pallas as pl
from jax.experimental.pallas import tpu as pltpu
from jax.sharding import Mesh
from jax.sharding import PartitionSpec as P

HEAD = 64
STATE = 128
ROW = 64
BLOCK = 128
HALO = 16
SP = ("sp_0", "sp_1")
SP_TP = ("sp_0", "sp_1", "tp")
NZ, NX, NY = 8, 4, 4
NS = NZ * NX

NORM_FLOOR = 1e-05
GATED_FLOOR = 1e-06
MESH = pl.DeviceIdType.MESH
F32 = jnp.float32
BF16 = jnp.bfloat16
HIGHEST = lax.Precision.HIGHEST
VMEM = pl.BlockSpec(memory_space=pltpu.VMEM)
ANY = pl.BlockSpec(memory_space=pl.ANY)


def silu(v):
    return v / (1.0 + jnp.exp(-v))


def remote(src, dst, send, recv, **where):
    return pltpu.make_async_remote_copy(
        src_ref=src, dst_ref=dst, send_sem=send, recv_sem=recv, device_id=where, device_id_type=MESH
    )


def position():
    return lax.axis_index("sp_0"), lax.axis_index("sp_1"), lax.axis_index("tp")


def lanes(start, size):
    return pl.ds(pl.multiple_of(start, 128), size)


def rows(start, size):
    return pl.ds(pl.multiple_of(start, 16), size)


def normed_rows(block, shift, scale):
    values = block.astype(F32)
    center = jnp.mean(values, -1, keepdims=True)
    off = values - center
    spread = jnp.mean(off * off, -1, keepdims=True)
    return (off * lax.rsqrt(spread + NORM_FLOOR) * (1.0 + scale) + shift).astype(BF16)


def conv_rows(pre, taps, run):
    length = pre.shape[0]
    at = lax.rem(lax.broadcasted_iota(jnp.int32, pre.shape, 0), run)
    total = pre * taps[2:3]
    for k in (0, 1, 3, 4):
        moved = pltpu.roll(pre, (2 - k) % length, 0)
        inside = (at + (k - 2) >= 0) & (at + (k - 2) < run)
        total = total + jnp.where(inside, moved, 0.0) * taps[k : k + 1]
    return silu(total)


def split2(v):
    high = v.astype(BF16)
    return high, (v - high.astype(F32)).astype(BF16)


def expand(v, spread):
    high, low = split2(v)
    return jnp.dot(high, spread, preferred_element_type=F32) + jnp.dot(
        low, spread, preferred_element_type=F32
    )


def softplus(v):
    return jnp.maximum(v, 0.0) + jnp.log1p(jnp.exp(-jnp.abs(v)))


def spread_matrix(spread):
    shape = spread.shape
    row = lax.broadcasted_iota(jnp.int32, shape, 0)
    col = lax.broadcasted_iota(jnp.int32, shape, 1)
    spread[...] = jnp.where(row == col // HEAD, 1.0, 0.0).astype(BF16)


def dot_on(a, b, ca, cb):
    return lax.dot_general(a, b, (((ca,), (cb,)), ((), ())), preferred_element_type=F32)


def mixer_kernel(
    lat_h, ctx_h, cond_h, ccond_h, shift_h, scale_h, gatem_h,
    wv_h, wg_h, ww_h, wr_h, ws_h, rate_h, pace_h, tv_h, tw_h, tr_h, gain_h, wo_h,
    out,
    cond, ccond, shift_m, scale_m, gate_m,
    w_value, w_gate, w_write, w_read, w_step, rates, pace, t_value, t_write, t_read, gain, w_out,
    part, zbuf, qbuf, ybuf, ybox, xbuf, fbuf, mod,
    gat, ctx_ext, hid, hid_c, val, wri, reads, gates, local,
    cum, stp, cdec, spread, inc, before, etot, tot,
    ends_s, ends_c, tot_s, tot_c, got_s, got_c, gtot_s, gtot_c, sent, start,
    inner, far, near_r, near_l, mine, got_far, got_r, got_l,
    in_sem, z_send, z_recv, y_send, y_recv, x_send, x_recv, g_send, g_recv,
    l_send, l_recv, f_send, f_recv, h_send, h_recv,
    s_send, s_recv, st_send, st_recv, c_send, c_recv, ct_send, ct_recv, b_send, b_recv,
    s1, r1, s2, r2,
):
    z, x, y = position()
    s = z * NX + x
    rank = s * NY + y
    right, left = lax.rem(y + 1, NY), lax.rem(y + NY - 1, NY)
    opposite = lax.rem(y + 2, NY)

    def at(t):
        return {"sp_0": t // NX, "sp_1": lax.rem(t, NX)}

    own_rows = gat.at[rows(y * 128, 128)]
    pairs = [
        (cond_h, cond), (ccond_h, ccond), (shift_h, shift_m), (scale_h, scale_m),
        (gatem_h, gate_m), (lat_h, own_rows), (ctx_h, ctx_ext.at[pl.ds(HALO, 2 * HALO)]),
        (wv_h, w_value), (ww_h, w_write), (ws_h, w_step), (rate_h, rates), (pace_h, pace),
        (tv_h, t_value), (tw_h, t_write), (wr_h, w_read), (wg_h, w_gate), (tr_h, t_read),
        (gain_h, gain), (wo_h, w_out),
    ]
    fetch = [pltpu.make_async_copy(a, b, in_sem.at[k]) for k, (a, b) in enumerate(pairs)]
    for copy in fetch:
        copy.start()

    barrier = pltpu.get_barrier_semaphore()

    def greet(p, none):
        pl.semaphore_signal(
            barrier, inc=1, device_id=at(lax.rem(s + p, NS)), device_id_type=MESH
        )
        return none

    lax.fori_loop(1, NS, greet, 0)
    for d in range(1, NY):
        pl.semaphore_signal(
            barrier, inc=1, device_id={"tp": lax.rem(y + d, NY)}, device_id_type=MESH
        )

    for copy in fetch[:5]:
        copy.wait()
    vec_row, vec_off = rank // 8, lax.rem(rank, 8) * 16
    lane = lax.broadcasted_iota(jnp.int32, (8, 128), 1)
    line = lax.broadcasted_iota(jnp.int32, (8, 128), 0)
    window = (lane >= vec_off) & (lane < vec_off + 16)
    both = jnp.where(
        line == 0,
        jnp.broadcast_to(cond[pl.ds(vec_row, 1), :], (8, 128)),
        jnp.broadcast_to(ccond[pl.ds(vec_row, 1), :], (8, 128)),
    )
    acts = jnp.where(window, silu(both), 0.0).astype(BF16)

    def product_of(matrix):
        tall = jnp.concatenate([matrix[...]] * 8, axis=0)
        return jnp.dot(acts, tall, preferred_element_type=F32)

    part[0:2, :] = product_of(shift_m)[0:2]
    part[2:4, :] = product_of(scale_m)[0:2]
    part[4:8, :] = product_of(gate_m)[0:4]
    fetch[5].wait()
    fetch[6].wait()
    pl.semaphore_wait(barrier, NS - 1 + NY - 1)

    z_copies = []
    for d in range(1, NZ):
        to = lax.rem(z + d, NZ)
        z_copies.append(
            remote(
                part.at[:, lanes(to * 256, 256)], zbuf.at[d - 1], z_send.at[d - 1],
                z_recv.at[d - 1], sp_0=to,
            )
        )
        z_copies[-1].start()

    l_copies = {}

    def latent_half(side, half):
        piece = gat.at[rows(y * 128 + half * 64, 64)]
        k = side * 2 + half
        copy = remote(
            piece, piece, l_send.at[k], l_recv.at[k], tp=right if side == 0 else left
        )
        copy.start()
        l_copies[side, half] = copy

    latent_half(0, 0)
    latent_half(1, 1)
    nxt, prv = lax.rem(s + 1, NS), lax.rem(s + NS - 1, NS)
    halo_next = remote(
        ctx_ext.at[pl.ds(2 * HALO, HALO)], ctx_ext.at[pl.ds(0, HALO)],
        h_send.at[0], h_recv.at[0], **at(nxt),
    )
    halo_prev = remote(
        ctx_ext.at[pl.ds(HALO, HALO)], ctx_ext.at[pl.ds(3 * HALO, HALO)],
        h_send.at[1], h_recv.at[1], **at(prv),
    )
    halo_next.start()
    halo_prev.start()

    total = part[:, lanes(z * 256, 256)]
    for d, copy in enumerate(z_copies):
        copy.wait()
        total = total + zbuf[d]
    qbuf[...] = total
    y_copies = []
    for d in range(1, NY):
        y_copies.append(
            remote(qbuf, ybuf.at[d - 1], y_send.at[d - 1], y_recv.at[d - 1], tp=lax.rem(y + d, NY))
        )
        y_copies[-1].start()
    latent_half(0, 1)
    latent_half(1, 0)

    spread_matrix(spread)
    heads = 8
    row64 = lax.broadcasted_iota(jnp.int32, (64, 128), 0)
    col64 = lax.broadcasted_iota(jnp.int32, (64, 128), 1)
    wanted = jnp.where(col64 < heads, y * heads + col64, 32 + y * heads + col64 - heads)
    pick = jnp.where((row64 == wanted) & (col64 < 2 * heads), 1.0, 0.0)
    pick16 = pick.astype(BF16)
    row = lax.broadcasted_iota(jnp.int32, (BLOCK, BLOCK), 0)
    col = lax.broadcasted_iota(jnp.int32, (BLOCK, BLOCK), 1)
    lower = jnp.where(col <= row, 1.0, 0.0)
    upper = jnp.where(col >= row, 1.0, 0.0)
    forward_lane = col < heads
    fl = forward_lane[0:1]

    for copy in y_copies:
        copy.wait()
    ybox[...] = (qbuf[...] + ybuf[0]) + (ybuf[1] + ybuf[2])
    x_copies = []
    for d in range(1, NX):
        x_copies.append(
            remote(
                ybox, xbuf.at[d - 1], x_send.at[d - 1], x_recv.at[d - 1], sp_1=lax.rem(x + d, NX)
            )
        )
        x_copies[-1].start()

    def forward(side):
        owner = left if side == 0 else right
        piece = gat.at[rows(owner * 128 + side * 64, 64)]
        return remote(
            piece, piece, f_send.at[side], f_recv.at[side], tp=right if side == 0 else left
        )

    for copy in x_copies:
        copy.wait()
    fbuf[...] = (ybox[...] + xbuf[0]) + (xbuf[1] + xbuf[2])
    g_copies = []
    for d in range(1, NZ):
        g_copies.append(
            remote(
                fbuf, mod.at[:, lanes(z * 256, 256)], g_send.at[d - 1], g_recv.at[d - 1],
                sp_0=lax.rem(z + d, NZ),
            )
        )
        g_copies[-1].start()
    mod[:, lanes(z * 256, 256)] = fbuf[...]

    ahead, back = forward(0), forward(1)
    l_copies[0, 0].wait_recv()
    ahead.start()
    l_copies[1, 1].wait_recv()
    back.start()

    for copy in fetch[7:]:
        copy.wait()
    rate_row = (
        jnp.dot(
            jnp.broadcast_to(rates[0:1, :], (8, 32)), pick[0:32], precision=HIGHEST,
            preferred_element_type=F32,
        )
        + jnp.dot(
            jnp.broadcast_to(rates[1:2, :], (8, 32)), pick[32:64], precision=HIGHEST,
            preferred_element_type=F32,
        )
    )[0:1]
    value_taps = t_value[:, lanes(y * 512, 512)]
    write_taps = t_write[:, lanes(y * 256, 256)]
    read_taps = t_read[:, lanes(y * 256, 256)]

    def steps_of(hidden):
        raw = dot_on(hidden, w_step[...], 1, 1).astype(BF16)
        return softplus(jnp.dot(raw, pick16, preferred_element_type=F32))

    for copy in g_copies:
        copy.wait()

    halo_next.wait()
    halo_prev.wait()
    for k in range(4):
        rs = pl.ds(k * HALO, HALO)
        hid_c[rs, :] = normed_rows(ctx_ext[rs, :], mod[1:2, :], mod[3:4, :])
    hidden_c = hid_c[...]
    line_c = lax.broadcasted_iota(jnp.int32, (4 * HALO, 1), 0)
    first = jnp.where(s == 0, HALO, 0)
    last = jnp.where(s == NS - 1, 3 * HALO, 4 * HALO)
    present = (line_c >= first) & (line_c < last)
    own_c = slice(HALO, 3 * HALO)
    cv = jnp.dot(hidden_c, w_value[...], preferred_element_type=F32).astype(BF16).astype(F32)
    cw = jnp.dot(hidden_c, w_write[...], preferred_element_type=F32).astype(BF16).astype(F32)
    cv = conv_rows(jnp.where(present, cv, 0.0), value_taps, 4 * HALO)[own_c].astype(BF16)
    cw = conv_rows(jnp.where(present, cw, 0.0), write_taps, 4 * HALO)[own_c].astype(BF16)
    cstep = steps_of(hidden_c)[own_c]
    cdecay = -rate_row * cstep
    r32 = lax.broadcasted_iota(jnp.int32, (2 * HALO, 2 * HALO), 0)
    c32 = lax.broadcasted_iota(jnp.int32, (2 * HALO, 2 * HALO), 1)
    later = jnp.dot(
        jnp.where(c32 > r32, 1.0, 0.0), cdecay, precision=HIGHEST, preferred_element_type=F32
    )
    earlier = jnp.dot(
        jnp.where(c32 < r32, 1.0, 0.0), cdecay, precision=HIGHEST, preferred_element_type=F32
    )
    cweight = jnp.exp(jnp.where(forward_lane[0 : 2 * HALO], later, earlier)) * cstep
    cvf = cv.astype(F32)
    cscaled = (jnp.concatenate([cvf, cvf], axis=1) * expand(cweight, spread[...])).astype(BF16)
    for g in range(2):
        wg = cw[:, g * 128 : (g + 1) * 128]
        for d in range(2):
            ls = slice((d * 2 + g) * 256, (d * 2 + g + 1) * 256)
            ends_c[:, ls] = dot_on(wg, cscaled[:, ls], 0, 0).astype(BF16)

    def expand3(v):
        high = v.astype(BF16)
        return jnp.dot(high, spread[...], preferred_element_type=F32) + expand(
            v - high.astype(F32), spread[...]
        )

    ctotal = jnp.broadcast_to(jnp.exp(jnp.sum(cdecay, axis=0, keepdims=True)), (8, 128))
    tot_c[...] = expand3(ctotal)[0:1]

    def state_copies(states, tots, got, gtot, a_send, a_recv, t_send, t_recv):
        def outgoing(p):
            t = lax.rem(s + p, NS)
            tz, tx = t // NX, lax.rem(t, NX)
            return (
                remote(
                    states.at[rows(tz * 16, 16), lanes(tx * 256, 256)], got.at[s],
                    a_send.at[t], a_recv.at[s], **at(t),
                ),
                remote(
                    tots.at[:, lanes(tx * 256, 256)], gtot.at[s],
                    t_send.at[t], t_recv.at[s], **at(t),
                ),
            )

        def send(p, none):
            for copy in outgoing(p):
                copy.start()
            return none

        def take(p, none):
            f = lax.rem(s + NS - p, NS)
            remote(got.at[f], got.at[f], a_send.at[f], a_recv.at[f], **at(f)).wait_recv()
            remote(gtot.at[f], gtot.at[f], t_send.at[f], t_recv.at[f], **at(f)).wait_recv()
            return none

        def done(p, none):
            for copy in outgoing(p):
                copy.wait_send()
            return none

        def keep():
            got[s] = states[rows(z * 16, 16), lanes(x * 256, 256)]
            gtot[s] = tots[:, lanes(x * 256, 256)]

        return send, take, done, keep

    send_c, take_c, done_c, keep_c = state_copies(
        ends_c, tot_c, got_c, gtot_c, c_send, c_recv, ct_send, ct_recv
    )
    lax.fori_loop(1, NS, send_c, 0)
    keep_c()

    def project(k, none):
        @pl.when(k == 1)
        def _():
            l_copies[0, 1].wait_recv()

        @pl.when(k == 2)
        def _():
            l_copies[1, 0].wait_recv()

        @pl.when(k == 3)
        def _():
            ahead.wait_recv()
            back.wait_recv()

        b = lax.rem(y + (lax.rem(k + 1, 3) + 1) * ((k + 3) // 4), NY)
        at_b = rows(b * 128, 128)

        def norm_part(i, none):
            rs = rows(b * 128 + i * 32, 32)
            hid[rs, :] = normed_rows(gat[rs, :], mod[0:1, :], mod[2:3, :])
            return none

        lax.fori_loop(0, 4, norm_part, 0)
        hidden = hid[at_b, :]
        pre = jnp.dot(hidden, w_value[...], preferred_element_type=F32).astype(BF16).astype(F32)
        vb = conv_rows(pre, value_taps, ROW).astype(BF16)
        val[at_b, :] = vb
        pre = jnp.dot(hidden, w_write[...], preferred_element_type=F32).astype(BF16).astype(F32)
        w = conv_rows(pre, write_taps, ROW).astype(BF16)
        wri[at_b, :] = w
        pace_row = pace[pl.ds(s * 4 + b, 1), :]
        step = steps_of(hidden) * jnp.transpose(jnp.broadcast_to(pace_row, (128, 128)))
        decay = -rate_row * step
        down = jnp.dot(lower, decay, precision=HIGHEST, preferred_element_type=F32)
        up = jnp.dot(upper, decay, precision=HIGHEST, preferred_element_type=F32)
        cums = jnp.where(forward_lane, down, up)
        total = jnp.where(fl, down[127:128], up[0:1])
        cum[at_b, :] = cums
        stp[at_b, :] = step
        weight = jnp.exp(total - cums) * step
        vf = vb.astype(F32)
        scaled = (jnp.concatenate([vf, vf], axis=1) * expand(weight, spread[...])).astype(BF16)
        for g in range(2):
            wg = w[:, g * 128 : (g + 1) * 128]
            for d in range(2):
                ls = slice((d * 2 + g) * 256, (d * 2 + g + 1) * 256)
                inc[b, :, ls] = dot_on(wg, scaled[:, ls], 0, 0)
        tot[pl.ds(b, 1), :] = total
        return none

    lax.fori_loop(0, 4, project, 0)

    t0, t1, t2, t3 = (tot[b : b + 1, :] for b in range(4))
    zero = jnp.zeros_like(t0)
    etot[...] = expand3(
        jnp.concatenate(
            [jnp.exp(t0), jnp.exp(t1), jnp.exp(t2), jnp.exp(t3), jnp.exp(t0 + t1 + t2 + t3),
             zero, zero, zero], axis=0,
        )
    )
    tot_s[...] = etot[4:5, :]
    tot[0:1, :] = jnp.where(fl, zero, t1 + t2 + t3)
    tot[1:2, :] = jnp.where(fl, t0, t2 + t3)
    tot[2:3, :] = jnp.where(fl, t0 + t1, t3)
    tot[3:4, :] = jnp.where(fl, t0 + t1 + t2, zero)
    for d, order in ((0, (0, 1, 2, 3)), (1, (3, 2, 1, 0))):
        for g in range(2):
            ls = slice((d * 2 + g) * 256, (d * 2 + g + 1) * 256)
            state = jnp.zeros((STATE, 256), F32)
            for b in order:
                before[b, :, ls] = state.astype(BF16)
                state = etot[b : b + 1, ls] * state + inc[b, :, ls]
            ends_s[:, ls] = state.astype(BF16)
    send_s, take_s, done_s, keep_s = state_copies(
        ends_s, tot_s, got_s, gtot_s, s_send, s_recv, st_send, st_recv
    )
    lax.fori_loop(1, NS, send_s, 0)
    keep_s()

    def within(b, none):
        at_b = rows(b * 128, 128)
        hidden = hid[at_b, :]
        pre = jnp.dot(hidden, w_read[...], preferred_element_type=F32).astype(BF16).astype(F32)
        rb = conv_rows(pre, read_taps, ROW).astype(BF16)
        reads[at_b, :] = rb
        gates[at_b, :] = silu(
            jnp.dot(hidden, w_gate[...], preferred_element_type=F32).astype(BF16).astype(F32)
        )
        cums = cum[at_b, :]
        step = stp[at_b, :]
        cums_t = jnp.transpose(cums)
        step_t = jnp.transpose(step)
        cdec[at_b, :] = jnp.exp(cums + tot[pl.ds(b, 1), :])
        grown = expand(jnp.exp(cums), spread[...])
        for g in range(2):
            r = rb[:, g * 128 : (g + 1) * 128]
            affinity = dot_on(r, wri[at_b, g * 128 : (g + 1) * 128], 1, 1)
            carried = jnp.zeros((128, 256), F32)
            for d in range(2):
                ls = slice((d * 2 + g) * 256, (d * 2 + g + 1) * 256)
                carried = carried + (
                    jnp.dot(r, before[b, :, ls], preferred_element_type=F32) * grown[:, ls]
                )
            for q in range(2):
                mixes = []
                for h in (g * 4 + q * 2, g * 4 + q * 2 + 1):
                    exponent = jnp.where(
                        col <= row,
                        cums[:, h : h + 1] - cums_t[h : h + 1, :],
                        cums[:, 8 + h : 9 + h] - cums_t[8 + h : 9 + h, :],
                    )
                    sf, sb = step_t[h : h + 1, :], step_t[8 + h : 9 + h, :]
                    amount = jnp.where(col < row, sf, jnp.where(col > row, sb, sf + sb))
                    mixes.append((affinity * jnp.exp(exponent) * amount).astype(BF16))
                ls = slice((g * 2 + q) * 128, (g * 2 + q + 1) * 128)
                pair = val[at_b, ls]
                none16 = jnp.zeros_like(pair)
                tall = jnp.concatenate(
                    [jnp.where(col < HEAD, pair, none16), jnp.where(col >= HEAD, pair, none16)],
                    axis=0,
                )
                got = jnp.dot(jnp.concatenate(mixes, axis=1), tall, preferred_element_type=F32)
                local[at_b, ls] = got + carried[:, q * 128 : (q + 1) * 128]
        return none

    lax.fori_loop(0, 4, within, 0)

    turned = x // 2

    def order_of(k):
        return k + turned * (NS - 1 - 2 * k)

    lax.fori_loop(1, NS, take_c, 0)

    def context_scan(k, state):
        j = order_of(k)
        return gtot_c[j] * state + got_c[j].astype(F32)

    state = lax.fori_loop(0, NS, context_scan, jnp.zeros((16, 256), F32))
    lax.fori_loop(1, NS, take_s, 0)

    def back_copy(j):
        return remote(
            sent.at[j], start.at[rows(z * 16, 16), lanes(x * 256, 256)],
            b_send.at[j], b_recv.at[s], **at(j),
        )

    def latent_scan(k, state):
        j = order_of(k)
        sent[j] = state.astype(BF16)

        @pl.when(j != s)
        def _():
            back_copy(j).start()

        return gtot_s[j] * state + got_s[j].astype(F32)

    lax.fori_loop(0, NS, latent_scan, state)
    start[rows(z * 16, 16), lanes(x * 256, 256)] = sent[s]

    def take_start(p, none):
        f = lax.rem(s + NS - p, NS)
        piece = start.at[rows((f // NX) * 16, 16), lanes(lax.rem(f, NX) * 256, 256)]
        remote(piece, piece, b_send.at[f], b_recv.at[f], **at(f)).wait_recv()
        return none

    lax.fori_loop(1, NS, take_start, 0)

    half = w_out.shape[1] // 2

    def make_inner(b):
        at_b = rows(b * 128, 128)
        grown = expand(cdec[at_b, :], spread[...])
        for g in range(2):
            r = reads[at_b, g * 128 : (g + 1) * 128]
            ch = slice(g * 256, (g + 1) * 256)
            total = local[at_b, ch]
            for d in range(2):
                ls = slice((d * 2 + g) * 256, (d * 2 + g + 1) * 256)
                total = total + jnp.dot(r, start[:, ls], preferred_element_type=F32) * grown[:, ls]
            gated = total * gates[at_b, ch]
            power = jnp.mean(gated * gated, -1, keepdims=True)
            gains = jnp.concatenate(
                [gain[pl.ds(y * 4 + g * 2, 1), :], gain[pl.ds(y * 4 + g * 2 + 1, 1), :]], axis=1
            )
            inner[:, ch] = (gated * lax.rsqrt(power + GATED_FLOOR) * gains).astype(BF16)

    def product(side):
        return jnp.dot(
            inner[...], w_out[:, side * half : (side + 1) * half], preferred_element_type=F32
        ).astype(BF16)

    make_inner(opposite)
    far[0] = product(0)
    far_r = remote(far.at[0], got_far.at[0], s1.at[0], r1.at[0], tp=right)
    far_r.start()
    far[1] = product(1)
    far_l = remote(far.at[1], got_far.at[1], s1.at[1], r1.at[1], tp=left)
    far_l.start()
    make_inner(right)
    near_r[1] = product(1)
    raw_r = remote(near_r.at[1], got_r.at[1], s2.at[0], r2.at[0], tp=right)
    raw_r.start()
    near_r[0] = product(0)
    make_inner(left)
    near_l[0] = product(0)
    raw_l = remote(near_l.at[0], got_l.at[0], s2.at[1], r2.at[1], tp=left)
    raw_l.start()
    near_l[1] = product(1)
    far_r.wait_recv()
    near_r[0] = (near_r[0].astype(F32) + got_far[0].astype(F32)).astype(BF16)
    sum_r = remote(near_r.at[0], got_r.at[0], s2.at[2], r2.at[2], tp=right)
    sum_r.start()
    far_l.wait_recv()
    near_l[1] = (near_l[1].astype(F32) + got_far[1].astype(F32)).astype(BF16)
    sum_l = remote(near_l.at[1], got_l.at[1], s2.at[3], r2.at[3], tp=left)
    sum_l.start()
    make_inner(y)
    mine[0] = product(0)
    mine[1] = product(1)

    def send_done(p, none):
        back_copy(lax.rem(s + p, NS)).wait_send()
        return done_s(p, done_c(p, none))

    lax.fori_loop(1, NS, send_done, 0)
    for copy in l_copies.values():
        copy.wait_send()
    ahead.wait_send()
    back.wait_send()

    def close(side):
        cs = slice(side * half, (side + 1) * half)
        mixed = (
            mine[side].astype(F32) + got_r[side].astype(F32) + got_l[side].astype(F32)
        ).astype(BF16)
        own = gat[rows(y * 128, 128), cs]
        out[:, cs] = (own.astype(F32) + mod[4:5, cs] * mixed.astype(F32)).astype(BF16)

    raw_r.wait_recv()
    raw_l.wait_recv()
    sum_r.wait_recv()
    sum_l.wait_recv()
    close(0)
    close(1)
    for copy in (far_r, far_l, raw_r, raw_l, sum_r, sum_l):
        copy.wait_send()


def mixer_call(*args):
    width = args[0].shape[1]
    tokens = NY * 128
    dma = pltpu.SemaphoreType.DMA
    vm = pltpu.VMEM
    copied = [vm(args[k].shape, args[k].dtype) for k in (2, 3, 4, 5, 6, 7, 8, 9, 10, 11, 12, 13,
                                                         14, 15, 16, 17, 18)]
    piece = vm((2, 128, width // 2), BF16)
    return pl.pallas_call(
        mixer_kernel,
        out_shape=jax.ShapeDtypeStruct((128, width), BF16),
        in_specs=[ANY] * 19,
        out_specs=VMEM,
        scratch_shapes=copied
        + [
            vm((8, width), F32), vm((NZ - 1, 8, 256), F32), vm((8, 256), F32),
            vm((NY - 1, 8, 256), F32), vm((8, 256), F32), vm((NX - 1, 8, 256), F32),
            vm((8, 256), F32), vm((8, width), F32),
            vm((tokens, width), BF16), vm((4 * HALO, width), BF16), vm((tokens, width), BF16),
            vm((4 * HALO, width), BF16), vm((tokens, 512), BF16), vm((tokens, 256), BF16),
            vm((tokens, 256), BF16), vm((tokens, 512), F32), vm((tokens, 512), F32),
            vm((tokens, 128), F32), vm((tokens, 128), F32), vm((tokens, 128), F32),
            vm((128, 1024), BF16), vm((4, STATE, 1024), F32), vm((4, STATE, 1024), BF16),
            vm((8, 1024), F32), vm((8, 128), F32),
            vm((STATE, 1024), BF16), vm((STATE, 1024), BF16), vm((1, 1024), F32),
            vm((1, 1024), F32), vm((NS, 16, 256), BF16), vm((NS, 16, 256), BF16),
            vm((NS, 1, 256), F32), vm((NS, 1, 256), F32), vm((NS, 16, 256), BF16),
            vm((STATE, 1024), BF16),
            vm((128, 512), BF16), piece, piece, piece, piece, piece, piece, piece,
            dma((19,)),
        ]
        + [dma((NZ - 1,))] * 2 + [dma((NY - 1,))] * 2 + [dma((NX - 1,))] * 2
        + [dma((NZ - 1,))] * 2
        + [dma((4,))] * 2 + [dma((2,))] * 2 + [dma((2,))] * 2
        + [dma((NS,))] * 10
        + [dma((2,)), dma((2,)), dma((4,)), dma((4,))],
        compiler_params=pltpu.CompilerParams(
            collective_id=0, has_side_effects=True, vmem_limit_bytes=60 << 20
        ),
        name="mixer",
    )(*args)


def per_device(
    latent, condition, context, context_cond, shift_matrix, scale_matrix, gate_matrix,
    value_proj, gate_proj, write_proj, read_proj, step_proj, decay_rate, pacing,
    value_taps, write_taps, read_taps, norm_gain, out_proj,
):
    width = latent.shape[2]
    updated = mixer_call(
        latent[0], context[0], condition.reshape(width // 128, 128),
        context_cond.reshape(width // 128, 128), shift_matrix, scale_matrix, gate_matrix,
        value_proj, gate_proj, write_proj, read_proj,
        step_proj.transpose(1, 2, 0).reshape(64, width), decay_rate, pacing.reshape(128, 128),
        value_taps, write_taps, read_taps, norm_gain.reshape(-1, 128), out_proj,
    )
    return updated[None]


def solution(mesh):
    torus = Mesh(
        mesh.devices.reshape(NZ, NX, mesh.shape["tp"], mesh.shape["dp"]),
        ("sp_0", "sp_1", "tp", "dp"),
    )
    placed = (
        P("dp", SP_TP, None), P("dp", None), P("dp", SP, None), P(),
        P(SP_TP, None), P(SP_TP, None), P(SP_TP, None),
        P(None, "tp"), P(None, "tp"), P(None, "tp"), P(None, "tp"),
        P(), P(), P("dp", None), P(), P(), P(), P(), P("tp", None),
    )
    return jax.shard_map(
        per_device, mesh=torus, in_specs=placed, out_specs=P("dp", SP_TP, None), check_vma=False
    )
```

```python
import jax
import jax.numpy as jnp
from jax import lax
from jax.experimental import pallas as pl
from jax.experimental.pallas import tpu as pltpu
from jax.sharding import Mesh
from jax.sharding import PartitionSpec as P

HEAD = 64
STATE = 128
ROW = 64
BLOCK = 128
HALO = 16
SP = ("sp_0", "sp_1")
SP_TP = ("sp_0", "sp_1", "tp")
NZ, NX, NY = 8, 4, 4
NS = NZ * NX

NORM_FLOOR = 1e-05
GATED_FLOOR = 1e-06
MESH = pl.DeviceIdType.MESH
F32 = jnp.float32
BF16 = jnp.bfloat16
HIGHEST = lax.Precision.HIGHEST
VMEM = pl.BlockSpec(memory_space=pltpu.VMEM)
ANY = pl.BlockSpec(memory_space=pl.ANY)


def silu(v):
    return v / (1.0 + jnp.exp(-v))


def remote(src, dst, send, recv, **where):
    return pltpu.make_async_remote_copy(
        src_ref=src, dst_ref=dst, send_sem=send, recv_sem=recv, device_id=where, device_id_type=MESH
    )


def position():
    return lax.axis_index("sp_0"), lax.axis_index("sp_1"), lax.axis_index("tp")


def lanes(start, size):
    return pl.ds(pl.multiple_of(start, 128), size)


def rows(start, size):
    return pl.ds(pl.multiple_of(start, 16), size)


def normed_rows(block):
    values = block.astype(F32)
    center = jnp.mean(values, -1, keepdims=True)
    off = values - center
    spread = jnp.mean(off * off, -1, keepdims=True)
    return off * lax.rsqrt(spread + NORM_FLOOR)


def conv_rows(pre, taps, run):
    length = pre.shape[0]
    at = lax.rem(lax.broadcasted_iota(jnp.int32, pre.shape, 0), run)
    total = pre * taps[2:3]
    for k in (0, 1, 3, 4):
        moved = pltpu.roll(pre, (2 - k) % length, 0)
        inside = (at + (k - 2) >= 0) & (at + (k - 2) < run)
        total = total + jnp.where(inside, moved, 0.0) * taps[k : k + 1]
    return silu(total)


def expand(v, spread):
    high = v.astype(BF16)
    low = (v - high.astype(F32)).astype(BF16)
    return jnp.dot(
        jnp.concatenate([high, low], axis=1), spread, preferred_element_type=F32
    )


def three_parts(v):
    high = v.astype(BF16)
    rest = v - high.astype(F32)
    mid = rest.astype(BF16)
    return high, mid, (rest - mid.astype(F32)).astype(BF16)


def softplus(v):
    return jnp.maximum(v, 0.0) + jnp.log1p(jnp.exp(-jnp.abs(v)))


def spread_matrix(spread):
    shape = spread.shape
    row = lax.rem(lax.broadcasted_iota(jnp.int32, shape, 0), 128)
    col = lax.broadcasted_iota(jnp.int32, shape, 1)
    spread[...] = jnp.where(row == col // HEAD, 1.0, 0.0).astype(BF16)


def dot_on(a, b, ca, cb):
    return lax.dot_general(a, b, (((ca,), (cb,)), ((), ())), preferred_element_type=F32)


def mixer_kernel(
    lat_h, ctx_h, cond_h, ccond_h, shift_h, scale_h, gatem_h,
    wv_h, wg_h, ww_h, wr_h, ws_h, rate_h, pace_h, tv_h, tw_h, tr_h, gain_h, wo_h,
    out,
    cond, ccond, shift_m, scale_m, gate_m,
    w_first, w_second, w_step, rates, pace, t_value, t_write, t_read, gain, w_out,
    part, zbuf, qbuf, xybuf, fbuf, mod,
    gat, ctx_ext, nrm, hid, pre_a, pre_b, val, wri, reads, gates, local,
    cum, stp, cdec, pcol, grown_c, spread, inc, before, etot, tot,
    ends_s, ends_c, tot_b, got_s, got_c, gtot, sent, start,
    inner, far, near_r, near_l, mine, got_far, got_r, got_l,
    in_sem, z_send, z_recv, xy_send, xy_recv, g_send, g_recv,
    l_send, l_recv, f_send, f_recv, h_send, h_recv,
    s_send, s_recv, t_send, t_recv, c_send, c_recv, b_send, b_recv,
    s1, r1, s2, r2,
):
    z, x, y = position()
    s = z * NX + x
    rank = s * NY + y
    right, left = lax.rem(y + 1, NY), lax.rem(y + NY - 1, NY)
    opposite = lax.rem(y + 2, NY)
    heads = 8

    def at(t):
        return {"sp_0": t // NX, "sp_1": lax.rem(t, NX)}

    def at_xy(q, sign):
        return {
            "sp_1": lax.rem(x + NX + sign * (q // NY), NX),
            "tp": lax.rem(y + NY + sign * lax.rem(q, NY), NY),
        }

    own_rows = gat.at[rows(y * 128, 128)]
    pairs = [
        (cond_h, cond), (ccond_h, ccond), (shift_h, shift_m), (scale_h, scale_m),
        (gatem_h, gate_m), (lat_h, own_rows), (ctx_h, ctx_ext.at[pl.ds(HALO, 2 * HALO)]),
        (ws_h, w_step), (rate_h, rates), (pace_h, pace),
        (wv_h, w_first.at[:, pl.ds(0, 512)]), (ww_h, w_first.at[:, pl.ds(512, 256)]),
        (tv_h, t_value), (tw_h, t_write), (wr_h, w_second.at[:, pl.ds(0, 256)]),
        (wg_h, w_second.at[:, pl.ds(256, 512)]), (tr_h, t_read),
        (gain_h, gain), (wo_h, w_out),
    ]
    fetch = [pltpu.make_async_copy(a, b, in_sem.at[k]) for k, (a, b) in enumerate(pairs)]
    for copy in fetch:
        copy.start()

    barrier = pltpu.get_barrier_semaphore()

    def greet(p, none):
        pl.semaphore_signal(
            barrier, inc=1, device_id=at(lax.rem(s + p, NS)), device_id_type=MESH
        )
        return none

    lax.fori_loop(1, NS, greet, 0)

    def greet_xy(q, none):
        @pl.when(lax.rem(q, NY) != 0)
        def _():
            pl.semaphore_signal(barrier, inc=1, device_id=at_xy(q, 1), device_id_type=MESH)

        return none

    lax.fori_loop(1, NX * NY, greet_xy, 0)

    for copy in fetch[:5]:
        copy.wait()
    vec_row, vec_off = rank // 8, lax.rem(rank, 8) * 16
    lane = lax.broadcasted_iota(jnp.int32, (8, 128), 1)
    line = lax.broadcasted_iota(jnp.int32, (8, 128), 0)
    window = (lane >= vec_off) & (lane < vec_off + 16)
    both = jnp.where(
        line == 0,
        jnp.broadcast_to(cond[pl.ds(vec_row, 1), :], (8, 128)),
        jnp.broadcast_to(ccond[pl.ds(vec_row, 1), :], (8, 128)),
    )
    acts = jnp.where(window, silu(both), 0.0).astype(BF16)

    def product_of(matrix):
        tall = jnp.concatenate([matrix[...]] * 8, axis=0)
        return jnp.dot(acts, tall, preferred_element_type=F32)

    part[0:2, :] = product_of(shift_m)[0:2]
    part[2:4, :] = product_of(scale_m)[0:2]
    part[4:8, :] = product_of(gate_m)[0:4]
    fetch[5].wait()
    fetch[6].wait()

    def norm_at(base, count):
        def chunk(i, none):
            rs = rows(base + i * 32, 32)
            nrm[rs, :] = normed_rows(gat[rs, :])
            return none

        lax.fori_loop(0, count // 32, chunk, 0)

    def norm_ctx(base):
        nrm[pl.ds(512 + base, HALO), :] = normed_rows(ctx_ext[pl.ds(base, HALO), :])

    norm_at(y * 128, 64)
    pl.semaphore_wait(barrier, NS - 1 + NX * (NY - 1))

    z_copies = []
    for d in range(1, NZ):
        to = lax.rem(z + d, NZ)
        z_copies.append(
            remote(
                part.at[:, lanes(to * 256, 256)], zbuf.at[d - 1], z_send.at[d - 1],
                z_recv.at[d - 1], sp_0=to,
            )
        )
        z_copies[-1].start()

    l_copies = {}

    def latent_half(side, half):
        piece = gat.at[rows(y * 128 + half * 64, 64)]
        k = side * 2 + half
        copy = remote(
            piece, piece, l_send.at[k], l_recv.at[k], tp=right if side == 0 else left
        )
        copy.start()
        l_copies[side, half] = copy

    latent_half(0, 0)
    latent_half(1, 1)

    def latent_ahead(side):
        owner = left if side == 0 else right
        piece = gat.at[rows(owner * 128 + side * 64, 64)]
        return remote(
            piece, piece, f_send.at[side], f_recv.at[side], tp=right if side == 0 else left
        )

    nxt, prv = lax.rem(s + 1, NS), lax.rem(s + NS - 1, NS)
    halo_next = remote(
        ctx_ext.at[pl.ds(2 * HALO, HALO)], ctx_ext.at[pl.ds(0, HALO)],
        h_send.at[0], h_recv.at[0], **at(nxt),
    )
    halo_prev = remote(
        ctx_ext.at[pl.ds(HALO, HALO)], ctx_ext.at[pl.ds(3 * HALO, HALO)],
        h_send.at[1], h_recv.at[1], **at(prv),
    )
    halo_next.start()
    halo_prev.start()

    norm_at(y * 128 + 64, 64)
    norm_ctx(HALO)
    norm_ctx(2 * HALO)
    spread_matrix(spread)
    row64 = lax.broadcasted_iota(jnp.int32, (64, 128), 0)
    col64 = lax.broadcasted_iota(jnp.int32, (64, 128), 1)
    wanted = jnp.where(col64 < heads, y * heads + col64, 32 + y * heads + col64 - heads)
    pick = jnp.where((row64 == wanted) & (col64 < 2 * heads), 1.0, 0.0)
    row = lax.broadcasted_iota(jnp.int32, (BLOCK, BLOCK), 0)
    col = lax.broadcasted_iota(jnp.int32, (BLOCK, BLOCK), 1)
    lower = jnp.where(col <= row, 1.0, 0.0).astype(BF16)
    upper = jnp.where(col >= row, 1.0, 0.0).astype(BF16)
    forward_lane = col < heads
    fl = forward_lane[0:1]
    for copy in fetch[7:10]:
        copy.wait()
    w_first[:, 768:896] = dot_on(w_step[...], pick.astype(BF16), 0, 0).astype(BF16)
    for b in range(4):
        pace_row = pace[pl.ds(s * 4 + b, 1), :]
        pcol[b * 128 : (b + 1) * 128, :] = jnp.transpose(
            jnp.broadcast_to(pace_row, (128, 128))
        )

    total = part[:, lanes(z * 256, 256)]
    for d, copy in enumerate(z_copies):
        copy.wait()
        total = total + zbuf[d]
    qbuf[...] = total
    def xy_copy(q):
        return remote(qbuf, xybuf.at[q], xy_send.at[q], xy_recv.at[q], **at_xy(q, 1))

    def send_xy(k, none):
        xy_copy(NX * NY - 1 - k).start()
        return none

    lax.fori_loop(0, NX * NY - 1, send_xy, 0)
    latent_half(0, 1)
    latent_half(1, 0)

    l_copies[0, 0].wait_recv()
    ahead = latent_ahead(0)
    ahead.start()
    l_copies[1, 1].wait_recv()
    back = latent_ahead(1)
    back.start()
    norm_at(left * 128, 64)
    norm_at(right * 128 + 64, 64)

    def wait_xy(q, none):
        xy_copy(q).wait()
        return none

    lax.fori_loop(1, NX * NY, wait_xy, 0)
    total = qbuf[...]
    for q in range(1, NX * NY):
        total = total + xybuf[q]
    fbuf[...] = total
    g_copies = []
    for d in (4, 3, 5, 2, 6, 1, 7):
        g_copies.append(
            remote(
                fbuf, mod.at[:, lanes(z * 256, 256)], g_send.at[d - 1], g_recv.at[d - 1],
                sp_0=lax.rem(z + d, NZ),
            )
        )
        g_copies[-1].start()
    mod[:, lanes(z * 256, 256)] = total

    halo_next.wait()
    halo_prev.wait()
    norm_ctx(0)
    norm_ctx(3 * HALO)
    l_copies[0, 1].wait_recv()
    l_copies[1, 0].wait_recv()
    norm_at(left * 128 + 64, 64)
    norm_at(right * 128, 64)

    for copy in fetch[10:]:
        copy.wait()
    rate_row = (
        jnp.dot(
            jnp.broadcast_to(rates[0:1, :], (8, 32)), pick[0:32], precision=HIGHEST,
            preferred_element_type=F32,
        )
        + jnp.dot(
            jnp.broadcast_to(rates[1:2, :], (8, 32)), pick[32:64], precision=HIGHEST,
            preferred_element_type=F32,
        )
    )[0:1]
    value_taps = t_value[:, lanes(y * 512, 512)]
    write_taps = t_write[:, lanes(y * 256, 256)]
    read_taps = t_read[:, lanes(y * 256, 256)]

    for copy in g_copies:
        copy.wait()

    def modulate(b, none):
        def chunk(i, none):
            rs = rows(b * 128 + i * 32, 32)
            hid[rs, :] = (nrm[rs, :] * (1.0 + mod[2:3, :]) + mod[0:1, :]).astype(BF16)
            return none

        lax.fori_loop(0, 4, chunk, 0)
        return none

    modulate(y, 0)
    modulate(left, 0)
    modulate(right, 0)
    for k in range(2):
        rs = pl.ds(512 + k * 32, 32)
        hid[rs, :] = (nrm[rs, :] * (1.0 + mod[3:4, :]) + mod[1:2, :]).astype(BF16)
    ahead.wait_recv()
    back.wait_recv()
    norm_at(opposite * 128, 128)
    modulate(opposite, 0)

    for c in (slice(0, 256), slice(256, 512), slice(512, 768), slice(768, 896)):
        pre_a[:, c] = jnp.dot(hid[...], w_first[:, c], preferred_element_type=F32).astype(BF16)

    line_c = lax.broadcasted_iota(jnp.int32, (4 * HALO, 1), 0)
    first = jnp.where(s == 0, HALO, 0)
    last = jnp.where(s == NS - 1, 3 * HALO, 4 * HALO)
    present = (line_c >= first) & (line_c < last)
    own_c = slice(HALO, 3 * HALO)
    cv = pre_a[512:576, 0:512].astype(F32)
    cw = pre_a[512:576, 512:768].astype(F32)
    cv = conv_rows(jnp.where(present, cv, 0.0), value_taps, 4 * HALO)[own_c].astype(BF16)
    cw = conv_rows(jnp.where(present, cw, 0.0), write_taps, 4 * HALO)[own_c].astype(BF16)
    cstep = softplus(pre_a[512 + HALO : 512 + 3 * HALO, 768:896].astype(F32))
    cdecay = -rate_row * cstep
    r32 = lax.broadcasted_iota(jnp.int32, (2 * HALO, 2 * HALO), 0)
    c32 = lax.broadcasted_iota(jnp.int32, (2 * HALO, 2 * HALO), 1)
    cparts = jnp.concatenate(three_parts(cdecay), axis=1)

    def ctx_sum(allowed):
        got = jnp.dot(
            jnp.where(allowed, 1.0, 0.0).astype(BF16), cparts, preferred_element_type=F32
        )
        return got[:, 0:128] + got[:, 128:256] + got[:, 256:384]

    later, earlier = ctx_sum(c32 > r32), ctx_sum(c32 < r32)
    cweight = jnp.exp(jnp.where(forward_lane[0 : 2 * HALO], later, earlier)) * cstep
    cvf = cv.astype(F32)
    cscaled = (jnp.concatenate([cvf, cvf], axis=1) * expand(cweight, spread[...])).astype(BF16)
    for g in range(2):
        wg = cw[:, g * 128 : (g + 1) * 128]
        for d in range(2):
            ls = slice((d * 2 + g) * 256, (d * 2 + g + 1) * 256)
            ends_c[:, ls] = dot_on(wg, cscaled[:, ls], 0, 0).astype(BF16)

    def expand3(v):
        high = v.astype(BF16)
        rest = v - high.astype(F32)
        return jnp.dot(high, spread[0:128, :], preferred_element_type=F32) + expand(
            rest, spread[...]
        )

    ctotal = jnp.exp(jnp.sum(cdecay, axis=0, keepdims=True))

    def far_first(k):
        return NS // 2 + ((k + 1) // 2) * (1 - 2 * lax.rem(k, 2))

    def state_copies(states, got, a_send, a_recv):
        def outgoing(p):
            t = lax.rem(s + p, NS)
            return remote(
                states.at[rows((t // NX) * 16, 16), lanes(lax.rem(t, NX) * 256, 256)],
                got.at[s], a_send.at[t], a_recv.at[s], **at(t),
            )

        def take(p, none):
            f = lax.rem(s + NS - p, NS)
            remote(got.at[f], got.at[f], a_send.at[f], a_recv.at[f], **at(f)).wait_recv()
            return none

        return outgoing, take

    out_c, take_c = state_copies(ends_c, got_c, c_send, c_recv)

    def send_c(k, none):
        out_c(far_first(k)).start()
        return none

    lax.fori_loop(0, NS - 1, send_c, 0)
    got_c[s] = ends_c[rows(z * 16, 16), lanes(x * 256, 256)]

    def block_states(b, none):
        at_b = rows(b * 128, 128)
        vb = conv_rows(pre_a[at_b, 0:512].astype(F32), value_taps, ROW).astype(BF16)
        val[at_b, :] = vb
        w = conv_rows(pre_a[at_b, 512:768].astype(F32), write_taps, ROW).astype(BF16)
        wri[at_b, :] = w
        step = softplus(pre_a[at_b, 768:896].astype(F32)) * pcol[at_b, :]
        decay = -rate_row * step
        parts = jnp.concatenate(three_parts(decay), axis=1)
        down = jnp.dot(lower, parts, preferred_element_type=F32)
        up = jnp.dot(upper, parts, preferred_element_type=F32)
        both = jnp.where(jnp.concatenate([forward_lane] * 3, axis=1), down, up)
        cums = both[:, 0:128] + both[:, 128:256] + both[:, 256:384]
        total = jnp.where(fl, cums[127:128], cums[0:1])
        cum[at_b, :] = cums
        stp[at_b, :] = step
        weight = jnp.exp(total - cums) * step
        vf = vb.astype(F32)
        scaled = (jnp.concatenate([vf, vf], axis=1) * expand(weight, spread[...])).astype(BF16)
        for g in range(2):
            wg = w[:, g * 128 : (g + 1) * 128]
            for d in range(2):
                ls = slice((d * 2 + g) * 256, (d * 2 + g + 1) * 256)
                inc[b, :, ls] = dot_on(wg, scaled[:, ls], 0, 0)
        tot[pl.ds(b, 1), :] = total
        return none

    lax.fori_loop(0, 4, block_states, 0)

    t0, t1, t2, t3 = (tot[b : b + 1, :] for b in range(4))
    zero = jnp.zeros_like(t0)
    etot[...] = expand3(
        jnp.concatenate(
            [jnp.exp(t0), jnp.exp(t1), jnp.exp(t2), jnp.exp(t3), jnp.exp(t0 + t1 + t2 + t3),
             ctotal, zero, zero], axis=0,
        )
    )
    tot_b[...] = etot[4:6, :]
    tot[0:1, :] = jnp.where(fl, zero, t1 + t2 + t3)
    tot[1:2, :] = jnp.where(fl, t0, t2 + t3)
    tot[2:3, :] = jnp.where(fl, t0 + t1, t3)
    tot[3:4, :] = jnp.where(fl, t0 + t1 + t2, zero)
    for d, order in ((0, (0, 1, 2, 3)), (1, (3, 2, 1, 0))):
        for g in range(2):
            ls = slice((d * 2 + g) * 256, (d * 2 + g + 1) * 256)
            state = jnp.zeros((STATE, 256), F32)
            for b in order:
                before[b, :, ls] = state.astype(BF16)
                state = etot[b : b + 1, ls] * state + inc[b, :, ls]
            ends_s[:, ls] = state.astype(BF16)
    out_s, take_s = state_copies(ends_s, got_s, s_send, s_recv)

    def out_t(p):
        t = lax.rem(s + p, NS)
        return remote(
            tot_b.at[:, lanes(lax.rem(t, NX) * 256, 256)], gtot.at[s],
            t_send.at[t], t_recv.at[s], **at(t),
        )

    def send_s(k, none):
        out_s(far_first(k)).start()
        out_t(far_first(k)).start()
        return none

    lax.fori_loop(0, NS - 1, send_s, 0)
    got_s[s] = ends_s[rows(z * 16, 16), lanes(x * 256, 256)]
    gtot[s] = tot_b[:, lanes(x * 256, 256)]

    for c in (slice(0, 256), slice(256, 512), slice(512, 768)):
        pre_b[:, c] = jnp.dot(
            hid[0:512, :], w_second[:, c], preferred_element_type=F32
        ).astype(BF16)

    def within(b, none):
        at_b = rows(b * 128, 128)
        rb = conv_rows(pre_b[at_b, 0:256].astype(F32), read_taps, ROW).astype(BF16)
        reads[at_b, :] = rb
        cums = cum[at_b, :]
        step = stp[at_b, :]
        cums_t = jnp.transpose(cums)
        step_t = jnp.transpose(step)
        cdec[at_b, :] = jnp.exp(cums + tot[pl.ds(b, 1), :])
        grown = expand(jnp.exp(cums), spread[...])
        for g in range(2):
            r = rb[:, g * 128 : (g + 1) * 128]
            affinity = dot_on(r, wri[at_b, g * 128 : (g + 1) * 128], 1, 1)
            carried = jnp.zeros((128, 256), F32)
            for d in range(2):
                ls = slice((d * 2 + g) * 256, (d * 2 + g + 1) * 256)
                carried = carried + (
                    jnp.dot(r, before[b, :, ls], preferred_element_type=F32) * grown[:, ls]
                )
            for q in range(2):
                mixes = []
                for h in (g * 4 + q * 2, g * 4 + q * 2 + 1):
                    exponent = jnp.where(
                        col <= row,
                        cums[:, h : h + 1] - cums_t[h : h + 1, :],
                        cums[:, 8 + h : 9 + h] - cums_t[8 + h : 9 + h, :],
                    )
                    sf, sb = step_t[h : h + 1, :], step_t[8 + h : 9 + h, :]
                    amount = jnp.where(col < row, sf, jnp.where(col > row, sb, sf + sb))
                    mixes.append((affinity * jnp.exp(exponent) * amount).astype(BF16))
                ls = slice((g * 2 + q) * 128, (g * 2 + q + 1) * 128)
                pair = val[at_b, ls]
                none16 = jnp.zeros_like(pair)
                tall = jnp.concatenate(
                    [jnp.where(col < HEAD, pair, none16), jnp.where(col >= HEAD, pair, none16)],
                    axis=0,
                )
                got = jnp.dot(jnp.concatenate(mixes, axis=1), tall, preferred_element_type=F32)
                local[at_b, ls] = got + carried[:, q * 128 : (q + 1) * 128]
        return none

    lax.fori_loop(0, 4, within, 0)

    turned = x // 2

    def order_of(k):
        return k + turned * (NS - 1 - 2 * k)

    def take_t(p, none):
        f = lax.rem(s + NS - p, NS)
        remote(gtot.at[f], gtot.at[f], t_send.at[f], t_recv.at[f], **at(f)).wait_recv()
        return none

    lax.fori_loop(1, NS, take_c, 0)
    lax.fori_loop(1, NS, take_t, 0)

    def context_scan(k, state):
        j = order_of(k)
        return gtot[j, 1:2, :] * state + got_c[j].astype(F32)

    state = lax.fori_loop(0, NS, context_scan, jnp.zeros((16, 256), F32))
    lax.fori_loop(1, NS, take_s, 0)

    def back_copy(j):
        return remote(
            sent.at[j], start.at[rows(z * 16, 16), lanes(x * 256, 256)],
            b_send.at[j], b_recv.at[s], **at(j),
        )

    def latent_scan(k, state):
        j = order_of(k)
        sent[j] = state.astype(BF16)

        @pl.when(j != s)
        def _():
            back_copy(j).start()

        return gtot[j, 0:1, :] * state + got_s[j].astype(F32)

    lax.fori_loop(0, NS, latent_scan, state)
    start[rows(z * 16, 16), lanes(x * 256, 256)] = sent[s]

    def last_tables(b, none):
        at_b = rows(b * 128, 128)
        grown_c[at_b, :] = expand(cdec[at_b, :], spread[...])
        gates[at_b, :] = silu(pre_b[at_b, 256:768].astype(F32))
        return none

    lax.fori_loop(0, 4, last_tables, 0)

    def take_start(p, none):
        f = lax.rem(s + NS - p, NS)
        piece = start.at[rows((f // NX) * 16, 16), lanes(lax.rem(f, NX) * 256, 256)]
        remote(piece, piece, b_send.at[f], b_recv.at[f], **at(f)).wait_recv()
        return none

    lax.fori_loop(1, NS, take_start, 0)

    half = w_out.shape[1] // 2

    def make_inner(b):
        at_b = rows(b * 128, 128)
        for g in range(2):
            r = reads[at_b, g * 128 : (g + 1) * 128]
            ch = slice(g * 256, (g + 1) * 256)
            total = local[at_b, ch]
            for d in range(2):
                ls = slice((d * 2 + g) * 256, (d * 2 + g + 1) * 256)
                total = total + jnp.dot(r, start[:, ls], preferred_element_type=F32) * (
                    grown_c[at_b, ls]
                )
            gated = total * gates[at_b, ch]
            power = jnp.mean(gated * gated, -1, keepdims=True)
            gains = jnp.concatenate(
                [gain[pl.ds(y * 4 + g * 2, 1), :], gain[pl.ds(y * 4 + g * 2 + 1, 1), :]], axis=1
            )
            inner[:, ch] = (gated * lax.rsqrt(power + GATED_FLOOR) * gains).astype(BF16)

    def product(side):
        return jnp.dot(
            inner[...], w_out[:, side * half : (side + 1) * half], preferred_element_type=F32
        ).astype(BF16)

    make_inner(opposite)
    far[0] = product(0)
    far_r = remote(far.at[0], got_far.at[0], s1.at[0], r1.at[0], tp=right)
    far_r.start()
    far[1] = product(1)
    far_l = remote(far.at[1], got_far.at[1], s1.at[1], r1.at[1], tp=left)
    far_l.start()
    make_inner(right)
    near_r[1] = product(1)
    raw_r = remote(near_r.at[1], got_r.at[1], s2.at[0], r2.at[0], tp=right)
    raw_r.start()
    near_r[0] = product(0)
    make_inner(left)
    near_l[0] = product(0)
    raw_l = remote(near_l.at[0], got_l.at[0], s2.at[1], r2.at[1], tp=left)
    raw_l.start()
    near_l[1] = product(1)
    far_r.wait_recv()
    near_r[0] = (near_r[0].astype(F32) + got_far[0].astype(F32)).astype(BF16)
    sum_r = remote(near_r.at[0], got_r.at[0], s2.at[2], r2.at[2], tp=right)
    sum_r.start()
    far_l.wait_recv()
    near_l[1] = (near_l[1].astype(F32) + got_far[1].astype(F32)).astype(BF16)
    sum_l = remote(near_l.at[1], got_l.at[1], s2.at[3], r2.at[3], tp=left)
    sum_l.start()
    make_inner(y)
    mine[0] = product(0)
    mine[1] = product(1)

    def send_done(p, none):
        back_copy(lax.rem(s + p, NS)).wait_send()
        out_s(p).wait_send()
        out_t(p).wait_send()
        out_c(p).wait_send()
        return none

    lax.fori_loop(1, NS, send_done, 0)
    for copy in l_copies.values():
        copy.wait_send()
    ahead.wait_send()
    back.wait_send()

    def close(side):
        cs = slice(side * half, (side + 1) * half)
        mixed = (
            mine[side].astype(F32) + got_r[side].astype(F32) + got_l[side].astype(F32)
        ).astype(BF16)
        own = gat[rows(y * 128, 128), cs]
        out[:, cs] = (own.astype(F32) + mod[4:5, cs] * mixed.astype(F32)).astype(BF16)

    raw_r.wait_recv()
    raw_l.wait_recv()
    sum_r.wait_recv()
    sum_l.wait_recv()
    close(0)
    close(1)
    for copy in (far_r, far_l, raw_r, raw_l, sum_r, sum_l):
        copy.wait_send()


def mixer_call(*args):
    width = args[0].shape[1]
    tokens = NY * 128
    dma = pltpu.SemaphoreType.DMA
    vm = pltpu.VMEM
    same = [vm(args[k].shape, args[k].dtype) for k in range(19)]
    copied = same[2:7] + [vm((width, 896), BF16), vm((width, 768), BF16)] + same[11:19]
    piece = vm((2, 128, width // 2), BF16)
    return pl.pallas_call(
        mixer_kernel,
        out_shape=jax.ShapeDtypeStruct((128, width), BF16),
        in_specs=[ANY] * 19,
        out_specs=VMEM,
        scratch_shapes=copied
        + [
            vm((8, width), F32), vm((NZ - 1, 8, 256), F32), vm((8, 256), F32),
            vm((NX * NY, 8, 256), F32), vm((8, 256), F32), vm((8, width), F32),
            vm((tokens, width), BF16), vm((4 * HALO, width), BF16),
            vm((tokens + 4 * HALO, width), F32), vm((tokens + 4 * HALO, width), BF16),
            vm((tokens + 4 * HALO, 896), BF16), vm((tokens, 768), BF16),
            vm((tokens, 512), BF16), vm((tokens, 256), BF16), vm((tokens, 256), BF16),
            vm((tokens, 512), F32), vm((tokens, 512), F32),
            vm((tokens, 128), F32), vm((tokens, 128), F32), vm((tokens, 128), F32),
            vm((tokens, 128), F32), vm((tokens, 1024), F32),
            vm((256, 1024), BF16), vm((4, STATE, 1024), F32), vm((4, STATE, 1024), BF16),
            vm((8, 1024), F32), vm((8, 128), F32),
            vm((STATE, 1024), BF16), vm((STATE, 1024), BF16), vm((2, 1024), F32),
            vm((NS, 16, 256), BF16), vm((NS, 16, 256), BF16), vm((NS, 2, 256), F32),
            vm((NS, 16, 256), BF16), vm((STATE, 1024), BF16),
            vm((128, 512), BF16), piece, piece, piece, piece, piece, piece, piece,
            dma((19,)),
        ]
        + [dma((NZ - 1,))] * 2 + [dma((NX * NY,))] * 2 + [dma((NZ - 1,))] * 2
        + [dma((4,))] * 2 + [dma((2,))] * 2 + [dma((2,))] * 2
        + [dma((NS,))] * 8
        + [dma((2,)), dma((2,)), dma((4,)), dma((4,))],
        compiler_params=pltpu.CompilerParams(
            collective_id=0, has_side_effects=True, vmem_limit_bytes=60 << 20
        ),
        name="mixer",
    )(*args)


def per_device(
    latent, condition, context, context_cond, shift_matrix, scale_matrix, gate_matrix,
    value_proj, gate_proj, write_proj, read_proj, step_proj, decay_rate, pacing,
    value_taps, write_taps, read_taps, norm_gain, out_proj,
):
    width = latent.shape[2]
    updated = mixer_call(
        latent[0], context[0], condition.reshape(width // 128, 128),
        context_cond.reshape(width // 128, 128), shift_matrix, scale_matrix, gate_matrix,
        value_proj, gate_proj, write_proj, read_proj,
        step_proj.transpose(1, 2, 0).reshape(64, width), decay_rate, pacing.reshape(128, 128),
        value_taps, write_taps, read_taps, norm_gain.reshape(-1, 128), out_proj,
    )
    return updated[None]


def solution(mesh):
    torus = Mesh(
        mesh.devices.reshape(NZ, NX, mesh.shape["tp"], mesh.shape["dp"]),
        ("sp_0", "sp_1", "tp", "dp"),
    )
    placed = (
        P("dp", SP_TP, None), P("dp", None), P("dp", SP, None), P(),
        P(SP_TP, None), P(SP_TP, None), P(SP_TP, None),
        P(None, "tp"), P(None, "tp"), P(None, "tp"), P(None, "tp"),
        P(), P(), P("dp", None), P(), P(), P(), P(), P("tp", None),
    )
    return jax.shard_map(
        per_device, mesh=torus, in_specs=placed, out_specs=P("dp", SP_TP, None), check_vma=False
    )
```

```python
import jax
import jax.numpy as jnp
from jax import lax
from jax.experimental import pallas as pl
from jax.experimental.pallas import tpu as pltpu
from jax.sharding import Mesh
from jax.sharding import PartitionSpec as P

HEAD = 64
STATE = 128
ROW = 64
BLOCK = 128
HALO = 16
SP = ("sp_0", "sp_1")
SP_TP = ("sp_0", "sp_1", "tp")
NZ, NX, NY = 8, 4, 4
NS = NZ * NX

NORM_FLOOR = 1e-05
GATED_FLOOR = 1e-06
MESH = pl.DeviceIdType.MESH
F32 = jnp.float32
BF16 = jnp.bfloat16
HIGHEST = lax.Precision.HIGHEST
VMEM = pl.BlockSpec(memory_space=pltpu.VMEM)
ANY = pl.BlockSpec(memory_space=pl.ANY)


def silu(v):
    return v / (1.0 + jnp.exp(-v))


def remote(src, dst, send, recv, **where):
    return pltpu.make_async_remote_copy(
        src_ref=src, dst_ref=dst, send_sem=send, recv_sem=recv, device_id=where, device_id_type=MESH
    )


def position():
    return lax.axis_index("sp_0"), lax.axis_index("sp_1"), lax.axis_index("tp")


def lanes(start, size):
    return pl.ds(pl.multiple_of(start, 128), size)


def rows(start, size):
    return pl.ds(pl.multiple_of(start, 16), size)


def normed_rows(block):
    values = block.astype(F32)
    center = jnp.mean(values, -1, keepdims=True)
    off = values - center
    spread = jnp.mean(off * off, -1, keepdims=True)
    return off * lax.rsqrt(spread + NORM_FLOOR)


def conv_rows(pre, taps, run):
    length = pre.shape[0]
    at = lax.rem(lax.broadcasted_iota(jnp.int32, pre.shape, 0), run)
    total = pre * taps[2:3]
    for k in (0, 1, 3, 4):
        moved = pltpu.roll(pre, (2 - k) % length, 0)
        inside = (at + (k - 2) >= 0) & (at + (k - 2) < run)
        total = total + jnp.where(inside, moved, 0.0) * taps[k : k + 1]
    return silu(total)


def expand(v, spread):
    high = v.astype(BF16)
    low = (v - high.astype(F32)).astype(BF16)
    return jnp.dot(
        jnp.concatenate([high, low], axis=1), spread, preferred_element_type=F32
    )


def three_parts(v):
    high = v.astype(BF16)
    rest = v - high.astype(F32)
    mid = rest.astype(BF16)
    return high, mid, (rest - mid.astype(F32)).astype(BF16)


def softplus(v):
    return jnp.maximum(v, 0.0) + jnp.log1p(jnp.exp(-jnp.abs(v)))


def spread_matrix(spread):
    shape = spread.shape
    row = lax.rem(lax.broadcasted_iota(jnp.int32, shape, 0), 128)
    col = lax.broadcasted_iota(jnp.int32, shape, 1)
    spread[...] = jnp.where(row == col // HEAD, 1.0, 0.0).astype(BF16)


def dot_on(a, b, ca, cb):
    return lax.dot_general(a, b, (((ca,), (cb,)), ((), ())), preferred_element_type=F32)


def mixer_kernel(
    lat_h, ctx_h, cond_h, ccond_h, shift_h, scale_h, gatem_h,
    wv_h, wg_h, ww_h, wr_h, ws_h, rate_h, pace_h, tv_h, tw_h, tr_h, gain_h, wo_h,
    out,
    cond, ccond, shift_m, scale_m, gate_m,
    w_first, w_second, w_step, rates, pace, t_value, t_write, t_read, gain, w_out,
    part, zbuf, qbuf, xybuf, fbuf, mod,
    gat, ctx_ext, nrm, hid, pre_a, pre_b, val, wri, reads, gates, local,
    cum, stp, cdec, pcol, grown_c, spread, inc, before, etot, tot,
    ends_s, ends_c, tot_b, got_s, got_c, gtot, sent, start,
    inner, far, near_r, near_l, mine, got_far, got_r, got_l,
    in_sem, z_send, z_recv, xy_send, xy_recv, g_send, g_recv,
    l_send, l_recv, f_send, f_recv, h_send, h_recv,
    s_send, s_recv, t_send, t_recv, c_send, c_recv, b_send, b_recv,
    s1, r1, s2, r2,
):
    z, x, y = position()
    s = z * NX + x
    rank = s * NY + y
    right, left = lax.rem(y + 1, NY), lax.rem(y + NY - 1, NY)
    opposite = lax.rem(y + 2, NY)
    heads = 8

    def at(t):
        return {"sp_0": t // NX, "sp_1": lax.rem(t, NX)}

    def at_xy(q, sign):
        return {
            "sp_1": lax.rem(x + NX + sign * (q // NY), NX),
            "tp": lax.rem(y + NY + sign * lax.rem(q, NY), NY),
        }

    own_rows = gat.at[rows(y * 128, 128)]
    pairs = [
        (cond_h, cond), (ccond_h, ccond), (shift_h, shift_m), (scale_h, scale_m),
        (gatem_h, gate_m), (lat_h, own_rows), (ctx_h, ctx_ext.at[pl.ds(HALO, 2 * HALO)]),
        (ws_h, w_step), (rate_h, rates), (pace_h, pace),
        (wv_h, w_first.at[:, pl.ds(0, 512)]), (ww_h, w_first.at[:, pl.ds(512, 256)]),
        (tv_h, t_value), (tw_h, t_write), (wr_h, w_second.at[:, pl.ds(0, 256)]),
        (wg_h, w_second.at[:, pl.ds(256, 512)]), (tr_h, t_read),
        (gain_h, gain), (wo_h, w_out),
    ]
    fetch = [pltpu.make_async_copy(a, b, in_sem.at[k]) for k, (a, b) in enumerate(pairs)]
    for copy in fetch:
        copy.start()

    barrier = pltpu.get_barrier_semaphore()

    def greet(p, none):
        pl.semaphore_signal(
            barrier, inc=1, device_id=at(lax.rem(s + p, NS)), device_id_type=MESH
        )
        return none

    lax.fori_loop(1, NS, greet, 0)

    def greet_xy(q, none):
        @pl.when(lax.rem(q, NY) != 0)
        def _():
            pl.semaphore_signal(barrier, inc=1, device_id=at_xy(q, 1), device_id_type=MESH)

        return none

    lax.fori_loop(1, NX * NY, greet_xy, 0)

    for copy in fetch[:5]:
        copy.wait()
    vec_row, vec_off = rank // 8, lax.rem(rank, 8) * 16
    lane = lax.broadcasted_iota(jnp.int32, (8, 128), 1)
    line = lax.broadcasted_iota(jnp.int32, (8, 128), 0)
    window = (lane >= vec_off) & (lane < vec_off + 16)
    both = jnp.where(
        line == 0,
        jnp.broadcast_to(cond[pl.ds(vec_row, 1), :], (8, 128)),
        jnp.broadcast_to(ccond[pl.ds(vec_row, 1), :], (8, 128)),
    )
    acts = jnp.where(window, silu(both), 0.0).astype(BF16)

    def product_of(matrix):
        tall = jnp.concatenate([matrix[...]] * 8, axis=0)
        return jnp.dot(acts, tall, preferred_element_type=F32)

    part[0:2, :] = product_of(shift_m)[0:2]
    part[2:4, :] = product_of(scale_m)[0:2]
    part[4:8, :] = product_of(gate_m)[0:4]
    fetch[5].wait()
    fetch[6].wait()

    def norm_at(base, count):
        def chunk(i, none):
            rs = rows(base + i * 32, 32)
            nrm[rs, :] = normed_rows(gat[rs, :])
            return none

        lax.fori_loop(0, count // 32, chunk, 0)

    def norm_ctx(base):
        nrm[pl.ds(512 + base, HALO), :] = normed_rows(ctx_ext[pl.ds(base, HALO), :])

    norm_at(y * 128, 64)
    pl.semaphore_wait(barrier, NS - 1 + NX * (NY - 1))

    nxt, prv = lax.rem(s + 1, NS), lax.rem(s + NS - 1, NS)

    def got_all(ref, recv):
        remote(ref, ref, recv, recv, **at(nxt)).wait_recv()

    def sent_all(ref, send):
        remote(ref, ref, send, send, **at(nxt)).wait_send()

    for d in (4, 3, 5, 2, 6, 1, 7):
        to = lax.rem(z + d, NZ)
        remote(
            part.at[:, lanes(to * 256, 256)], zbuf.at[d - 1], z_send.at[0], z_recv.at[0], sp_0=to
        ).start()

    def latent_piece(side, first_row, count, k):
        piece = gat.at[rows(y * 128 + first_row, count)]
        return remote(
            piece, piece, l_send.at[k], l_recv.at[k], tp=right if side == 0 else left
        )

    def latent_ahead(side):
        owner = left if side == 0 else right
        piece = gat.at[rows(owner * 128 + side * 64, 64)]
        return remote(
            piece, piece, f_send.at[side], f_recv.at[side], tp=right if side == 0 else left
        )

    l_first = [latent_piece(0, 0, 64, 0), latent_piece(1, 64, 64, 1)]
    l_next = [latent_piece(0, 64, 32, 2), latent_piece(1, 0, 32, 3)]
    l_last = [latent_piece(0, 96, 32, 4), latent_piece(1, 32, 32, 5)]
    ahead, back = latent_ahead(0), latent_ahead(1)

    def start_all(copies):
        for copy in copies:
            copy.start()

    def start_ahead():
        l_first[0].wait_recv()
        ahead.start()
        l_first[1].wait_recv()
        back.start()

    early = lax.axis_index("dp") == 1
    late = lax.axis_index("dp") == 0
    pl.when(early)(lambda: start_all(l_first + l_next))
    halo_next = remote(
        ctx_ext.at[pl.ds(2 * HALO, HALO)], ctx_ext.at[pl.ds(0, HALO)],
        h_send.at[0], h_recv.at[0], **at(nxt),
    )
    halo_prev = remote(
        ctx_ext.at[pl.ds(HALO, HALO)], ctx_ext.at[pl.ds(3 * HALO, HALO)],
        h_send.at[1], h_recv.at[1], **at(prv),
    )
    halo_next.start()
    halo_prev.start()

    norm_at(y * 128 + 64, 64)
    norm_ctx(HALO)
    norm_ctx(2 * HALO)
    spread_matrix(spread)
    row64 = lax.broadcasted_iota(jnp.int32, (64, 128), 0)
    col64 = lax.broadcasted_iota(jnp.int32, (64, 128), 1)
    wanted = jnp.where(col64 < heads, y * heads + col64, 32 + y * heads + col64 - heads)
    pick = jnp.where((row64 == wanted) & (col64 < 2 * heads), 1.0, 0.0)
    row = lax.broadcasted_iota(jnp.int32, (BLOCK, BLOCK), 0)
    col = lax.broadcasted_iota(jnp.int32, (BLOCK, BLOCK), 1)
    lower = jnp.where(col <= row, 1.0, 0.0).astype(BF16)
    upper = jnp.where(col >= row, 1.0, 0.0).astype(BF16)
    forward_lane = col < heads
    fl = forward_lane[0:1]
    for copy in fetch[7:10]:
        copy.wait()
    w_first[:, 768:896] = dot_on(w_step[...], pick.astype(BF16), 0, 0).astype(BF16)
    for b in range(4):
        pace_row = pace[pl.ds(s * 4 + b, 1), :]
        pcol[b * 128 : (b + 1) * 128, :] = jnp.transpose(
            jnp.broadcast_to(pace_row, (128, 128))
        )

    total = part[:, lanes(z * 256, 256)]
    got_all(zbuf, z_recv.at[0])
    for d in range(1, NZ):
        total = total + zbuf[d - 1]
    qbuf[...] = total
    def xy_copy(q):
        return remote(qbuf, xybuf.at[q], xy_send.at[0], xy_recv.at[0], **at_xy(q, 1))

    def send_xy(k, none):
        xy_copy(NX * NY - 1 - k).start()
        return none

    lax.fori_loop(0, NX * NY - 1, send_xy, 0)

    @pl.when(early)
    def _():
        start_all(l_last)
        start_ahead()
        norm_at(left * 128, 64)
        norm_at(right * 128 + 64, 64)

    pl.when(late)(lambda: start_all(l_first + l_next + l_last))

    got_all(xybuf.at[pl.ds(1, NX * NY - 1)], xy_recv.at[0])
    total = qbuf[...]
    for q in range(1, NX * NY):
        total = total + xybuf[q]
    fbuf[...] = total
    for d in (4, 3, 5, 2, 6, 1, 7):
        remote(
            fbuf, mod.at[:, lanes(z * 256, 256)], g_send.at[0], g_recv.at[0],
            sp_0=lax.rem(z + d, NZ),
        ).start()
    mod[:, lanes(z * 256, 256)] = total

    halo_next.wait()
    halo_prev.wait()
    norm_ctx(0)
    norm_ctx(3 * HALO)
    def second_halves():
        for copy in l_next + l_last:
            copy.wait_recv()
        norm_at(left * 128 + 64, 64)
        norm_at(right * 128, 64)

    pl.when(early)(second_halves)

    @pl.when(late)
    def _():
        start_ahead()
        norm_at(left * 128, 64)
        norm_at(right * 128 + 64, 64)

    for copy in fetch[10:]:
        copy.wait()
    rate_row = (
        jnp.dot(
            jnp.broadcast_to(rates[0:1, :], (8, 32)), pick[0:32], precision=HIGHEST,
            preferred_element_type=F32,
        )
        + jnp.dot(
            jnp.broadcast_to(rates[1:2, :], (8, 32)), pick[32:64], precision=HIGHEST,
            preferred_element_type=F32,
        )
    )[0:1]
    value_taps = t_value[:, lanes(y * 512, 512)]
    write_taps = t_write[:, lanes(y * 256, 256)]
    read_taps = t_read[:, lanes(y * 256, 256)]

    got_all(zbuf, g_recv.at[0])

    def block_of(k):
        return lax.rem(y + (lax.rem(k + 1, 3) + 1) * ((k + 3) // 4), NY)

    def modulate(k, none):
        b = block_of(k)

        def chunk(i, none):
            rs = rows(b * 128 + i * 32, 32)
            hid[rows(64 + k * 128 + i * 32, 32), :] = (
                nrm[rs, :] * (1.0 + mod[2:3, :]) + mod[0:1, :]
            ).astype(BF16)
            return none

        lax.fori_loop(0, 4, chunk, 0)
        return none

    def project(rs):
        for c in (slice(0, 256), slice(256, 512), slice(512, 768), slice(768, 896)):
            pre_a[rs, c] = jnp.dot(
                hid[rs, :], w_first[:, c], preferred_element_type=F32
            ).astype(BF16)

    for k in range(2):
        hid[pl.ds(k * 32, 32), :] = (
            nrm[pl.ds(512 + k * 32, 32), :] * (1.0 + mod[3:4, :]) + mod[1:2, :]
        ).astype(BF16)
    modulate(0, 0)
    project(slice(0, 192))

    line_c = lax.broadcasted_iota(jnp.int32, (4 * HALO, 1), 0)
    first = jnp.where(s == 0, HALO, 0)
    last = jnp.where(s == NS - 1, 3 * HALO, 4 * HALO)
    present = (line_c >= first) & (line_c < last)
    own_c = slice(HALO, 3 * HALO)
    cv = pre_a[0:64, 0:512].astype(F32)
    cw = pre_a[0:64, 512:768].astype(F32)
    cv = conv_rows(jnp.where(present, cv, 0.0), value_taps, 4 * HALO)[own_c].astype(BF16)
    cw = conv_rows(jnp.where(present, cw, 0.0), write_taps, 4 * HALO)[own_c].astype(BF16)
    cstep = softplus(pre_a[HALO : 3 * HALO, 768:896].astype(F32))
    cdecay = -rate_row * cstep
    r32 = lax.broadcasted_iota(jnp.int32, (2 * HALO, 2 * HALO), 0)
    c32 = lax.broadcasted_iota(jnp.int32, (2 * HALO, 2 * HALO), 1)
    cparts = jnp.concatenate(three_parts(cdecay), axis=1)

    def ctx_sum(allowed):
        got = jnp.dot(
            jnp.where(allowed, 1.0, 0.0).astype(BF16), cparts, preferred_element_type=F32
        )
        return got[:, 0:128] + got[:, 128:256] + got[:, 256:384]

    later, earlier = ctx_sum(c32 > r32), ctx_sum(c32 < r32)
    cweight = jnp.exp(jnp.where(forward_lane[0 : 2 * HALO], later, earlier)) * cstep
    cvf = cv.astype(F32)
    cscaled = (jnp.concatenate([cvf, cvf], axis=1) * expand(cweight, spread[...])).astype(BF16)
    for g in range(2):
        wg = cw[:, g * 128 : (g + 1) * 128]
        for d in range(2):
            ls = slice((d * 2 + g) * 256, (d * 2 + g + 1) * 256)
            ends_c[:, ls] = dot_on(wg, cscaled[:, ls], 0, 0).astype(BF16)

    def expand3(v):
        high = v.astype(BF16)
        rest = v - high.astype(F32)
        return jnp.dot(high, spread[0:128, :], preferred_element_type=F32) + expand(
            rest, spread[...]
        )

    ctotal = jnp.exp(jnp.sum(cdecay, axis=0, keepdims=True))

    xts = [x] + [lax.rem(x + dx, NX) for dx in range(1, NX)]

    def each_other(start):
        def line(k, none):
            zt = lax.rem(z + NZ // 2 + ((k + 1) // 2) * (1 - 2 * lax.rem(k, 2)), NZ)
            for xt in (xts[2], xts[1], xts[3], xts[0]):
                start(zt, xt)
            return none

        lax.fori_loop(0, NZ - 1, line, 0)
        for xt in (xts[2], xts[1], xts[3]):
            start(z, xt)

    def state_copies(states, got, a_send, a_recv):
        def outgoing(zt, xt):
            return remote(
                states.at[rows(zt * 16, 16), lanes(xt * 256, 256)],
                got.at[s], a_send.at[0], a_recv.at[0], sp_0=zt, sp_1=xt,
            )

        return outgoing

    out_c = state_copies(ends_c, got_c, c_send, c_recv)
    each_other(lambda zt, xt: out_c(zt, xt).start())
    got_c[s] = ends_c[rows(z * 16, 16), lanes(x * 256, 256)]

    def block_states(k, none):
        b = block_of(k)
        at_b = rows(b * 128, 128)
        at_k = rows(64 + k * 128, 128)
        vb = conv_rows(pre_a[at_k, 0:512].astype(F32), value_taps, ROW).astype(BF16)
        val[at_b, :] = vb
        w = conv_rows(pre_a[at_k, 512:768].astype(F32), write_taps, ROW).astype(BF16)
        wri[at_b, :] = w
        step = softplus(pre_a[at_k, 768:896].astype(F32)) * pcol[at_b, :]
        decay = -rate_row * step
        parts = jnp.concatenate(three_parts(decay), axis=1)
        down = jnp.dot(lower, parts, preferred_element_type=F32)
        up = jnp.dot(upper, parts, preferred_element_type=F32)
        both = jnp.where(jnp.concatenate([forward_lane] * 3, axis=1), down, up)
        cums = both[:, 0:128] + both[:, 128:256] + both[:, 256:384]
        total = jnp.where(fl, cums[127:128], cums[0:1])
        cum[at_b, :] = cums
        stp[at_b, :] = step
        weight = jnp.exp(total - cums) * step
        vf = vb.astype(F32)
        scaled = (jnp.concatenate([vf, vf], axis=1) * expand(weight, spread[...])).astype(BF16)
        for g in range(2):
            wg = w[:, g * 128 : (g + 1) * 128]
            for d in range(2):
                ls = slice((d * 2 + g) * 256, (d * 2 + g + 1) * 256)
                inc[b, :, ls] = dot_on(wg, scaled[:, ls], 0, 0)
        tot[pl.ds(b, 1), :] = total
        return none

    block_states(0, 0)

    pl.when(late)(second_halves)
    modulate(1, 0)
    modulate(2, 0)
    ahead.wait_recv()
    back.wait_recv()
    norm_at(opposite * 128, 128)
    modulate(3, 0)
    project(slice(192, 576))
    lax.fori_loop(1, 4, block_states, 0)

    t0, t1, t2, t3 = (tot[b : b + 1, :] for b in range(4))
    zero = jnp.zeros_like(t0)
    etot[...] = expand3(
        jnp.concatenate(
            [jnp.exp(t0), jnp.exp(t1), jnp.exp(t2), jnp.exp(t3), jnp.exp(t0 + t1 + t2 + t3),
             ctotal, zero, zero], axis=0,
        )
    )
    tot_b[...] = etot[4:6, :]
    tot[0:1, :] = jnp.where(fl, zero, t1 + t2 + t3)
    tot[1:2, :] = jnp.where(fl, t0, t2 + t3)
    tot[2:3, :] = jnp.where(fl, t0 + t1, t3)
    tot[3:4, :] = jnp.where(fl, t0 + t1 + t2, zero)
    for d, order in ((0, (0, 1, 2, 3)), (1, (3, 2, 1, 0))):
        for g in range(2):
            ls = slice((d * 2 + g) * 256, (d * 2 + g + 1) * 256)
            state = jnp.zeros((STATE, 256), F32)
            for b in order:
                before[b, :, ls] = state.astype(BF16)
                state = etot[b : b + 1, ls] * state + inc[b, :, ls]
            ends_s[:, ls] = state.astype(BF16)
    out_s = state_copies(ends_s, got_s, s_send, s_recv)

    def out_t(zt, xt):
        return remote(
            tot_b.at[:, lanes(xt * 256, 256)], gtot.at[s],
            t_send.at[0], t_recv.at[0], sp_0=zt, sp_1=xt,
        )

    def send_s(zt, xt):
        out_s(zt, xt).start()
        out_t(zt, xt).start()

    each_other(send_s)
    got_s[s] = ends_s[rows(z * 16, 16), lanes(x * 256, 256)]
    gtot[s] = tot_b[:, lanes(x * 256, 256)]

    for c in (slice(0, 256), slice(256, 512), slice(512, 768)):
        pre_b[:, c] = jnp.dot(
            hid[64:576, :], w_second[:, c], preferred_element_type=F32
        ).astype(BF16)

    def within(k, none):
        b = block_of(k)
        at_b = rows(b * 128, 128)
        at_k = rows(k * 128, 128)
        rb = conv_rows(pre_b[at_k, 0:256].astype(F32), read_taps, ROW).astype(BF16)
        reads[at_b, :] = rb
        cums = cum[at_b, :]
        step = stp[at_b, :]
        cums_t = jnp.transpose(cums)
        step_t = jnp.transpose(step)
        cdec[at_b, :] = jnp.exp(cums + tot[pl.ds(b, 1), :])
        grown = expand(jnp.exp(cums), spread[...])
        for g in range(2):
            r = rb[:, g * 128 : (g + 1) * 128]
            affinity = dot_on(r, wri[at_b, g * 128 : (g + 1) * 128], 1, 1)
            carried = jnp.zeros((128, 256), F32)
            for d in range(2):
                ls = slice((d * 2 + g) * 256, (d * 2 + g + 1) * 256)
                carried = carried + (
                    jnp.dot(r, before[b, :, ls], preferred_element_type=F32) * grown[:, ls]
                )
            for q in range(2):
                mixes = []
                for h in (g * 4 + q * 2, g * 4 + q * 2 + 1):
                    exponent = jnp.where(
                        col <= row,
                        cums[:, h : h + 1] - cums_t[h : h + 1, :],
                        cums[:, 8 + h : 9 + h] - cums_t[8 + h : 9 + h, :],
                    )
                    sf, sb = step_t[h : h + 1, :], step_t[8 + h : 9 + h, :]
                    amount = jnp.where(col < row, sf, jnp.where(col > row, sb, sf + sb))
                    mixes.append((affinity * jnp.exp(exponent) * amount).astype(BF16))
                ls = slice((g * 2 + q) * 128, (g * 2 + q + 1) * 128)
                pair = val[at_b, ls]
                none16 = jnp.zeros_like(pair)
                tall = jnp.concatenate(
                    [jnp.where(col < HEAD, pair, none16), jnp.where(col >= HEAD, pair, none16)],
                    axis=0,
                )
                got = jnp.dot(jnp.concatenate(mixes, axis=1), tall, preferred_element_type=F32)
                local[at_b, ls] = got + carried[:, q * 128 : (q + 1) * 128]
        return none

    lax.fori_loop(0, 4, within, 0)

    turned = x // 2

    def order_of(k):
        return k + turned * (NS - 1 - 2 * k)

    got_all(got_c.at[pl.ds(0, NS - 1)], c_recv.at[0])
    got_all(gtot.at[pl.ds(0, NS - 1)], t_recv.at[0])

    def context_scan(k, state):
        j = order_of(k)
        return gtot[j, 1:2, :] * state + got_c[j].astype(F32)

    state = lax.fori_loop(0, NS, context_scan, jnp.zeros((16, 256), F32))
    got_all(got_s.at[pl.ds(0, NS - 1)], s_recv.at[0])

    def back_copy(j):
        return remote(
            sent.at[j], start.at[rows(z * 16, 16), lanes(x * 256, 256)],
            b_send.at[0], b_recv.at[0], **at(j),
        )

    def latent_scan(k, state):
        j = order_of(k)
        sent[j] = state.astype(BF16)

        @pl.when(j != s)
        def _():
            back_copy(j).start()

        return gtot[j, 0:1, :] * state + got_s[j].astype(F32)

    lax.fori_loop(0, NS, latent_scan, state)
    start[rows(z * 16, 16), lanes(x * 256, 256)] = sent[s]

    def last_tables(k, none):
        at_b = rows(block_of(k) * 128, 128)
        grown_c[at_b, :] = expand(cdec[at_b, :], spread[...])
        gates[at_b, :] = silu(pre_b[rows(k * 128, 128), 256:768].astype(F32))
        return none

    lax.fori_loop(0, 4, last_tables, 0)

    got_all(got_s.at[pl.ds(0, NS - 1)], b_recv.at[0])

    half = w_out.shape[1] // 2

    def make_inner(b):
        at_b = rows(b * 128, 128)
        for g in range(2):
            r = reads[at_b, g * 128 : (g + 1) * 128]
            ch = slice(g * 256, (g + 1) * 256)
            total = local[at_b, ch]
            for d in range(2):
                ls = slice((d * 2 + g) * 256, (d * 2 + g + 1) * 256)
                total = total + jnp.dot(r, start[:, ls], preferred_element_type=F32) * (
                    grown_c[at_b, ls]
                )
            gated = total * gates[at_b, ch]
            power = jnp.mean(gated * gated, -1, keepdims=True)
            gains = jnp.concatenate(
                [gain[pl.ds(y * 4 + g * 2, 1), :], gain[pl.ds(y * 4 + g * 2 + 1, 1), :]], axis=1
            )
            inner[:, ch] = (gated * lax.rsqrt(power + GATED_FLOOR) * gains).astype(BF16)

    def product(side):
        return jnp.dot(
            inner[...], w_out[:, side * half : (side + 1) * half], preferred_element_type=F32
        ).astype(BF16)

    make_inner(opposite)
    far[0] = product(0)
    far_r = remote(far.at[0], got_far.at[0], s1.at[0], r1.at[0], tp=right)
    far_r.start()
    far[1] = product(1)
    far_l = remote(far.at[1], got_far.at[1], s1.at[1], r1.at[1], tp=left)
    far_l.start()
    make_inner(right)
    near_r[1] = product(1)
    raw_r = remote(near_r.at[1], got_r.at[1], s2.at[0], r2.at[0], tp=right)
    raw_r.start()
    near_r[0] = product(0)
    make_inner(left)
    near_l[0] = product(0)
    raw_l = remote(near_l.at[0], got_l.at[0], s2.at[1], r2.at[1], tp=left)
    raw_l.start()
    near_l[1] = product(1)
    far_r.wait_recv()
    near_r[0] = (near_r[0].astype(F32) + got_far[0].astype(F32)).astype(BF16)
    sum_r = remote(near_r.at[0], got_r.at[0], s2.at[2], r2.at[2], tp=right)
    sum_r.start()
    far_l.wait_recv()
    near_l[1] = (near_l[1].astype(F32) + got_far[1].astype(F32)).astype(BF16)
    sum_l = remote(near_l.at[1], got_l.at[1], s2.at[3], r2.at[3], tp=left)
    sum_l.start()
    make_inner(y)
    mine[0] = product(0)
    mine[1] = product(1)

    sent_all(zbuf, z_send.at[0])
    sent_all(xybuf.at[pl.ds(1, NX * NY - 1)], xy_send.at[0])
    sent_all(zbuf, g_send.at[0])
    sent_all(gtot.at[pl.ds(0, NS - 1)], t_send.at[0])
    for sem in (c_send, s_send, b_send):
        sent_all(got_s.at[pl.ds(0, NS - 1)], sem.at[0])
    for copy in l_first + l_next + l_last:
        copy.wait_send()
    ahead.wait_send()
    back.wait_send()

    def close(side):
        cs = slice(side * half, (side + 1) * half)
        mixed = (
            mine[side].astype(F32) + got_r[side].astype(F32) + got_l[side].astype(F32)
        ).astype(BF16)
        own = gat[rows(y * 128, 128), cs]
        out[:, cs] = (own.astype(F32) + mod[4:5, cs] * mixed.astype(F32)).astype(BF16)

    raw_r.wait_recv()
    raw_l.wait_recv()
    sum_r.wait_recv()
    sum_l.wait_recv()
    close(0)
    close(1)
    for copy in (far_r, far_l, raw_r, raw_l, sum_r, sum_l):
        copy.wait_send()


def mixer_call(*args):
    width = args[0].shape[1]
    tokens = NY * 128
    dma = pltpu.SemaphoreType.DMA
    vm = pltpu.VMEM
    same = [vm(args[k].shape, args[k].dtype) for k in range(19)]
    copied = same[2:7] + [vm((width, 896), BF16), vm((width, 768), BF16)] + same[11:19]
    piece = vm((2, 128, width // 2), BF16)
    return pl.pallas_call(
        mixer_kernel,
        out_shape=jax.ShapeDtypeStruct((128, width), BF16),
        in_specs=[ANY] * 19,
        out_specs=VMEM,
        scratch_shapes=copied
        + [
            vm((8, width), F32), vm((NZ - 1, 8, 256), F32), vm((8, 256), F32),
            vm((NX * NY, 8, 256), F32), vm((8, 256), F32), vm((8, width), F32),
            vm((tokens, width), BF16), vm((4 * HALO, width), BF16),
            vm((tokens + 4 * HALO, width), F32), vm((tokens + 4 * HALO, width), BF16),
            vm((tokens + 4 * HALO, 896), BF16), vm((tokens, 768), BF16),
            vm((tokens, 512), BF16), vm((tokens, 256), BF16), vm((tokens, 256), BF16),
            vm((tokens, 512), F32), vm((tokens, 512), F32),
            vm((tokens, 128), F32), vm((tokens, 128), F32), vm((tokens, 128), F32),
            vm((tokens, 128), F32), vm((tokens, 1024), F32),
            vm((256, 1024), BF16), vm((4, STATE, 1024), F32), vm((4, STATE, 1024), BF16),
            vm((8, 1024), F32), vm((8, 128), F32),
            vm((STATE, 1024), BF16), vm((STATE, 1024), BF16), vm((2, 1024), F32),
            vm((NS, 16, 256), BF16), vm((NS, 16, 256), BF16), vm((NS, 2, 256), F32),
            vm((NS, 16, 256), BF16), vm((STATE, 1024), BF16),
            vm((128, 512), BF16), piece, piece, piece, piece, piece, piece, piece,
            dma((19,)),
        ]
        + [dma((1,))] * 6
        + [dma((6,))] * 2 + [dma((2,))] * 2 + [dma((2,))] * 2
        + [dma((1,))] * 8
        + [dma((2,)), dma((2,)), dma((4,)), dma((4,))],
        compiler_params=pltpu.CompilerParams(
            collective_id=0, has_side_effects=True, vmem_limit_bytes=60 << 20
        ),
        name="mixer",
    )(*args)


def per_device(
    latent, condition, context, context_cond, shift_matrix, scale_matrix, gate_matrix,
    value_proj, gate_proj, write_proj, read_proj, step_proj, decay_rate, pacing,
    value_taps, write_taps, read_taps, norm_gain, out_proj,
):
    width = latent.shape[2]
    updated = mixer_call(
        latent[0], context[0], condition.reshape(width // 128, 128),
        context_cond.reshape(width // 128, 128), shift_matrix, scale_matrix, gate_matrix,
        value_proj, gate_proj, write_proj, read_proj,
        step_proj.transpose(1, 2, 0).reshape(64, width), decay_rate, pacing.reshape(128, 128),
        value_taps, write_taps, read_taps, norm_gain.reshape(-1, 128), out_proj,
    )
    return updated[None]


def solution(mesh):
    torus = Mesh(
        mesh.devices.reshape(NZ, NX, mesh.shape["tp"], mesh.shape["dp"]),
        ("sp_0", "sp_1", "tp", "dp"),
    )
    placed = (
        P("dp", SP_TP, None), P("dp", None), P("dp", SP, None), P(),
        P(SP_TP, None), P(SP_TP, None), P(SP_TP, None),
        P(None, "tp"), P(None, "tp"), P(None, "tp"), P(None, "tp"),
        P(), P(), P("dp", None), P(), P(), P(), P(), P("tp", None),
    )
    return jax.shard_map(
        per_device, mesh=torus, in_specs=placed, out_specs=P("dp", SP_TP, None), check_vma=False
    )
```

```python
import jax
import jax.numpy as jnp
from jax import lax
from jax.experimental import pallas as pl
from jax.experimental.pallas import tpu as pltpu
from jax.sharding import Mesh
from jax.sharding import PartitionSpec as P

HEAD = 64
STATE = 128
ROW = 64
BLOCK = 128
HALO = 16
SP = ("sp_0", "sp_1")
SP_TP = ("sp_0", "sp_1", "tp")
NZ, NX, NY = 8, 4, 4
NS = NZ * NX

NORM_FLOOR = 1e-05
GATED_FLOOR = 1e-06
MESH = pl.DeviceIdType.MESH
F32 = jnp.float32
BF16 = jnp.bfloat16
HIGHEST = lax.Precision.HIGHEST
VMEM = pl.BlockSpec(memory_space=pltpu.VMEM)
ANY = pl.BlockSpec(memory_space=pl.ANY)


def silu(v):
    return v / (1.0 + jnp.exp(-v))


def remote(src, dst, send, recv, **where):
    return pltpu.make_async_remote_copy(
        src_ref=src, dst_ref=dst, send_sem=send, recv_sem=recv, device_id=where, device_id_type=MESH
    )


def position():
    return lax.axis_index("sp_0"), lax.axis_index("sp_1"), lax.axis_index("tp")


def lanes(start, size):
    return pl.ds(pl.multiple_of(start, 128), size)


def rows(start, size):
    return pl.ds(pl.multiple_of(start, 16), size)


def normed_rows(block):
    values = block.astype(F32)
    center = jnp.mean(values, -1, keepdims=True)
    off = values - center
    spread = jnp.mean(off * off, -1, keepdims=True)
    return off * lax.rsqrt(spread + NORM_FLOOR)


def conv_rows(pre, taps, run):
    length = pre.shape[0]
    at = lax.rem(lax.broadcasted_iota(jnp.int32, pre.shape, 0), run)
    total = pre * taps[2:3]
    for k in (0, 1, 3, 4):
        moved = pltpu.roll(pre, (2 - k) % length, 0)
        inside = (at + (k - 2) >= 0) & (at + (k - 2) < run)
        total = total + jnp.where(inside, moved, 0.0) * taps[k : k + 1]
    return silu(total)


def expand(v, spread):
    high = v.astype(BF16)
    low = (v - high.astype(F32)).astype(BF16)
    return jnp.dot(
        jnp.concatenate([high, low], axis=1), spread, preferred_element_type=F32
    )


def three_parts(v):
    high = v.astype(BF16)
    rest = v - high.astype(F32)
    mid = rest.astype(BF16)
    return high, mid, (rest - mid.astype(F32)).astype(BF16)


def softplus(v):
    return jnp.maximum(v, 0.0) + jnp.log1p(jnp.exp(-jnp.abs(v)))


def spread_matrix(spread):
    shape = spread.shape
    row = lax.rem(lax.broadcasted_iota(jnp.int32, shape, 0), 128)
    col = lax.broadcasted_iota(jnp.int32, shape, 1)
    spread[...] = jnp.where(row == col // HEAD, 1.0, 0.0).astype(BF16)


def dot_on(a, b, ca, cb):
    return lax.dot_general(a, b, (((ca,), (cb,)), ((), ())), preferred_element_type=F32)


def mixer_kernel(
    lat_h, ctx_h, cond_h, ccond_h, shift_h, scale_h, gatem_h,
    wv_h, wg_h, ww_h, wr_h, ws_h, rate_h, pace_h, tv_h, tw_h, tr_h, gain_h, wo_h,
    out,
    cond, ccond, shift_m, scale_m, gate_m,
    w_first, w_second, w_step, rates, pace, t_value, t_write, t_read, gain, w_out,
    part, zbuf, qbuf, xybuf, fbuf, mod,
    gat, ctx_ext, nrm, hid, pre_a, pre_b, val, wri, reads, gates, local,
    cum, stp, cdec, pcol, grown_c, spread, inc, before, etot, tot,
    ends_s, ends_c, tot_b, got_s, got_c, gtot, grow_s, grow_c, sent, start,
    inner, far, near_r, near_l, mine, got_far, got_r, got_l,
    in_sem, z_send, z_recv, xy_send, xy_recv, g_send, g_recv,
    l_send, l_recv, f_send, f_recv, h_send, h_recv,
    s_send, s_recv, t_send, t_recv, c_send, c_recv, b_send, b_recv,
    s1, r1, s2, r2,
):
    z, x, y = position()
    s = z * NX + x
    rank = s * NY + y
    right, left = lax.rem(y + 1, NY), lax.rem(y + NY - 1, NY)
    opposite = lax.rem(y + 2, NY)
    heads = 8

    def at(t):
        return {"sp_0": t // NX, "sp_1": lax.rem(t, NX)}

    def at_xy(q, sign):
        return {
            "sp_1": lax.rem(x + NX + sign * (q // NY), NX),
            "tp": lax.rem(y + NY + sign * lax.rem(q, NY), NY),
        }

    own_rows = gat.at[rows(y * 128, 128)]
    pairs = [
        (cond_h, cond), (ccond_h, ccond), (shift_h, shift_m), (scale_h, scale_m),
        (gatem_h, gate_m), (lat_h, own_rows), (ctx_h, ctx_ext.at[pl.ds(HALO, 2 * HALO)]),
        (ws_h, w_step), (rate_h, rates), (pace_h, pace),
        (wv_h, w_first.at[:, pl.ds(0, 512)]), (ww_h, w_first.at[:, pl.ds(512, 256)]),
        (tv_h, t_value), (tw_h, t_write), (wr_h, w_second.at[:, pl.ds(0, 256)]),
        (wg_h, w_second.at[:, pl.ds(256, 512)]), (tr_h, t_read),
        (gain_h, gain), (wo_h, w_out),
    ]
    fetch = [pltpu.make_async_copy(a, b, in_sem.at[k]) for k, (a, b) in enumerate(pairs)]
    for copy in fetch[:7]:
        copy.start()

    xts = [x] + [lax.rem(x + dx, NX) for dx in range(1, NX)]

    def each_other(start):
        def line(k, none):
            zt = lax.rem(z + NZ // 2 + ((k + 1) // 2) * (1 - 2 * lax.rem(k, 2)), NZ)
            for xt in (xts[2], xts[1], xts[3], xts[0]):
                start(zt, xt)
            return none

        lax.fori_loop(0, NZ - 1, line, 0)
        for xt in (xts[2], xts[1], xts[3]):
            start(z, xt)

    barrier = pltpu.get_barrier_semaphore()
    each_other(
        lambda zt, xt: pl.semaphore_signal(
            barrier, inc=1, device_id={"sp_0": zt, "sp_1": xt}, device_id_type=MESH
        )
    )
    for dy in (2, 1, 3):
        for xt in xts:
            pl.semaphore_signal(
                barrier, inc=1, device_id={"sp_1": xt, "tp": lax.rem(y + dy, NY)},
                device_id_type=MESH,
            )

    for copy in fetch[:5]:
        copy.wait()
    vec_row, vec_off = rank // 8, lax.rem(rank, 8) * 16
    lane = lax.broadcasted_iota(jnp.int32, (8, 128), 1)
    line = lax.broadcasted_iota(jnp.int32, (8, 128), 0)
    window = (lane >= vec_off) & (lane < vec_off + 16)
    both = jnp.where(
        line == 0,
        jnp.broadcast_to(cond[pl.ds(vec_row, 1), :], (8, 128)),
        jnp.broadcast_to(ccond[pl.ds(vec_row, 1), :], (8, 128)),
    )
    acts = jnp.where(window, silu(both), 0.0).astype(BF16)

    def product_of(matrix):
        tall = jnp.concatenate([matrix[...]] * 8, axis=0)
        return jnp.dot(acts, tall, preferred_element_type=F32)

    part[0:2, :] = product_of(shift_m)[0:2]
    part[2:4, :] = product_of(scale_m)[0:2]
    part[4:8, :] = product_of(gate_m)[0:4]
    def norm_at(base, count):
        for k in range(count // 64):
            rs = rows(base + k * 64, 64)
            nrm[rs, :] = normed_rows(gat[rs, :])

    def norm_ctx(base):
        nrm[pl.ds(512 + base, HALO), :] = normed_rows(ctx_ext[pl.ds(base, HALO), :])

    pl.semaphore_wait(barrier, NS - 1 + NX * (NY - 1))

    nxt, prv = lax.rem(s + 1, NS), lax.rem(s + NS - 1, NS)

    def got_all(ref, recv):
        remote(ref, ref, recv, recv, **at(nxt)).wait_recv()

    def sent_all(ref, send):
        remote(ref, ref, send, send, **at(nxt)).wait_send()

    for d in (4, 3, 5, 2, 6, 1, 7):
        to = lax.rem(z + d, NZ)
        remote(
            part.at[:, lanes(to * 256, 256)], zbuf.at[d - 1], z_send.at[0], z_recv.at[0], sp_0=to
        ).start()

    def latent_piece(side, first_row, count, k):
        piece = gat.at[rows(y * 128 + first_row, count)]
        return remote(
            piece, piece, l_send.at[k], l_recv.at[k], tp=right if side == 0 else left
        )

    def latent_ahead(side):
        owner = left if side == 0 else right
        piece = gat.at[rows(owner * 128 + side * 64, 64)]
        return remote(
            piece, piece, f_send.at[side], f_recv.at[side], tp=right if side == 0 else left
        )

    l_first = [latent_piece(0, 0, 64, 0), latent_piece(1, 64, 64, 1)]
    l_next = [latent_piece(0, 64, 32, 2), latent_piece(1, 0, 32, 3)]
    l_last = [latent_piece(0, 96, 32, 4), latent_piece(1, 32, 32, 5)]
    ahead, back = latent_ahead(0), latent_ahead(1)

    def start_all(copies):
        for copy in copies:
            copy.start()

    def start_ahead():
        l_first[0].wait_recv()
        ahead.start()
        l_first[1].wait_recv()
        back.start()

    early = lax.axis_index("dp") == 1
    late = lax.axis_index("dp") == 0
    fetch[5].wait()
    fetch[6].wait()
    pl.when(early)(lambda: start_all(l_first + l_next))
    halo_next = remote(
        ctx_ext.at[pl.ds(2 * HALO, HALO)], ctx_ext.at[pl.ds(0, HALO)],
        h_send.at[0], h_recv.at[0], **at(nxt),
    )
    halo_prev = remote(
        ctx_ext.at[pl.ds(HALO, HALO)], ctx_ext.at[pl.ds(3 * HALO, HALO)],
        h_send.at[1], h_recv.at[1], **at(prv),
    )
    halo_next.start()
    halo_prev.start()

    for copy in fetch[7:]:
        copy.start()
    norm_at(y * 128, 128)
    norm_ctx(HALO)
    norm_ctx(2 * HALO)
    spread_matrix(spread)
    row64 = lax.broadcasted_iota(jnp.int32, (64, 128), 0)
    col64 = lax.broadcasted_iota(jnp.int32, (64, 128), 1)
    wanted = jnp.where(col64 < heads, y * heads + col64, 32 + y * heads + col64 - heads)
    pick = jnp.where((row64 == wanted) & (col64 < 2 * heads), 1.0, 0.0)
    row = lax.broadcasted_iota(jnp.int32, (BLOCK, BLOCK), 0)
    col = lax.broadcasted_iota(jnp.int32, (BLOCK, BLOCK), 1)
    lower = jnp.where(col <= row, 1.0, 0.0).astype(BF16)
    upper = jnp.where(col >= row, 1.0, 0.0).astype(BF16)
    forward_lane = col < heads
    fl = forward_lane[0:1]
    for copy in fetch[7:10]:
        copy.wait()
    w_first[:, 768:896] = dot_on(w_step[...], pick.astype(BF16), 0, 0).astype(BF16)
    for b in range(4):
        pace_row = pace[pl.ds(s * 4 + b, 1), :]
        pcol[b * 128 : (b + 1) * 128, :] = jnp.transpose(
            jnp.broadcast_to(pace_row, (128, 128))
        )

    total = part[:, lanes(z * 256, 256)]
    got_all(zbuf, z_recv.at[0])
    for d in range(1, NZ):
        total = total + zbuf[d - 1]
    qbuf[...] = total
    def xy_copy(q):
        return remote(qbuf, xybuf.at[q], xy_send.at[0], xy_recv.at[0], **at_xy(q, 1))

    def send_xy(k, none):
        xy_copy(NX * NY - 1 - k).start()
        return none

    lax.fori_loop(0, NX * NY - 1, send_xy, 0)

    @pl.when(early)
    def _():
        start_all(l_last)
        start_ahead()
        norm_at(left * 128, 64)
        norm_at(right * 128 + 64, 64)

    pl.when(late)(lambda: start_all(l_first + l_next + l_last))

    got_all(xybuf.at[pl.ds(1, NX * NY - 1)], xy_recv.at[0])
    total = qbuf[...]
    for q in range(1, NX * NY):
        total = total + xybuf[q]
    fbuf[...] = total
    for d in (4, 3, 5, 2, 6, 1, 7):
        remote(
            fbuf, mod.at[:, lanes(z * 256, 256)], g_send.at[0], g_recv.at[0],
            sp_0=lax.rem(z + d, NZ),
        ).start()
    mod[:, lanes(z * 256, 256)] = total

    halo_next.wait()
    halo_prev.wait()
    norm_ctx(0)
    norm_ctx(3 * HALO)
    def second_halves():
        for copy in l_next + l_last:
            copy.wait_recv()
        norm_at(left * 128 + 64, 64)
        norm_at(right * 128, 64)

    pl.when(early)(second_halves)

    @pl.when(late)
    def _():
        start_ahead()
        norm_at(left * 128, 64)
        norm_at(right * 128 + 64, 64)

    for copy in fetch[10:]:
        copy.wait()
    rate_row = (
        jnp.dot(
            jnp.broadcast_to(rates[0:1, :], (8, 32)), pick[0:32], precision=HIGHEST,
            preferred_element_type=F32,
        )
        + jnp.dot(
            jnp.broadcast_to(rates[1:2, :], (8, 32)), pick[32:64], precision=HIGHEST,
            preferred_element_type=F32,
        )
    )[0:1]
    value_taps = t_value[:, lanes(y * 512, 512)]
    write_taps = t_write[:, lanes(y * 256, 256)]
    read_taps = t_read[:, lanes(y * 256, 256)]

    got_all(zbuf, g_recv.at[0])

    def block_of(k):
        return lax.rem(y + (lax.rem(k + 1, 3) + 1) * ((k + 3) // 4), NY)

    def modulate(k, none):
        b = block_of(k)

        for i in range(2):
            rs = rows(b * 128 + i * 64, 64)
            hid[rows(64 + k * 128 + i * 64, 64), :] = (
                nrm[rs, :] * (1.0 + mod[2:3, :]) + mod[0:1, :]
            ).astype(BF16)
        return none

    def project(rs):
        for c in (slice(0, 256), slice(256, 512), slice(512, 768), slice(768, 896)):
            pre_a[rs, c] = jnp.dot(
                hid[rs, :], w_first[:, c], preferred_element_type=F32
            ).astype(BF16)

    for k in range(2):
        hid[pl.ds(k * 32, 32), :] = (
            nrm[pl.ds(512 + k * 32, 32), :] * (1.0 + mod[3:4, :]) + mod[1:2, :]
        ).astype(BF16)
    modulate(0, 0)
    project(slice(0, 192))

    line_c = lax.broadcasted_iota(jnp.int32, (4 * HALO, 1), 0)
    first = jnp.where(s == 0, HALO, 0)
    last = jnp.where(s == NS - 1, 3 * HALO, 4 * HALO)
    present = (line_c >= first) & (line_c < last)
    own_c = slice(HALO, 3 * HALO)
    cv = pre_a[0:64, 0:512].astype(F32)
    cw = pre_a[0:64, 512:768].astype(F32)
    cv = conv_rows(jnp.where(present, cv, 0.0), value_taps, 4 * HALO)[own_c].astype(BF16)
    cw = conv_rows(jnp.where(present, cw, 0.0), write_taps, 4 * HALO)[own_c].astype(BF16)
    cstep = softplus(pre_a[HALO : 3 * HALO, 768:896].astype(F32))
    cdecay = -rate_row * cstep
    r32 = lax.broadcasted_iota(jnp.int32, (2 * HALO, 2 * HALO), 0)
    c32 = lax.broadcasted_iota(jnp.int32, (2 * HALO, 2 * HALO), 1)
    cparts = jnp.concatenate(three_parts(cdecay), axis=1)

    def ctx_sum(allowed):
        got = jnp.dot(
            jnp.where(allowed, 1.0, 0.0).astype(BF16), cparts, preferred_element_type=F32
        )
        return got[:, 0:128] + got[:, 128:256] + got[:, 256:384]

    later, earlier = ctx_sum(c32 > r32), ctx_sum(c32 < r32)
    cweight = jnp.exp(jnp.where(forward_lane[0 : 2 * HALO], later, earlier)) * cstep
    cvf = cv.astype(F32)
    cscaled = (jnp.concatenate([cvf, cvf], axis=1) * expand(cweight, spread[...])).astype(BF16)
    for g in range(2):
        wg = cw[:, g * 128 : (g + 1) * 128]
        for d in range(2):
            ls = slice((d * 2 + g) * 256, (d * 2 + g + 1) * 256)
            ends_c[:, ls] = dot_on(wg, cscaled[:, ls], 0, 0).astype(BF16)

    def expand3(v):
        high = v.astype(BF16)
        rest = v - high.astype(F32)
        return jnp.dot(high, spread[0:128, :], preferred_element_type=F32) + expand(
            rest, spread[...]
        )

    ctotal = jnp.exp(jnp.sum(cdecay, axis=0, keepdims=True))

    def state_copies(states, got, a_send, a_recv):
        def outgoing(zt, xt):
            return remote(
                states.at[rows(zt * 16, 16), lanes(xt * 256, 256)],
                got.at[s], a_send.at[0], a_recv.at[0], sp_0=zt, sp_1=xt,
            )

        return outgoing

    out_c = state_copies(ends_c, got_c, c_send, c_recv)
    each_other(lambda zt, xt: out_c(zt, xt).start())
    got_c[s] = ends_c[rows(z * 16, 16), lanes(x * 256, 256)]

    def block_states(k, none):
        b = block_of(k)
        at_b = rows(b * 128, 128)
        at_k = rows(64 + k * 128, 128)
        vb = conv_rows(pre_a[at_k, 0:512].astype(F32), value_taps, ROW).astype(BF16)
        val[at_b, :] = vb
        w = conv_rows(pre_a[at_k, 512:768].astype(F32), write_taps, ROW).astype(BF16)
        wri[at_b, :] = w
        step = softplus(pre_a[at_k, 768:896].astype(F32)) * pcol[at_b, :]
        decay = -rate_row * step
        parts = jnp.concatenate(three_parts(decay), axis=1)
        down = jnp.dot(lower, parts, preferred_element_type=F32)
        up = jnp.dot(upper, parts, preferred_element_type=F32)
        both = jnp.where(jnp.concatenate([forward_lane] * 3, axis=1), down, up)
        cums = both[:, 0:128] + both[:, 128:256] + both[:, 256:384]
        total = jnp.where(fl, cums[127:128], cums[0:1])
        cum[at_b, :] = cums
        stp[at_b, :] = step
        weight = jnp.exp(total - cums) * step
        vf = vb.astype(F32)
        scaled = (jnp.concatenate([vf, vf], axis=1) * expand(weight, spread[...])).astype(BF16)
        for g in range(2):
            fs = slice(g * 256, (g + 1) * 256)
            bs = slice(512 + g * 256, 512 + (g + 1) * 256)
            states = dot_on(
                w[:, g * 128 : (g + 1) * 128],
                jnp.concatenate([scaled[:, fs], scaled[:, bs]], axis=1), 0, 0,
            )
            inc[b, :, fs] = states[:, 0:256]
            inc[b, :, bs] = states[:, 256:512]
        tot[pl.ds(b, 1), :] = total
        return none

    block_states(0, 0)

    pl.when(late)(second_halves)
    modulate(1, 0)
    modulate(2, 0)
    ahead.wait_recv()
    back.wait_recv()
    norm_at(opposite * 128, 128)
    modulate(3, 0)
    project(slice(192, 576))
    lax.fori_loop(1, 4, block_states, 0)

    t0, t1, t2, t3 = (tot[b : b + 1, :] for b in range(4))
    zero = jnp.zeros_like(t0)
    etot[...] = expand3(
        jnp.concatenate(
            [jnp.exp(t0), jnp.exp(t1), jnp.exp(t2), jnp.exp(t3), jnp.exp(t0 + t1 + t2 + t3),
             zero, zero, zero], axis=0,
        )
    )
    lane1 = lane[0:1]
    tot_b[...] = jnp.where(
        lane1 < 2 * heads, jnp.exp(t0 + t1 + t2 + t3),
        jnp.where(lane1 < 4 * heads, pltpu.roll(ctotal, 2 * heads, 1), 0.0),
    )
    tot[0:1, :] = jnp.where(fl, zero, t1 + t2 + t3)
    tot[1:2, :] = jnp.where(fl, t0, t2 + t3)
    tot[2:3, :] = jnp.where(fl, t0 + t1, t3)
    tot[3:4, :] = jnp.where(fl, t0 + t1 + t2, zero)
    for d, order in ((0, (0, 1, 2, 3)), (1, (3, 2, 1, 0))):
        for g in range(2):
            ls = slice((d * 2 + g) * 256, (d * 2 + g + 1) * 256)
            state = jnp.zeros((STATE, 256), F32)
            for b in order:
                before[b, :, ls] = state.astype(BF16)
                state = etot[b : b + 1, ls] * state + inc[b, :, ls]
            ends_s[:, ls] = state.astype(BF16)
    out_s = state_copies(ends_s, got_s, s_send, s_recv)

    def out_t(zt, xt):
        return remote(tot_b, gtot.at[s], t_send.at[0], t_recv.at[0], sp_0=zt, sp_1=xt)

    def send_s(zt, xt):
        out_t(zt, xt).start()
        out_s(zt, xt).start()

    each_other(send_s)
    got_s[s] = ends_s[rows(z * 16, 16), lanes(x * 256, 256)]
    gtot[s] = tot_b[...]

    for c in (slice(0, 256), slice(256, 512), slice(512, 768)):
        pre_b[:, c] = jnp.dot(
            hid[64:576, :], w_second[:, c], preferred_element_type=F32
        ).astype(BF16)

    def within(k, none):
        b = block_of(k)
        at_b = rows(b * 128, 128)
        at_k = rows(k * 128, 128)
        rb = conv_rows(pre_b[at_k, 0:256].astype(F32), read_taps, ROW).astype(BF16)
        reads[at_b, :] = rb
        cums = cum[at_b, :]
        step = stp[at_b, :]
        cums_t = jnp.transpose(cums)
        step_t = jnp.transpose(step)
        cdec[at_b, :] = jnp.exp(cums + tot[pl.ds(b, 1), :])
        grown = expand(jnp.exp(cums), spread[...])
        for g in range(2):
            r = rb[:, g * 128 : (g + 1) * 128]
            affinity = dot_on(r, wri[at_b, g * 128 : (g + 1) * 128], 1, 1)
            carried = jnp.zeros((128, 256), F32)
            for d in range(2):
                ls = slice((d * 2 + g) * 256, (d * 2 + g + 1) * 256)
                carried = carried + (
                    jnp.dot(r, before[b, :, ls], preferred_element_type=F32) * grown[:, ls]
                )
            for q in range(2):
                mixes = []
                for h in (g * 4 + q * 2, g * 4 + q * 2 + 1):
                    exponent = jnp.where(
                        col <= row,
                        cums[:, h : h + 1] - cums_t[h : h + 1, :],
                        cums[:, 8 + h : 9 + h] - cums_t[8 + h : 9 + h, :],
                    )
                    sf, sb = step_t[h : h + 1, :], step_t[8 + h : 9 + h, :]
                    amount = jnp.where(col < row, sf, jnp.where(col > row, sb, sf + sb))
                    mixes.append((affinity * jnp.exp(exponent) * amount).astype(BF16))
                ls = slice((g * 2 + q) * 128, (g * 2 + q + 1) * 128)
                pair = val[at_b, ls]
                none16 = jnp.zeros_like(pair)
                tall = jnp.concatenate(
                    [jnp.where(col < HEAD, pair, none16), jnp.where(col >= HEAD, pair, none16)],
                    axis=0,
                )
                got = jnp.dot(jnp.concatenate(mixes, axis=1), tall, preferred_element_type=F32)
                local[at_b, ls] = got + carried[:, q * 128 : (q + 1) * 128]
        return none

    lax.fori_loop(0, 4, within, 0)

    turned = x // 2

    def order_of(k):
        return k + turned * (NS - 1 - 2 * k)

    got_all(gtot.at[pl.ds(0, NS - 1)], t_recv.at[0])

    def spread_own(v):
        high, mid, low = three_parts(v)
        own = lanes(x * 256, 256)
        return jnp.dot(high, spread[0:128, own], preferred_element_type=F32) + jnp.dot(
            jnp.concatenate([mid, low], axis=1), spread[:, own], preferred_element_type=F32
        )

    ranges = gtot[...].reshape(NS, 128)
    grow_s[...] = spread_own(ranges)
    grow_c[...] = spread_own(pltpu.roll(ranges, 128 - 2 * heads, 1))
    got_all(got_c.at[pl.ds(0, NS - 1)], c_recv.at[0])

    def context_scan(k, state):
        j = order_of(k)
        return grow_c[pl.ds(j, 1), :] * state + got_c[j].astype(F32)

    state = lax.fori_loop(0, NS, context_scan, jnp.zeros((16, 256), F32))
    got_all(got_s.at[pl.ds(0, NS - 1)], s_recv.at[0])

    def back_copy(j):
        return remote(
            sent.at[j], start.at[rows(z * 16, 16), lanes(x * 256, 256)],
            b_send.at[0], b_recv.at[0], **at(j),
        )

    def latent_scan(k, state):
        j = order_of(k)
        sent[j] = state.astype(BF16)

        @pl.when(j != s)
        def _():
            back_copy(j).start()

        return grow_s[pl.ds(j, 1), :] * state + got_s[j].astype(F32)

    lax.fori_loop(0, NS, latent_scan, state)
    start[rows(z * 16, 16), lanes(x * 256, 256)] = sent[s]

    def last_tables(k, none):
        at_b = rows(block_of(k) * 128, 128)
        grown_c[at_b, :] = expand(cdec[at_b, :], spread[...])
        gates[at_b, :] = silu(pre_b[rows(k * 128, 128), 256:768].astype(F32))
        return none

    lax.fori_loop(0, 4, last_tables, 0)

    got_all(got_s.at[pl.ds(0, NS - 1)], b_recv.at[0])

    half = w_out.shape[1] // 2

    def make_inner(b):
        at_b = rows(b * 128, 128)
        for g in range(2):
            r = reads[at_b, g * 128 : (g + 1) * 128]
            ch = slice(g * 256, (g + 1) * 256)
            total = local[at_b, ch]
            for d in range(2):
                ls = slice((d * 2 + g) * 256, (d * 2 + g + 1) * 256)
                total = total + jnp.dot(r, start[:, ls], preferred_element_type=F32) * (
                    grown_c[at_b, ls]
                )
            gated = total * gates[at_b, ch]
            power = jnp.mean(gated * gated, -1, keepdims=True)
            gains = jnp.concatenate(
                [gain[pl.ds(y * 4 + g * 2, 1), :], gain[pl.ds(y * 4 + g * 2 + 1, 1), :]], axis=1
            )
            inner[:, ch] = (gated * lax.rsqrt(power + GATED_FLOOR) * gains).astype(BF16)

    def product(side):
        return jnp.dot(
            inner[...], w_out[:, side * half : (side + 1) * half], preferred_element_type=F32
        ).astype(BF16)

    make_inner(opposite)
    far[0] = product(0)
    far_r = remote(far.at[0], got_far.at[0], s1.at[0], r1.at[0], tp=right)
    far_r.start()
    far[1] = product(1)
    far_l = remote(far.at[1], got_far.at[1], s1.at[1], r1.at[1], tp=left)
    far_l.start()
    make_inner(right)
    near_r[1] = product(1)
    raw_r = remote(near_r.at[1], got_r.at[1], s2.at[0], r2.at[0], tp=right)
    raw_r.start()
    near_r[0] = product(0)
    make_inner(left)
    near_l[0] = product(0)
    raw_l = remote(near_l.at[0], got_l.at[0], s2.at[1], r2.at[1], tp=left)
    raw_l.start()
    near_l[1] = product(1)
    far_r.wait_recv()
    near_r[0] = (near_r[0].astype(F32) + got_far[0].astype(F32)).astype(BF16)
    sum_r = remote(near_r.at[0], got_r.at[0], s2.at[2], r2.at[2], tp=right)
    sum_r.start()
    far_l.wait_recv()
    near_l[1] = (near_l[1].astype(F32) + got_far[1].astype(F32)).astype(BF16)
    sum_l = remote(near_l.at[1], got_l.at[1], s2.at[3], r2.at[3], tp=left)
    sum_l.start()
    make_inner(y)
    mine[0] = product(0)
    mine[1] = product(1)

    sent_all(zbuf, z_send.at[0])
    sent_all(xybuf.at[pl.ds(1, NX * NY - 1)], xy_send.at[0])
    sent_all(zbuf, g_send.at[0])
    sent_all(gtot.at[pl.ds(0, NS - 1)], t_send.at[0])
    for sem in (c_send, s_send, b_send):
        sent_all(got_s.at[pl.ds(0, NS - 1)], sem.at[0])
    for copy in l_first + l_next + l_last:
        copy.wait_send()
    ahead.wait_send()
    back.wait_send()

    def close(side):
        cs = slice(side * half, (side + 1) * half)
        mixed = (
            mine[side].astype(F32) + got_r[side].astype(F32) + got_l[side].astype(F32)
        ).astype(BF16)
        own = gat[rows(y * 128, 128), cs]
        out[:, cs] = (own.astype(F32) + mod[4:5, cs] * mixed.astype(F32)).astype(BF16)

    raw_r.wait_recv()
    raw_l.wait_recv()
    sum_r.wait_recv()
    sum_l.wait_recv()
    close(0)
    close(1)
    for copy in (far_r, far_l, raw_r, raw_l, sum_r, sum_l):
        copy.wait_send()


def mixer_call(*args):
    width = args[0].shape[1]
    tokens = NY * 128
    dma = pltpu.SemaphoreType.DMA
    vm = pltpu.VMEM
    same = [vm(args[k].shape, args[k].dtype) for k in range(19)]
    copied = same[2:7] + [vm((width, 896), BF16), vm((width, 768), BF16)] + same[11:19]
    piece = vm((2, 128, width // 2), BF16)
    return pl.pallas_call(
        mixer_kernel,
        out_shape=pltpu.VMEM((128, width), BF16),
        in_specs=[ANY] * 19,
        out_specs=VMEM,
        scratch_shapes=copied
        + [
            vm((8, width), F32), vm((NZ - 1, 8, 256), F32), vm((8, 256), F32),
            vm((NX * NY, 8, 256), F32), vm((8, 256), F32), vm((8, width), F32),
            vm((tokens, width), BF16), vm((4 * HALO, width), BF16),
            vm((tokens + 4 * HALO, width), F32), vm((tokens + 4 * HALO, width), BF16),
            vm((tokens + 4 * HALO, 896), BF16), vm((tokens, 768), BF16),
            vm((tokens, 512), BF16), vm((tokens, 256), BF16), vm((tokens, 256), BF16),
            vm((tokens, 512), F32), vm((tokens, 512), F32),
            vm((tokens, 128), F32), vm((tokens, 128), F32), vm((tokens, 128), F32),
            vm((tokens, 128), F32), vm((tokens, 1024), F32),
            vm((256, 1024), BF16), vm((4, STATE, 1024), F32), vm((4, STATE, 1024), BF16),
            vm((8, 1024), F32), vm((8, 128), F32),
            vm((STATE, 1024), BF16), vm((STATE, 1024), BF16), vm((1, 128), F32),
            vm((NS, 16, 256), BF16), vm((NS, 16, 256), BF16), vm((NS, 1, 128), F32),
            vm((NS, 256), F32), vm((NS, 256), F32),
            vm((NS, 16, 256), BF16), vm((STATE, 1024), BF16),
            vm((128, 512), BF16), piece, piece, piece, piece, piece, piece, piece,
            dma((19,)),
        ]
        + [dma((1,))] * 6
        + [dma((6,))] * 2 + [dma((2,))] * 2 + [dma((2,))] * 2
        + [dma((1,))] * 8
        + [dma((2,)), dma((2,)), dma((4,)), dma((4,))],
        compiler_params=pltpu.CompilerParams(
            collective_id=0, has_side_effects=True, vmem_limit_bytes=56 << 20
        ),
        name="mixer",
    )(*args)


def per_device(
    latent, condition, context, context_cond, shift_matrix, scale_matrix, gate_matrix,
    value_proj, gate_proj, write_proj, read_proj, step_proj, decay_rate, pacing,
    value_taps, write_taps, read_taps, norm_gain, out_proj,
):
    width = latent.shape[2]
    updated = mixer_call(
        latent[0], context[0], condition.reshape(width // 128, 128),
        context_cond.reshape(width // 128, 128), shift_matrix, scale_matrix, gate_matrix,
        value_proj, gate_proj, write_proj, read_proj,
        step_proj.transpose(1, 2, 0).reshape(64, width), decay_rate, pacing.reshape(128, 128),
        value_taps, write_taps, read_taps, norm_gain.reshape(-1, 128), out_proj,
    )
    return updated[None]


def solution(mesh):
    torus = Mesh(
        mesh.devices.reshape(NZ, NX, mesh.shape["tp"], mesh.shape["dp"]),
        ("sp_0", "sp_1", "tp", "dp"),
    )
    placed = (
        P("dp", SP_TP, None), P("dp", None), P("dp", SP, None), P(),
        P(SP_TP, None), P(SP_TP, None), P(SP_TP, None),
        P(None, "tp"), P(None, "tp"), P(None, "tp"), P(None, "tp"),
        P(), P(), P("dp", None), P(), P(), P(), P(), P("tp", None),
    )
    return jax.shard_map(
        per_device, mesh=torus, in_specs=placed, out_specs=P("dp", SP_TP, None), check_vma=False
    )
```

```python
import jax
import jax.numpy as jnp
from jax import lax
from jax.experimental import pallas as pl
from jax.experimental.pallas import tpu as pltpu
from jax.sharding import Mesh
from jax.sharding import PartitionSpec as P

HEAD = 64
STATE = 128
ROW = 64
BLOCK = 128
HALO = 16
SP = ("sp_0", "sp_1")
SP_TP = ("sp_0", "sp_1", "tp")
NZ, NX, NY = 8, 4, 4
NS = NZ * NX

NORM_FLOOR = 1e-05
GATED_FLOOR = 1e-06
MESH = pl.DeviceIdType.MESH
F32 = jnp.float32
BF16 = jnp.bfloat16
HIGHEST = lax.Precision.HIGHEST
VMEM = pl.BlockSpec(memory_space=pltpu.VMEM)
ANY = pl.BlockSpec(memory_space=pl.ANY)


def silu(v):
    return v / (1.0 + jnp.exp(-v))


def remote(src, dst, send, recv, **where):
    return pltpu.make_async_remote_copy(
        src_ref=src, dst_ref=dst, send_sem=send, recv_sem=recv, device_id=where, device_id_type=MESH
    )


def position():
    return lax.axis_index("sp_0"), lax.axis_index("sp_1"), lax.axis_index("tp")


def lanes(start, size):
    return pl.ds(pl.multiple_of(start, 128), size)


def rows(start, size):
    return pl.ds(pl.multiple_of(start, 16), size)


def normed_rows(block):
    values = block.astype(F32)
    center = jnp.mean(values, -1, keepdims=True)
    off = values - center
    spread = jnp.mean(off * off, -1, keepdims=True)
    return off * lax.rsqrt(spread + NORM_FLOOR)


def conv_rows(pre, taps, run):
    length = pre.shape[0]
    at = lax.rem(lax.broadcasted_iota(jnp.int32, pre.shape, 0), run)
    total = pre * taps[2:3]
    for k in (0, 1, 3, 4):
        moved = pltpu.roll(pre, (2 - k) % length, 0)
        inside = (at + (k - 2) >= 0) & (at + (k - 2) < run)
        total = total + jnp.where(inside, moved, 0.0) * taps[k : k + 1]
    return silu(total)


def expand(v, spread):
    high = v.astype(BF16)
    low = (v - high.astype(F32)).astype(BF16)
    return jnp.dot(
        jnp.concatenate([high, low], axis=1), spread, preferred_element_type=F32
    )


def three_parts(v):
    high = v.astype(BF16)
    rest = v - high.astype(F32)
    mid = rest.astype(BF16)
    return high, mid, (rest - mid.astype(F32)).astype(BF16)


def softplus(v):
    return jnp.maximum(v, 0.0) + jnp.log1p(jnp.exp(-jnp.abs(v)))


def spread_matrix(spread):
    shape = spread.shape
    row = lax.rem(lax.broadcasted_iota(jnp.int32, shape, 0), 128)
    col = lax.broadcasted_iota(jnp.int32, shape, 1)
    spread[...] = jnp.where(row == col // HEAD, 1.0, 0.0).astype(BF16)


def dot_on(a, b, ca, cb):
    return lax.dot_general(a, b, (((ca,), (cb,)), ((), ())), preferred_element_type=F32)


def mixer_kernel(
    lat_h, ctx_h, cond_h, ccond_h, shift_h, scale_h, gatem_h,
    wv_h, wg_h, ww_h, wr_h, ws_h, rate_h, pace_h, tv_h, tw_h, tr_h, gain_h, wo_h,
    out,
    cond, ccond, shift_m, scale_m, gate_m,
    w_first, w_second, w_step, rates, pace, t_value, t_write, t_read, gain, w_out,
    part, zbuf, qbuf, xybuf, fbuf, mod,
    gpart, gz, gq, gxy, gf, gmod,
    gat, ctx_ext, nrm, hid, pre_a, pre_b, val, wri, reads, gates, local,
    cum, stp, cdec, pcol, grown_c, spread, inc, before, etot, tot,
    ends_s, ends_c, tot_b, got_s, got_c, gtot, grow_s, grow_c, sent, start,
    inner, far, near_r, near_l, mine, got_far, got_r, got_l,
    in_sem, z_send, z_recv, xy_send, xy_recv, g_send, g_recv,
    gz_send, gz_recv, gxy_send, gxy_recv, gg_send, gg_recv,
    l_send, l_recv, f_send, f_recv, h_send, h_recv,
    s_send, s_recv, t_send, t_recv, c_send, c_recv, b_send, b_recv,
    s1, r1, s2, r2,
):
    z, x, y = position()
    s = z * NX + x
    rank = s * NY + y
    right, left = lax.rem(y + 1, NY), lax.rem(y + NY - 1, NY)
    opposite = lax.rem(y + 2, NY)
    heads = 8

    def at(t):
        return {"sp_0": t // NX, "sp_1": lax.rem(t, NX)}

    def at_xy(q, sign):
        return {
            "sp_1": lax.rem(x + NX + sign * (q // NY), NX),
            "tp": lax.rem(y + NY + sign * lax.rem(q, NY), NY),
        }

    own_rows = gat.at[rows(y * 128, 128)]
    pairs = [
        (cond_h, cond), (ccond_h, ccond), (shift_h, shift_m), (scale_h, scale_m),
        (gatem_h, gate_m), (lat_h, own_rows), (ctx_h, ctx_ext.at[pl.ds(HALO, 2 * HALO)]),
        (ws_h, w_step), (rate_h, rates), (pace_h, pace),
        (wv_h, w_first.at[:, pl.ds(0, 512)]), (ww_h, w_first.at[:, pl.ds(512, 256)]),
        (tv_h, t_value), (tw_h, t_write), (wr_h, w_second.at[:, pl.ds(0, 256)]),
        (wg_h, w_second.at[:, pl.ds(256, 512)]), (tr_h, t_read),
        (gain_h, gain), (wo_h, w_out),
    ]
    fetch = [pltpu.make_async_copy(a, b, in_sem.at[k]) for k, (a, b) in enumerate(pairs)]
    for copy in fetch[:7]:
        copy.start()

    xts = [x] + [lax.rem(x + dx, NX) for dx in range(1, NX)]

    def each_other(start):
        def line(k, none):
            zt = lax.rem(z + NZ // 2 + ((k + 1) // 2) * (1 - 2 * lax.rem(k, 2)), NZ)
            for xt in (xts[2], xts[1], xts[3], xts[0]):
                start(zt, xt)
            return none

        lax.fori_loop(0, NZ - 1, line, 0)
        for xt in (xts[2], xts[1], xts[3]):
            start(z, xt)

    barrier = pltpu.get_barrier_semaphore()
    each_other(
        lambda zt, xt: pl.semaphore_signal(
            barrier, inc=1, device_id={"sp_0": zt, "sp_1": xt}, device_id_type=MESH
        )
    )
    for dy in (2, 1, 3):
        for xt in xts:
            pl.semaphore_signal(
                barrier, inc=1, device_id={"sp_1": xt, "tp": lax.rem(y + dy, NY)},
                device_id_type=MESH,
            )

    for copy in fetch[:5]:
        copy.wait()
    vec_row, vec_off = rank // 8, lax.rem(rank, 8) * 16
    lane = lax.broadcasted_iota(jnp.int32, (8, 128), 1)
    line = lax.broadcasted_iota(jnp.int32, (8, 128), 0)
    window = (lane >= vec_off) & (lane < vec_off + 16)
    both = jnp.where(
        line == 0,
        jnp.broadcast_to(cond[pl.ds(vec_row, 1), :], (8, 128)),
        jnp.broadcast_to(ccond[pl.ds(vec_row, 1), :], (8, 128)),
    )
    acts = jnp.where(window, silu(both), 0.0).astype(BF16)

    def product_of(matrix):
        tall = jnp.concatenate([matrix[...]] * 8, axis=0)
        return jnp.dot(acts, tall, preferred_element_type=F32)

    part[0:2, :] = product_of(shift_m)[0:2]
    part[2:4, :] = product_of(scale_m)[0:2]
    gpart[...] = product_of(gate_m)[0:1]
    def norm_at(base, count):
        for k in range(count // 64):
            rs = rows(base + k * 64, 64)
            nrm[rs, :] = normed_rows(gat[rs, :])

    def norm_ctx(base):
        nrm[pl.ds(512 + base, HALO), :] = normed_rows(ctx_ext[pl.ds(base, HALO), :])

    pl.semaphore_wait(barrier, NS - 1 + NX * (NY - 1))

    nxt, prv = lax.rem(s + 1, NS), lax.rem(s + NS - 1, NS)

    def got_all(ref, recv):
        remote(ref, ref, recv, recv, **at(nxt)).wait_recv()

    def sent_all(ref, send):
        remote(ref, ref, send, send, **at(nxt)).wait_send()

    def scatter_z(whole, buf, send, recv):
        for d in (4, 3, 5, 2, 6, 1, 7):
            to = lax.rem(z + d, NZ)
            remote(
                whole.at[:, lanes(to * 256, 256)], buf.at[d - 1], send.at[0], recv.at[0], sp_0=to
            ).start()

    def sum_z(whole, buf, recv, piece):
        got_all(buf, recv.at[0])
        total = whole[:, lanes(z * 256, 256)]
        for d in range(1, NZ):
            total = total + buf[d - 1]
        piece[...] = total

    def send_xy(piece, buf, send, recv):
        def one(k, none):
            q = NX * NY - 1 - k
            remote(piece, buf.at[q], send.at[0], recv.at[0], **at_xy(q, 1)).start()
            return none

        lax.fori_loop(0, NX * NY - 1, one, 0)

    def sum_xy(piece, buf, recv, last):
        got_all(buf.at[pl.ds(1, NX * NY - 1)], recv.at[0])
        total = piece[...]
        for q in range(1, NX * NY):
            total = total + buf[q]
        last[...] = total

    def gather_z(last, whole, send, recv):
        for d in (4, 3, 5, 2, 6, 1, 7):
            remote(
                last, whole.at[:, lanes(z * 256, 256)], send.at[0], recv.at[0],
                sp_0=lax.rem(z + d, NZ),
            ).start()
        whole[:, lanes(z * 256, 256)] = last[...]

    scatter_z(part, zbuf, z_send, z_recv)

    def latent_piece(side, first_row, count, k):
        piece = gat.at[rows(y * 128 + first_row, count)]
        return remote(
            piece, piece, l_send.at[k], l_recv.at[k], tp=right if side == 0 else left
        )

    def latent_ahead(side):
        owner = left if side == 0 else right
        piece = gat.at[rows(owner * 128 + side * 64, 64)]
        return remote(
            piece, piece, f_send.at[side], f_recv.at[side], tp=right if side == 0 else left
        )

    l_first = [latent_piece(0, 0, 64, 0), latent_piece(1, 64, 64, 1)]
    l_next = [latent_piece(0, 64, 32, 2), latent_piece(1, 0, 32, 3)]
    l_last = [latent_piece(0, 96, 32, 4), latent_piece(1, 32, 32, 5)]
    ahead, back = latent_ahead(0), latent_ahead(1)

    def start_all(copies):
        for copy in copies:
            copy.start()

    def start_ahead():
        l_first[0].wait_recv()
        ahead.start()
        l_first[1].wait_recv()
        back.start()

    early = lax.axis_index("dp") == 1
    late = lax.axis_index("dp") == 0
    fetch[5].wait()
    fetch[6].wait()
    pl.when(early)(lambda: start_all(l_first + l_next))
    halo_next = remote(
        ctx_ext.at[pl.ds(2 * HALO, HALO)], ctx_ext.at[pl.ds(0, HALO)],
        h_send.at[0], h_recv.at[0], **at(nxt),
    )
    halo_prev = remote(
        ctx_ext.at[pl.ds(HALO, HALO)], ctx_ext.at[pl.ds(3 * HALO, HALO)],
        h_send.at[1], h_recv.at[1], **at(prv),
    )
    halo_next.start()
    halo_prev.start()

    scatter_z(gpart, gz, gz_send, gz_recv)
    for copy in fetch[7:]:
        copy.start()
    norm_at(y * 128, 128)
    norm_ctx(HALO)
    norm_ctx(2 * HALO)
    spread_matrix(spread)
    row64 = lax.broadcasted_iota(jnp.int32, (64, 128), 0)
    col64 = lax.broadcasted_iota(jnp.int32, (64, 128), 1)
    wanted = jnp.where(col64 < heads, y * heads + col64, 32 + y * heads + col64 - heads)
    pick = jnp.where((row64 == wanted) & (col64 < 2 * heads), 1.0, 0.0)
    row = lax.broadcasted_iota(jnp.int32, (BLOCK, BLOCK), 0)
    col = lax.broadcasted_iota(jnp.int32, (BLOCK, BLOCK), 1)
    lower = jnp.where(col <= row, 1.0, 0.0).astype(BF16)
    upper = jnp.where(col >= row, 1.0, 0.0).astype(BF16)
    forward_lane = col < heads
    fl = forward_lane[0:1]
    for copy in fetch[7:10]:
        copy.wait()
    w_first[:, 768:896] = dot_on(w_step[...], pick.astype(BF16), 0, 0).astype(BF16)
    for b in range(4):
        pace_row = pace[pl.ds(s * 4 + b, 1), :]
        pcol[b * 128 : (b + 1) * 128, :] = jnp.transpose(
            jnp.broadcast_to(pace_row, (128, 128))
        )

    sum_z(part, zbuf, z_recv, qbuf)
    send_xy(qbuf, xybuf, xy_send, xy_recv)

    @pl.when(early)
    def _():
        start_all(l_last)
        start_ahead()
        norm_at(left * 128, 64)
        norm_at(right * 128 + 64, 64)

    pl.when(late)(lambda: start_all(l_first + l_next + l_last))

    sum_xy(qbuf, xybuf, xy_recv, fbuf)
    gather_z(fbuf, mod, g_send, g_recv)

    halo_next.wait()
    halo_prev.wait()
    norm_ctx(0)
    norm_ctx(3 * HALO)
    def second_halves():
        for copy in l_next + l_last:
            copy.wait_recv()
        norm_at(left * 128 + 64, 64)
        norm_at(right * 128, 64)

    pl.when(early)(second_halves)

    @pl.when(late)
    def _():
        start_ahead()
        norm_at(left * 128, 64)
        norm_at(right * 128 + 64, 64)

    for copy in fetch[10:]:
        copy.wait()
    rate_row = (
        jnp.dot(
            jnp.broadcast_to(rates[0:1, :], (8, 32)), pick[0:32], precision=HIGHEST,
            preferred_element_type=F32,
        )
        + jnp.dot(
            jnp.broadcast_to(rates[1:2, :], (8, 32)), pick[32:64], precision=HIGHEST,
            preferred_element_type=F32,
        )
    )[0:1]
    value_taps = t_value[:, lanes(y * 512, 512)]
    write_taps = t_write[:, lanes(y * 256, 256)]
    read_taps = t_read[:, lanes(y * 256, 256)]

    got_all(zbuf, g_recv.at[0])

    def block_of(k):
        return lax.rem(y + (lax.rem(k + 1, 3) + 1) * ((k + 3) // 4), NY)

    def modulate(k, none):
        b = block_of(k)

        for i in range(2):
            rs = rows(b * 128 + i * 64, 64)
            hid[rows(64 + k * 128 + i * 64, 64), :] = (
                nrm[rs, :] * (1.0 + mod[2:3, :]) + mod[0:1, :]
            ).astype(BF16)
        return none

    def project(lo, count):
        for c in range(4):
            cs = slice(c * 256, min(c * 256 + 256, 896))
            pre_a[lo : lo + count, cs] = jnp.dot(
                hid[lo : lo + count, :], w_first[:, cs], preferred_element_type=F32
            ).astype(BF16)

    for k in range(2):
        hid[pl.ds(k * 32, 32), :] = (
            nrm[pl.ds(512 + k * 32, 32), :] * (1.0 + mod[3:4, :]) + mod[1:2, :]
        ).astype(BF16)
    modulate(0, 0)
    project(0, 192)

    line_c = lax.broadcasted_iota(jnp.int32, (4 * HALO, 1), 0)
    first = jnp.where(s == 0, HALO, 0)
    last = jnp.where(s == NS - 1, 3 * HALO, 4 * HALO)
    present = (line_c >= first) & (line_c < last)
    own_c = slice(HALO, 3 * HALO)
    cv = pre_a[0:64, 0:512].astype(F32)
    cw = pre_a[0:64, 512:768].astype(F32)
    cv = conv_rows(jnp.where(present, cv, 0.0), value_taps, 4 * HALO)[own_c].astype(BF16)
    cw = conv_rows(jnp.where(present, cw, 0.0), write_taps, 4 * HALO)[own_c].astype(BF16)
    cstep = softplus(pre_a[HALO : 3 * HALO, 768:896].astype(F32))
    cdecay = -rate_row * cstep
    r32 = lax.broadcasted_iota(jnp.int32, (2 * HALO, 2 * HALO), 0)
    c32 = lax.broadcasted_iota(jnp.int32, (2 * HALO, 2 * HALO), 1)
    cparts = jnp.concatenate(three_parts(cdecay), axis=1)

    def ctx_sum(allowed):
        got = jnp.dot(
            jnp.where(allowed, 1.0, 0.0).astype(BF16), cparts, preferred_element_type=F32
        )
        return got[:, 0:128] + got[:, 128:256] + got[:, 256:384]

    later, earlier = ctx_sum(c32 > r32), ctx_sum(c32 < r32)
    cweight = jnp.exp(jnp.where(forward_lane[0 : 2 * HALO], later, earlier)) * cstep
    cvf = cv.astype(F32)
    cscaled = (jnp.concatenate([cvf, cvf], axis=1) * expand(cweight, spread[...])).astype(BF16)
    for g in range(2):
        wg = cw[:, g * 128 : (g + 1) * 128]
        for d in range(2):
            ls = slice((d * 2 + g) * 256, (d * 2 + g + 1) * 256)
            ends_c[:, ls] = dot_on(wg, cscaled[:, ls], 0, 0).astype(BF16)

    def expand3(v):
        high = v.astype(BF16)
        rest = v - high.astype(F32)
        return jnp.dot(high, spread[0:128, :], preferred_element_type=F32) + expand(
            rest, spread[...]
        )

    ctotal = jnp.exp(jnp.sum(cdecay, axis=0, keepdims=True))

    def state_copies(states, got, a_send, a_recv):
        def outgoing(zt, xt):
            return remote(
                states.at[rows(zt * 16, 16), lanes(xt * 256, 256)],
                got.at[s], a_send.at[0], a_recv.at[0], sp_0=zt, sp_1=xt,
            )

        return outgoing

    out_c = state_copies(ends_c, got_c, c_send, c_recv)
    each_other(lambda zt, xt: out_c(zt, xt).start())
    got_c[s] = ends_c[rows(z * 16, 16), lanes(x * 256, 256)]

    def block_states(k, none):
        b = block_of(k)
        at_k = rows(k * 128, 128)
        at_a = rows(64 + k * 128, 128)
        vb = conv_rows(pre_a[at_a, 0:512].astype(F32), value_taps, ROW).astype(BF16)
        val[at_k, :] = vb
        w = conv_rows(pre_a[at_a, 512:768].astype(F32), write_taps, ROW).astype(BF16)
        wri[at_k, :] = w
        step = softplus(pre_a[at_a, 768:896].astype(F32)) * pcol[rows(b * 128, 128), :]
        decay = -rate_row * step
        parts = jnp.concatenate(three_parts(decay), axis=1)
        down = jnp.dot(lower, parts, preferred_element_type=F32)
        up = jnp.dot(upper, parts, preferred_element_type=F32)
        both = jnp.where(jnp.concatenate([forward_lane] * 3, axis=1), down, up)
        cums = both[:, 0:128] + both[:, 128:256] + both[:, 256:384]
        total = jnp.where(fl, cums[127:128], cums[0:1])
        cum[at_k, :] = cums
        stp[at_k, :] = step
        weight = jnp.exp(total - cums) * step
        vf = vb.astype(F32)
        scaled = (jnp.concatenate([vf, vf], axis=1) * expand(weight, spread[...])).astype(BF16)
        for g in range(2):
            fs = slice(g * 256, (g + 1) * 256)
            bs = slice(512 + g * 256, 512 + (g + 1) * 256)
            states = dot_on(
                w[:, g * 128 : (g + 1) * 128],
                jnp.concatenate([scaled[:, fs], scaled[:, bs]], axis=1), 0, 0,
            )
            inc[b, :, fs] = states[:, 0:256]
            inc[b, :, bs] = states[:, 256:512]
        tot[pl.ds(b, 1), :] = total
        return none

    block_states(0, 0)

    pl.when(late)(second_halves)
    modulate(1, 0)
    modulate(2, 0)
    pl.when(late)(lambda: project(192, 256))
    ahead.wait_recv()
    back.wait_recv()
    norm_at(opposite * 128, 128)
    modulate(3, 0)
    pl.when(early)(lambda: project(192, 384))
    pl.when(late)(lambda: project(448, 128))
    for k in (1, 2, 3):
        block_states(k, 0)

    t0, t1, t2, t3 = (tot[b : b + 1, :] for b in range(4))
    zero = jnp.zeros_like(t0)
    etot[...] = expand3(
        jnp.concatenate(
            [jnp.exp(t0), jnp.exp(t1), jnp.exp(t2), jnp.exp(t3), jnp.exp(t0 + t1 + t2 + t3),
             zero, zero, zero], axis=0,
        )
    )
    lane1 = lane[0:1]
    tot_b[...] = jnp.where(
        lane1 < 2 * heads, jnp.exp(t0 + t1 + t2 + t3),
        jnp.where(lane1 < 4 * heads, pltpu.roll(ctotal, 2 * heads, 1), 0.0),
    )
    tot[0:1, :] = jnp.where(fl, zero, t1 + t2 + t3)
    tot[1:2, :] = jnp.where(fl, t0, t2 + t3)
    tot[2:3, :] = jnp.where(fl, t0 + t1, t3)
    tot[3:4, :] = jnp.where(fl, t0 + t1 + t2, zero)
    each_other(
        lambda zt, xt: remote(
            tot_b, gtot.at[s], t_send.at[0], t_recv.at[0], sp_0=zt, sp_1=xt
        ).start()
    )
    gtot[s] = tot_b[...]
    out_s = state_copies(ends_s, got_s, s_send, s_recv)
    for d, order in ((0, (0, 1, 2, 3)), (1, (3, 2, 1, 0))):
        for g in range(2):
            lg = d * 2 + g
            ls = slice(lg * 256, (lg + 1) * 256)
            state = jnp.zeros((STATE, 256), F32)
            for b in order:
                before[b, :, ls] = state.astype(BF16)
                state = etot[b : b + 1, ls] * state + inc[b, :, ls]
            ends_s[:, ls] = state.astype(BF16)

            def send_line(k, none, lg=lg):
                turn = NZ // 2 + ((k + 1) // 2) * (1 - 2 * lax.rem(k, 2))
                out_s(lax.rem(z + turn, NZ), lg).start()
                return none

            lax.fori_loop(0, NZ - 1, send_line, 0)

            @pl.when(x != lg)
            def _(lg=lg):
                out_s(z, lg).start()

    got_s[s] = ends_s[rows(z * 16, 16), lanes(x * 256, 256)]

    sum_z(gpart, gz, gz_recv, gq)
    send_xy(gq, gxy, gxy_send, gxy_recv)
    def project_second(c):
        pre_b[:, c] = jnp.dot(
            hid[64:576, :], w_second[:, c], preferred_element_type=F32
        ).astype(BF16)

    project_second(slice(0, 256))

    def within(k, none):
        b = block_of(k)
        at_k = rows(k * 128, 128)
        rb = conv_rows(pre_b[at_k, 0:256].astype(F32), read_taps, ROW).astype(BF16)
        reads[at_k, :] = rb
        cums = cum[at_k, :]
        step = stp[at_k, :]
        cums_t = jnp.transpose(cums)
        step_t = jnp.transpose(step)
        cdec[at_k, :] = jnp.exp(cums + tot[pl.ds(b, 1), :])
        grown = expand(jnp.exp(cums), spread[...])
        for g in range(2):
            r = rb[:, g * 128 : (g + 1) * 128]
            affinity = dot_on(r, wri[at_k, g * 128 : (g + 1) * 128], 1, 1)
            carried = jnp.zeros((128, 256), F32)
            for d in range(2):
                ls = slice((d * 2 + g) * 256, (d * 2 + g + 1) * 256)
                carried = carried + (
                    jnp.dot(r, before[b, :, ls], preferred_element_type=F32) * grown[:, ls]
                )
            for q in range(2):
                mixes = []
                for h in (g * 4 + q * 2, g * 4 + q * 2 + 1):
                    exponent = jnp.where(
                        col <= row,
                        cums[:, h : h + 1] - cums_t[h : h + 1, :],
                        cums[:, 8 + h : 9 + h] - cums_t[8 + h : 9 + h, :],
                    )
                    sf, sb = step_t[h : h + 1, :], step_t[8 + h : 9 + h, :]
                    amount = jnp.where(col < row, sf, jnp.where(col > row, sb, sf + sb))
                    mixes.append((affinity * jnp.exp(exponent) * amount).astype(BF16))
                ls = slice((g * 2 + q) * 128, (g * 2 + q + 1) * 128)
                pair = val[at_k, ls]
                none16 = jnp.zeros_like(pair)
                tall = jnp.concatenate(
                    [jnp.where(col < HEAD, pair, none16), jnp.where(col >= HEAD, pair, none16)],
                    axis=0,
                )
                got = jnp.dot(jnp.concatenate(mixes, axis=1), tall, preferred_element_type=F32)
                local[at_k, ls] = got + carried[:, q * 128 : (q + 1) * 128]
        return none

    lax.fori_loop(0, 4, within, 0)

    turned = x // 2

    def order_of(k):
        return k + turned * (NS - 1 - 2 * k)

    got_all(gtot.at[pl.ds(0, NS - 1)], t_recv.at[0])

    def spread_own(v):
        high, mid, low = three_parts(v)
        own = lanes(x * 256, 256)
        return jnp.dot(high, spread[0:128, own], preferred_element_type=F32) + jnp.dot(
            jnp.concatenate([mid, low], axis=1), spread[:, own], preferred_element_type=F32
        )

    ranges = gtot[...].reshape(NS, 128)
    grow_s[...] = spread_own(ranges)
    grow_c[...] = spread_own(pltpu.roll(ranges, 128 - 2 * heads, 1))
    got_all(got_c.at[pl.ds(0, NS - 1)], c_recv.at[0])

    def context_scan(k, state):
        j = order_of(k)
        return grow_c[pl.ds(j, 1), :] * state + got_c[j].astype(F32)

    state = lax.fori_loop(0, NS, context_scan, jnp.zeros((16, 256), F32))
    got_all(got_s.at[pl.ds(0, NS - 1)], s_recv.at[0])

    def back_copy(j):
        return remote(
            sent.at[j], start.at[rows(z * 16, 16), lanes(x * 256, 256)],
            b_send.at[0], b_recv.at[0], **at(j),
        )

    def latent_scan(k, state):
        j = order_of(k)
        sent[j] = state.astype(BF16)

        @pl.when(j != s)
        def _():
            back_copy(j).start()

        return grow_s[pl.ds(j, 1), :] * state + got_s[j].astype(F32)

    lax.fori_loop(0, NS, latent_scan, state)
    start[rows(z * 16, 16), lanes(x * 256, 256)] = sent[s]

    def last_tables(k, none):
        at_k = rows(k * 128, 128)
        grown_c[at_k, :] = expand(cdec[at_k, :], spread[...])
        gates[at_k, :] = silu(pre_b[at_k, 256:768].astype(F32))
        return none

    sum_xy(gq, gxy, gxy_recv, gf)
    gather_z(gf, gmod, gg_send, gg_recv)
    project_second(slice(256, 512))
    project_second(slice(512, 768))
    lax.fori_loop(0, 4, last_tables, 0)

    got_all(got_s.at[pl.ds(0, NS - 1)], b_recv.at[0])

    half = w_out.shape[1] // 2

    def make_inner(slot):
        at_k = slice(slot * 128, (slot + 1) * 128)
        for g in range(2):
            r = reads[at_k, g * 128 : (g + 1) * 128]
            ch = slice(g * 256, (g + 1) * 256)
            total = local[at_k, ch]
            for d in range(2):
                ls = slice((d * 2 + g) * 256, (d * 2 + g + 1) * 256)
                total = total + jnp.dot(r, start[:, ls], preferred_element_type=F32) * (
                    grown_c[at_k, ls]
                )
            gated = total * gates[at_k, ch]
            power = jnp.mean(gated * gated, -1, keepdims=True)
            gains = jnp.concatenate(
                [gain[pl.ds(y * 4 + g * 2, 1), :], gain[pl.ds(y * 4 + g * 2 + 1, 1), :]], axis=1
            )
            inner[:, ch] = (gated * lax.rsqrt(power + GATED_FLOOR) * gains).astype(BF16)

    def product(side):
        return jnp.dot(
            inner[...], w_out[:, side * half : (side + 1) * half], preferred_element_type=F32
        ).astype(BF16)

    make_inner(3)
    far[0] = product(0)
    far_r = remote(far.at[0], got_far.at[0], s1.at[0], r1.at[0], tp=right)
    far_r.start()
    far[1] = product(1)
    far_l = remote(far.at[1], got_far.at[1], s1.at[1], r1.at[1], tp=left)
    far_l.start()
    make_inner(2)
    near_r[1] = product(1)
    raw_r = remote(near_r.at[1], got_r.at[1], s2.at[0], r2.at[0], tp=right)
    raw_r.start()
    near_r[0] = product(0)
    make_inner(1)
    near_l[0] = product(0)
    raw_l = remote(near_l.at[0], got_l.at[0], s2.at[1], r2.at[1], tp=left)
    raw_l.start()
    near_l[1] = product(1)
    far_r.wait_recv()
    near_r[0] = (near_r[0].astype(F32) + got_far[0].astype(F32)).astype(BF16)
    sum_r = remote(near_r.at[0], got_r.at[0], s2.at[2], r2.at[2], tp=right)
    sum_r.start()
    far_l.wait_recv()
    near_l[1] = (near_l[1].astype(F32) + got_far[1].astype(F32)).astype(BF16)
    sum_l = remote(near_l.at[1], got_l.at[1], s2.at[3], r2.at[3], tp=left)
    sum_l.start()
    make_inner(0)
    mine[0] = product(0)
    mine[1] = product(1)

    got_all(gz, gg_recv.at[0])
    sent_all(zbuf, z_send.at[0])
    sent_all(xybuf.at[pl.ds(1, NX * NY - 1)], xy_send.at[0])
    sent_all(zbuf, g_send.at[0])
    sent_all(gz, gz_send.at[0])
    sent_all(gxy.at[pl.ds(1, NX * NY - 1)], gxy_send.at[0])
    sent_all(gz, gg_send.at[0])
    sent_all(gtot.at[pl.ds(0, NS - 1)], t_send.at[0])
    for sem in (c_send, s_send, b_send):
        sent_all(got_s.at[pl.ds(0, NS - 1)], sem.at[0])
    for copy in l_first + l_next + l_last:
        copy.wait_send()
    ahead.wait_send()
    back.wait_send()

    def close(side):
        cs = slice(side * half, (side + 1) * half)
        mixed = (
            mine[side].astype(F32) + got_r[side].astype(F32) + got_l[side].astype(F32)
        ).astype(BF16)
        own = gat[rows(y * 128, 128), cs]
        out[:, cs] = (own.astype(F32) + gmod[:, cs] * mixed.astype(F32)).astype(BF16)

    raw_r.wait_recv()
    raw_l.wait_recv()
    sum_r.wait_recv()
    sum_l.wait_recv()
    close(0)
    close(1)
    for copy in (far_r, far_l, raw_r, raw_l, sum_r, sum_l):
        copy.wait_send()


def mixer_call(*args):
    width = args[0].shape[1]
    tokens = NY * 128
    dma = pltpu.SemaphoreType.DMA
    vm = pltpu.VMEM
    same = [vm(args[k].shape, args[k].dtype) for k in range(19)]
    copied = same[2:7] + [vm((width, 896), BF16), vm((width, 768), BF16)] + same[11:19]
    piece = vm((2, 128, width // 2), BF16)
    return pl.pallas_call(
        mixer_kernel,
        out_shape=pltpu.VMEM((128, width), BF16),
        in_specs=[ANY] * 19,
        out_specs=VMEM,
        scratch_shapes=copied
        + [
            vm((4, width), F32), vm((NZ - 1, 4, 256), F32), vm((4, 256), F32),
            vm((NX * NY, 4, 256), F32), vm((4, 256), F32), vm((4, width), F32),
            vm((1, width), F32), vm((NZ - 1, 1, 256), F32), vm((1, 256), F32),
            vm((NX * NY, 1, 256), F32), vm((1, 256), F32), vm((1, width), F32),
            vm((tokens, width), BF16), vm((4 * HALO, width), BF16),
            vm((tokens + 4 * HALO, width), F32), vm((tokens + 4 * HALO, width), BF16),
            vm((tokens + 4 * HALO, 896), BF16), vm((tokens, 768), BF16),
            vm((tokens, 512), BF16), vm((tokens, 256), BF16), vm((tokens, 256), BF16),
            vm((tokens, 512), F32), vm((tokens, 512), F32),
            vm((tokens, 128), F32), vm((tokens, 128), F32), vm((tokens, 128), F32),
            vm((tokens, 128), F32), vm((tokens, 1024), F32),
            vm((256, 1024), BF16), vm((4, STATE, 1024), F32), vm((4, STATE, 1024), BF16),
            vm((8, 1024), F32), vm((8, 128), F32),
            vm((STATE, 1024), BF16), vm((STATE, 1024), BF16), vm((1, 128), F32),
            vm((NS, 16, 256), BF16), vm((NS, 16, 256), BF16), vm((NS, 1, 128), F32),
            vm((NS, 256), F32), vm((NS, 256), F32),
            vm((NS, 16, 256), BF16), vm((STATE, 1024), BF16),
            vm((128, 512), BF16), piece, piece, piece, piece, piece, piece, piece,
            dma((19,)),
        ]
        + [dma((1,))] * 12
        + [dma((6,))] * 2 + [dma((2,))] * 2 + [dma((2,))] * 2
        + [dma((1,))] * 8
        + [dma((2,)), dma((2,)), dma((4,)), dma((4,))],
        compiler_params=pltpu.CompilerParams(
            collective_id=0, has_side_effects=True, vmem_limit_bytes=56 << 20
        ),
        name="mixer",
    )(*args)


def per_device(
    latent, condition, context, context_cond, shift_matrix, scale_matrix, gate_matrix,
    value_proj, gate_proj, write_proj, read_proj, step_proj, decay_rate, pacing,
    value_taps, write_taps, read_taps, norm_gain, out_proj,
):
    width = latent.shape[2]
    updated = mixer_call(
        latent[0], context[0], condition.reshape(width // 128, 128),
        context_cond.reshape(width // 128, 128), shift_matrix, scale_matrix, gate_matrix,
        value_proj, gate_proj, write_proj, read_proj,
        step_proj.transpose(1, 2, 0).reshape(64, width), decay_rate, pacing.reshape(128, 128),
        value_taps, write_taps, read_taps, norm_gain.reshape(-1, 128), out_proj,
    )
    return updated[None]


def solution(mesh):
    torus = Mesh(
        mesh.devices.reshape(NZ, NX, mesh.shape["tp"], mesh.shape["dp"]),
        ("sp_0", "sp_1", "tp", "dp"),
    )
    placed = (
        P("dp", SP_TP, None), P("dp", None), P("dp", SP, None), P(),
        P(SP_TP, None), P(SP_TP, None), P(SP_TP, None),
        P(None, "tp"), P(None, "tp"), P(None, "tp"), P(None, "tp"),
        P(), P(), P("dp", None), P(), P(), P(), P(), P("tp", None),
    )
    return jax.shard_map(
        per_device, mesh=torus, in_specs=placed, out_specs=P("dp", SP_TP, None), check_vma=False
    )
```

```python
import jax
import jax.numpy as jnp
from jax import lax
from jax.experimental import pallas as pl
from jax.experimental.pallas import tpu as pltpu
from jax.sharding import Mesh
from jax.sharding import PartitionSpec as P

HEAD = 64
STATE = 128
ROW = 64
BLOCK = 128
HALO = 16
SP = ("sp_0", "sp_1")
SP_TP = ("sp_0", "sp_1", "tp")
NZ, NX, NY = 8, 4, 4
NS = NZ * NX

NORM_FLOOR = 1e-05
GATED_FLOOR = 1e-06
MESH = pl.DeviceIdType.MESH
F32 = jnp.float32
BF16 = jnp.bfloat16
HIGHEST = lax.Precision.HIGHEST
VMEM = pl.BlockSpec(memory_space=pltpu.VMEM)
ANY = pl.BlockSpec(memory_space=pl.ANY)


def silu(v):
    return v / (1.0 + jnp.exp(-v))


def remote(src, dst, send, recv, **where):
    return pltpu.make_async_remote_copy(
        src_ref=src, dst_ref=dst, send_sem=send, recv_sem=recv, device_id=where, device_id_type=MESH
    )


def position():
    return lax.axis_index("sp_0"), lax.axis_index("sp_1"), lax.axis_index("tp")


def lanes(start, size):
    return pl.ds(pl.multiple_of(start, 128), size)


def rows(start, size):
    return pl.ds(pl.multiple_of(start, 16), size)


def normed_rows(block):
    values = block.astype(F32)
    center = jnp.mean(values, -1, keepdims=True)
    off = values - center
    spread = jnp.mean(off * off, -1, keepdims=True)
    return off * lax.rsqrt(spread + NORM_FLOOR)


def conv_rows(pre, taps, run):
    length = pre.shape[0]
    at = lax.rem(lax.broadcasted_iota(jnp.int32, pre.shape, 0), run)
    total = pre * taps[2:3]
    for k in (0, 1, 3, 4):
        moved = pltpu.roll(pre, (2 - k) % length, 0)
        inside = (at + (k - 2) >= 0) & (at + (k - 2) < run)
        total = total + jnp.where(inside, moved, 0.0) * taps[k : k + 1]
    return silu(total)


def expand(v, spread):
    high = v.astype(BF16)
    low = (v - high.astype(F32)).astype(BF16)
    return jnp.dot(
        jnp.concatenate([high, low], axis=1), spread, preferred_element_type=F32
    )


def three_parts(v):
    high = v.astype(BF16)
    rest = v - high.astype(F32)
    mid = rest.astype(BF16)
    return high, mid, (rest - mid.astype(F32)).astype(BF16)


def softplus(v):
    return jnp.maximum(v, 0.0) + jnp.log1p(jnp.exp(-jnp.abs(v)))


def spread_matrix(spread):
    shape = spread.shape
    row = lax.rem(lax.broadcasted_iota(jnp.int32, shape, 0), 128)
    col = lax.broadcasted_iota(jnp.int32, shape, 1)
    head = lax.rem(col // 256, 2) * 8 + (col // 512) * 4 + lax.rem(col, 256) // HEAD
    spread[...] = jnp.where(row == head, 1.0, 0.0).astype(BF16)


def both_ways(v):
    return jnp.concatenate([v[:, 0:256], v[:, 0:256], v[:, 256:512], v[:, 256:512]], axis=1)


def dot_on(a, b, ca, cb):
    return lax.dot_general(a, b, (((ca,), (cb,)), ((), ())), preferred_element_type=F32)


def mixer_kernel(
    lat_h, ctx_h, cond_h, ccond_h, shift_h, scale_h, gatem_h,
    wv_h, wg_h, ww_h, wr_h, ws_h, rate_h, pace_h, tv_h, tw_h, tr_h, gain_h, wo_h,
    out,
    cond, ccond, shift_m, scale_m, gate_m,
    w_first, w_second, w_step, rates, pace, t_value, t_write, t_read, gain, w_out,
    part, zbuf, qbuf, xybuf, fbuf, mod,
    gpart, gz, gq, gxy, gf, gmod,
    gat, ctx_ext, nrm, hid, pre_a, pre_b, val, wri, reads, gates, local,
    cum, stp, cdec, pcol, grown_c, spread, inc, before, etot, tot,
    ends_s, ends_c, tot_b, got_s, got_c, gtot, grow_s, grow_c, sent, start,
    inner, far, near_r, near_l, mine, got_far, got_r, got_l,
    in_sem, z_send, z_recv, xy_send, xy_recv, g_send, g_recv,
    gz_send, gz_recv, gxy_send, gxy_recv, gg_send, gg_recv,
    l_send, l_recv, f_send, f_recv, h_send, h_recv,
    s_send, s_recv, t_send, t_recv, c_send, c_recv, b_send, b_recv,
    s1, r1, s2, r2,
):
    z, x, y = position()
    s = z * NX + x
    rank = s * NY + y
    right, left = lax.rem(y + 1, NY), lax.rem(y + NY - 1, NY)
    opposite = lax.rem(y + 2, NY)
    heads = 8

    def at(t):
        return {"sp_0": t // NX, "sp_1": lax.rem(t, NX)}

    def at_xy(q, sign):
        return {
            "sp_1": lax.rem(x + NX + sign * (q // NY), NX),
            "tp": lax.rem(y + NY + sign * lax.rem(q, NY), NY),
        }

    own_rows = gat.at[rows(y * 128, 128)]
    pairs = [
        (cond_h, cond), (ccond_h, ccond), (shift_h, shift_m), (scale_h, scale_m),
        (gatem_h, gate_m), (lat_h, own_rows), (ctx_h, ctx_ext.at[pl.ds(HALO, 2 * HALO)]),
        (ws_h, w_step), (rate_h, rates), (pace_h, pace),
        (wv_h, w_first.at[:, pl.ds(0, 512)]), (ww_h, w_first.at[:, pl.ds(512, 256)]),
        (tv_h, t_value), (tw_h, t_write), (wr_h, w_second.at[:, pl.ds(0, 256)]),
        (wg_h, w_second.at[:, pl.ds(256, 512)]), (tr_h, t_read),
        (gain_h, gain), (wo_h, w_out),
    ]
    fetch = [pltpu.make_async_copy(a, b, in_sem.at[k]) for k, (a, b) in enumerate(pairs)]
    for copy in fetch[:7]:
        copy.start()

    xts = [x] + [lax.rem(x + dx, NX) for dx in range(1, NX)]

    def each_other(start):
        def line(k, none):
            zt = lax.rem(z + NZ // 2 + ((k + 1) // 2) * (1 - 2 * lax.rem(k, 2)), NZ)
            for xt in (xts[2], xts[1], xts[3], xts[0]):
                start(zt, xt)
            return none

        lax.fori_loop(0, NZ - 1, line, 0)
        for xt in (xts[2], xts[1], xts[3]):
            start(z, xt)

    barrier = pltpu.get_barrier_semaphore()
    nxt, prv = lax.rem(s + 1, NS), lax.rem(s + NS - 1, NS)

    def greet(**where):
        pl.semaphore_signal(barrier, inc=1, device_id=where, device_id_type=MESH)

    for d in (4, 3, 5, 2, 6, 1, 7):
        greet(sp_0=lax.rem(z + d, NZ))
    for dy in (2, 1, 3):
        for xt in xts:
            greet(sp_1=xt, tp=lax.rem(y + dy, NY))
    for xt in xts[1:]:
        greet(sp_1=xt)
    greet(**at(nxt))
    greet(**at(prv))

    for copy in fetch[:5]:
        copy.wait()
    vec_row, vec_off = rank // 8, lax.rem(rank, 8) * 16
    lane = lax.broadcasted_iota(jnp.int32, (8, 128), 1)
    line = lax.broadcasted_iota(jnp.int32, (8, 128), 0)
    window = (lane >= vec_off) & (lane < vec_off + 16)
    both = jnp.where(
        line == 0,
        jnp.broadcast_to(cond[pl.ds(vec_row, 1), :], (8, 128)),
        jnp.broadcast_to(ccond[pl.ds(vec_row, 1), :], (8, 128)),
    )
    acts = jnp.where(window, silu(both), 0.0).astype(BF16)

    def product_of(matrix):
        tall = jnp.concatenate([matrix[...]] * 8, axis=0)
        return jnp.dot(acts, tall, preferred_element_type=F32)

    part[0:2, :] = product_of(shift_m)[0:2]
    part[2:4, :] = product_of(scale_m)[0:2]
    gpart[...] = product_of(gate_m)[0:1]
    def norm_at(base, count):
        for k in range(count // 64):
            rs = rows(base + k * 64, 64)
            nrm[rs, :] = normed_rows(gat[rs, :])

    def norm_ctx(base):
        nrm[pl.ds(512 + base, HALO), :] = normed_rows(ctx_ext[pl.ds(base, HALO), :])

    pl.semaphore_wait(barrier, NZ - 1 + NX * NY - 1 + 2)

    def got_all(ref, recv):
        remote(ref, ref, recv, recv, **at(nxt)).wait_recv()

    def sent_all(ref, send):
        remote(ref, ref, send, send, **at(nxt)).wait_send()

    def scatter_z(whole, buf, send, recv):
        for d in (4, 3, 5, 2, 6, 1, 7):
            to = lax.rem(z + d, NZ)
            remote(
                whole.at[:, lanes(to * 256, 256)], buf.at[d - 1], send.at[0], recv.at[0], sp_0=to
            ).start()

    def sum_z(whole, buf, recv, piece):
        got_all(buf, recv.at[0])
        total = whole[:, lanes(z * 256, 256)]
        for d in range(1, NZ):
            total = total + buf[d - 1]
        piece[...] = total

    def send_xy(piece, buf, send, recv):
        def one(k, none):
            q = NX * NY - 1 - k
            remote(piece, buf.at[q], send.at[0], recv.at[0], **at_xy(q, 1)).start()
            return none

        lax.fori_loop(0, NX * NY - 1, one, 0)

    def sum_xy(piece, buf, recv, last):
        got_all(buf.at[pl.ds(1, NX * NY - 1)], recv.at[0])
        total = piece[...]
        for q in range(1, NX * NY):
            total = total + buf[q]
        last[...] = total

    def gather_z(last, whole, send, recv):
        for d in (4, 3, 5, 2, 6, 1, 7):
            remote(
                last, whole.at[:, lanes(z * 256, 256)], send.at[0], recv.at[0],
                sp_0=lax.rem(z + d, NZ),
            ).start()
        whole[:, lanes(z * 256, 256)] = last[...]

    scatter_z(part, zbuf, z_send, z_recv)

    def latent_piece(side, first_row, count, k):
        piece = gat.at[rows(y * 128 + first_row, count)]
        return remote(
            piece, piece, l_send.at[k], l_recv.at[k], tp=right if side == 0 else left
        )

    def latent_ahead(side):
        owner = left if side == 0 else right
        piece = gat.at[rows(owner * 128 + side * 64, 64)]
        return remote(
            piece, piece, f_send.at[side], f_recv.at[side], tp=right if side == 0 else left
        )

    l_first = [latent_piece(0, 0, 64, 0), latent_piece(1, 64, 64, 1)]
    l_next = [latent_piece(0, 64, 32, 2), latent_piece(1, 0, 32, 3)]
    l_last = [latent_piece(0, 96, 32, 4), latent_piece(1, 32, 32, 5)]
    ahead, back = latent_ahead(0), latent_ahead(1)

    def start_all(copies):
        for copy in copies:
            copy.start()

    def start_ahead():
        l_first[0].wait_recv()
        ahead.start()
        l_first[1].wait_recv()
        back.start()

    early = lax.axis_index("dp") == 1
    late = lax.axis_index("dp") == 0
    fetch[5].wait()
    fetch[6].wait()
    pl.when(early)(lambda: start_all(l_first + l_next))
    halo_next = remote(
        ctx_ext.at[pl.ds(2 * HALO, HALO)], ctx_ext.at[pl.ds(0, HALO)],
        h_send.at[0], h_recv.at[0], **at(nxt),
    )
    halo_prev = remote(
        ctx_ext.at[pl.ds(HALO, HALO)], ctx_ext.at[pl.ds(3 * HALO, HALO)],
        h_send.at[1], h_recv.at[1], **at(prv),
    )
    halo_next.start()
    halo_prev.start()

    scatter_z(gpart, gz, gz_send, gz_recv)
    for copy in fetch[7:]:
        copy.start()
    norm_at(y * 128, 128)
    norm_ctx(HALO)
    norm_ctx(2 * HALO)
    spread_matrix(spread)
    row64 = lax.broadcasted_iota(jnp.int32, (64, 128), 0)
    col64 = lax.broadcasted_iota(jnp.int32, (64, 128), 1)
    wanted = jnp.where(col64 < heads, y * heads + col64, 32 + y * heads + col64 - heads)
    pick = jnp.where((row64 == wanted) & (col64 < 2 * heads), 1.0, 0.0)
    row = lax.broadcasted_iota(jnp.int32, (BLOCK, BLOCK), 0)
    col = lax.broadcasted_iota(jnp.int32, (BLOCK, BLOCK), 1)
    lower = jnp.where(col <= row, 1.0, 0.0).astype(BF16)
    upper = jnp.where(col >= row, 1.0, 0.0).astype(BF16)
    forward_lane = col < heads
    fl = forward_lane[0:1]
    for copy in fetch[7:10]:
        copy.wait()
    w_first[:, 768:896] = dot_on(w_step[...], pick.astype(BF16), 0, 0).astype(BF16)
    for b in range(4):
        pace_row = pace[pl.ds(s * 4 + b, 1), :]
        pcol[b * 128 : (b + 1) * 128, :] = jnp.transpose(
            jnp.broadcast_to(pace_row, (128, 128))
        )

    sum_z(part, zbuf, z_recv, qbuf)
    send_xy(qbuf, xybuf, xy_send, xy_recv)

    @pl.when(early)
    def _():
        start_all(l_last)
        start_ahead()
        norm_at(left * 128, 64)
        norm_at(right * 128 + 64, 64)

    pl.when(late)(lambda: start_all(l_first + l_next + l_last))

    sum_xy(qbuf, xybuf, xy_recv, fbuf)
    gather_z(fbuf, mod, g_send, g_recv)

    halo_next.wait()
    halo_prev.wait()
    norm_ctx(0)
    norm_ctx(3 * HALO)
    def second_halves():
        for copy in l_next + l_last:
            copy.wait_recv()
        norm_at(left * 128 + 64, 64)
        norm_at(right * 128, 64)

    pl.when(early)(second_halves)

    @pl.when(late)
    def _():
        start_ahead()
        norm_at(left * 128, 64)
        norm_at(right * 128 + 64, 64)

    for copy in fetch[10:]:
        copy.wait()
    rate_row = (
        jnp.dot(
            jnp.broadcast_to(rates[0:1, :], (8, 32)), pick[0:32], precision=HIGHEST,
            preferred_element_type=F32,
        )
        + jnp.dot(
            jnp.broadcast_to(rates[1:2, :], (8, 32)), pick[32:64], precision=HIGHEST,
            preferred_element_type=F32,
        )
    )[0:1]
    value_taps = t_value[:, lanes(y * 512, 512)]
    write_taps = t_write[:, lanes(y * 256, 256)]
    read_taps = t_read[:, lanes(y * 256, 256)]

    got_all(zbuf, g_recv.at[0])

    def block_of(k):
        return lax.rem(y + (lax.rem(k + 1, 3) + 1) * ((k + 3) // 4), NY)

    def modulate(k, none):
        b = block_of(k)

        for i in range(2):
            rs = rows(b * 128 + i * 64, 64)
            hid[rows(64 + k * 128 + i * 64, 64), :] = (
                nrm[rs, :] * (1.0 + mod[2:3, :]) + mod[0:1, :]
            ).astype(BF16)
        return none

    def project(lo, count):
        for cs in (slice(0, 512), slice(512, 896)):
            pre_a[lo : lo + count, cs] = jnp.dot(
                hid[lo : lo + count, :], w_first[:, cs], preferred_element_type=F32
            ).astype(BF16)

    for k in range(2):
        hid[pl.ds(k * 32, 32), :] = (
            nrm[pl.ds(512 + k * 32, 32), :] * (1.0 + mod[3:4, :]) + mod[1:2, :]
        ).astype(BF16)
    modulate(0, 0)
    project(0, 192)

    line_c = lax.broadcasted_iota(jnp.int32, (4 * HALO, 1), 0)
    first = jnp.where(s == 0, HALO, 0)
    last = jnp.where(s == NS - 1, 3 * HALO, 4 * HALO)
    present = (line_c >= first) & (line_c < last)
    own_c = slice(HALO, 3 * HALO)
    cv = pre_a[0:64, 0:512].astype(F32)
    cw = pre_a[0:64, 512:768].astype(F32)
    cv = conv_rows(jnp.where(present, cv, 0.0), value_taps, 4 * HALO)[own_c].astype(BF16)
    cw = conv_rows(jnp.where(present, cw, 0.0), write_taps, 4 * HALO)[own_c].astype(BF16)
    cstep = softplus(pre_a[HALO : 3 * HALO, 768:896].astype(F32))
    cdecay = -rate_row * cstep
    r32 = lax.broadcasted_iota(jnp.int32, (2 * HALO, 2 * HALO), 0)
    c32 = lax.broadcasted_iota(jnp.int32, (2 * HALO, 2 * HALO), 1)
    cparts = jnp.concatenate(three_parts(cdecay), axis=1)

    def ctx_sum(allowed):
        got = jnp.dot(
            jnp.where(allowed, 1.0, 0.0).astype(BF16), cparts, preferred_element_type=F32
        )
        return got[:, 0:128] + got[:, 128:256] + got[:, 256:384]

    later, earlier = ctx_sum(c32 > r32), ctx_sum(c32 < r32)
    cweight = jnp.exp(jnp.where(forward_lane[0 : 2 * HALO], later, earlier)) * cstep
    cvf = cv.astype(F32)
    cscaled = (both_ways(cvf) * expand(cweight, spread[...])).astype(BF16)
    for g in range(2):
        gs = slice(g * 512, (g + 1) * 512)
        ends_c[:, gs] = dot_on(
            cw[:, g * 128 : (g + 1) * 128], cscaled[:, gs], 0, 0
        ).astype(BF16)

    def expand3(v):
        high = v.astype(BF16)
        rest = v - high.astype(F32)
        return jnp.dot(high, spread[0:128, :], preferred_element_type=F32) + expand(
            rest, spread[...]
        )

    ctotal = jnp.exp(jnp.sum(cdecay, axis=0, keepdims=True))

    def state_copies(states, got, a_send, a_recv):
        def outgoing(zt, xt):
            return remote(
                states.at[rows(zt * 16, 16), lanes(xt * 256, 256)],
                got.at[s], a_send.at[0], a_recv.at[0], sp_0=zt, sp_1=xt,
            )

        return outgoing

    out_c = state_copies(ends_c, got_c, c_send, c_recv)
    each_other(lambda zt, xt: out_c(zt, xt).start())
    got_c[s] = ends_c[rows(z * 16, 16), lanes(x * 256, 256)]

    def block_states(k, none):
        b = block_of(k)
        at_k = rows(k * 128, 128)
        at_a = rows(64 + k * 128, 128)
        vb = conv_rows(pre_a[at_a, 0:512].astype(F32), value_taps, ROW).astype(BF16)
        val[at_k, :] = vb
        w = conv_rows(pre_a[at_a, 512:768].astype(F32), write_taps, ROW).astype(BF16)
        wri[at_k, :] = w
        step = softplus(pre_a[at_a, 768:896].astype(F32)) * pcol[rows(b * 128, 128), :]
        decay = -rate_row * step
        parts = jnp.concatenate(three_parts(decay), axis=1)
        down = jnp.dot(lower, parts, preferred_element_type=F32)
        up = jnp.dot(upper, parts, preferred_element_type=F32)
        both = jnp.where(jnp.concatenate([forward_lane] * 3, axis=1), down, up)
        cums = both[:, 0:128] + both[:, 128:256] + both[:, 256:384]
        total = jnp.where(fl, cums[127:128], cums[0:1])
        cum[at_k, :] = cums
        stp[at_k, :] = step
        weight = jnp.exp(total - cums) * step
        vf = vb.astype(F32)
        scaled = (both_ways(vf) * expand(weight, spread[...])).astype(BF16)
        for g in range(2):
            gs = slice(g * 512, (g + 1) * 512)
            inc[b, :, gs] = dot_on(w[:, g * 128 : (g + 1) * 128], scaled[:, gs], 0, 0)
        tot[pl.ds(b, 1), :] = total
        return none

    block_states(0, 0)

    pl.when(late)(second_halves)
    modulate(1, 0)
    modulate(2, 0)
    pl.when(late)(lambda: project(192, 256))
    ahead.wait_recv()
    back.wait_recv()
    norm_at(opposite * 128, 128)
    modulate(3, 0)
    pl.when(early)(lambda: project(192, 384))
    pl.when(late)(lambda: project(448, 128))
    for k in (1, 2, 3):
        block_states(k, 0)

    t0, t1, t2, t3 = (tot[b : b + 1, :] for b in range(4))
    zero = jnp.zeros_like(t0)
    etot[...] = expand3(
        jnp.concatenate(
            [jnp.exp(t0), jnp.exp(t1), jnp.exp(t2), jnp.exp(t3), jnp.exp(t0 + t1 + t2 + t3),
             zero, zero, zero], axis=0,
        )
    )
    lane1 = lane[0:1]
    tot_b[...] = jnp.where(
        lane1 < 2 * heads, jnp.exp(t0 + t1 + t2 + t3),
        jnp.where(lane1 < 4 * heads, pltpu.roll(ctotal, 2 * heads, 1), 0.0),
    )
    tot[0:1, :] = jnp.where(fl, zero, t1 + t2 + t3)
    tot[1:2, :] = jnp.where(fl, t0, t2 + t3)
    tot[2:3, :] = jnp.where(fl, t0 + t1, t3)
    tot[3:4, :] = jnp.where(fl, t0 + t1 + t2, zero)
    each_other(
        lambda zt, xt: remote(
            tot_b, gtot.at[s], t_send.at[0], t_recv.at[0], sp_0=zt, sp_1=xt
        ).start()
    )
    gtot[s] = tot_b[...]
    out_s = state_copies(ends_s, got_s, s_send, s_recv)
    for g in range(2):
        for d, order in ((0, (0, 1, 2, 3)), (1, (3, 2, 1, 0))):
            lg = g * 2 + d
            ls = slice(lg * 256, (lg + 1) * 256)
            state = jnp.zeros((STATE, 256), F32)
            for b in order:
                before[b, :, ls] = state.astype(BF16)
                state = etot[b : b + 1, ls] * state + inc[b, :, ls]
            ends_s[:, ls] = state.astype(BF16)

            def send_line(k, none, lg=lg):
                turn = NZ // 2 + ((k + 1) // 2) * (1 - 2 * lax.rem(k, 2))
                out_s(lax.rem(z + turn, NZ), lg).start()
                return none

            lax.fori_loop(0, NZ - 1, send_line, 0)

            @pl.when(x != lg)
            def _(lg=lg):
                out_s(z, lg).start()

    got_s[s] = ends_s[rows(z * 16, 16), lanes(x * 256, 256)]

    sum_z(gpart, gz, gz_recv, gq)
    send_xy(gq, gxy, gxy_send, gxy_recv)
    def project_second(c):
        pre_b[:, c] = jnp.dot(
            hid[64:576, :], w_second[:, c], preferred_element_type=F32
        ).astype(BF16)

    project_second(slice(0, 256))

    def within(k, none):
        b = block_of(k)
        at_k = rows(k * 128, 128)
        rb = conv_rows(pre_b[at_k, 0:256].astype(F32), read_taps, ROW).astype(BF16)
        reads[at_k, :] = rb
        cums = cum[at_k, :]
        step = stp[at_k, :]
        cums_t = jnp.transpose(cums)
        step_t = jnp.transpose(step)
        cdec[at_k, :] = jnp.exp(cums + tot[pl.ds(b, 1), :])
        grown = expand(jnp.exp(cums), spread[...])
        for g in range(2):
            r = rb[:, g * 128 : (g + 1) * 128]
            affinity = dot_on(r, wri[at_k, g * 128 : (g + 1) * 128], 1, 1)
            gs = slice(g * 512, (g + 1) * 512)
            carried = jnp.dot(r, before[b, :, gs], preferred_element_type=F32) * grown[:, gs]
            carried = carried[:, 0:256] + carried[:, 256:512]
            for q in range(2):
                mixes = []
                for h in (g * 4 + q * 2, g * 4 + q * 2 + 1):
                    exponent = jnp.where(
                        col <= row,
                        cums[:, h : h + 1] - cums_t[h : h + 1, :],
                        cums[:, 8 + h : 9 + h] - cums_t[8 + h : 9 + h, :],
                    )
                    sf, sb = step_t[h : h + 1, :], step_t[8 + h : 9 + h, :]
                    amount = jnp.where(col < row, sf, jnp.where(col > row, sb, sf + sb))
                    mixes.append((affinity * jnp.exp(exponent) * amount).astype(BF16))
                ls = slice((g * 2 + q) * 128, (g * 2 + q + 1) * 128)
                pair = val[at_k, ls]
                none16 = jnp.zeros_like(pair)
                tall = jnp.concatenate(
                    [jnp.where(col < HEAD, pair, none16), jnp.where(col >= HEAD, pair, none16)],
                    axis=0,
                )
                got = jnp.dot(jnp.concatenate(mixes, axis=1), tall, preferred_element_type=F32)
                local[at_k, ls] = got + carried[:, q * 128 : (q + 1) * 128]
        return none

    lax.fori_loop(0, 4, within, 0)

    turned = lax.rem(x, 2)

    def order_of(k):
        return k + turned * (NS - 1 - 2 * k)

    got_all(gtot.at[pl.ds(0, NS - 1)], t_recv.at[0])

    def spread_own(v):
        high, mid, low = three_parts(v)
        own = lanes(x * 256, 256)
        return jnp.dot(high, spread[0:128, own], preferred_element_type=F32) + jnp.dot(
            jnp.concatenate([mid, low], axis=1), spread[:, own], preferred_element_type=F32
        )

    ranges = gtot[...].reshape(NS, 128)
    grow_s[...] = spread_own(ranges)
    grow_c[...] = spread_own(pltpu.roll(ranges, 128 - 2 * heads, 1))
    got_all(got_c.at[pl.ds(0, NS - 1)], c_recv.at[0])

    def context_scan(k, state):
        j = order_of(k)
        return grow_c[pl.ds(j, 1), :] * state + got_c[j].astype(F32)

    state = lax.fori_loop(0, NS, context_scan, jnp.zeros((16, 256), F32))
    got_all(got_s.at[pl.ds(0, NS - 1)], s_recv.at[0])

    def back_copy(j):
        return remote(
            sent.at[j], start.at[rows(z * 16, 16), lanes(x * 256, 256)],
            b_send.at[0], b_recv.at[0], **at(j),
        )

    def latent_scan(k, state):
        j = order_of(k)
        sent[j] = state.astype(BF16)

        @pl.when(j != s)
        def _():
            back_copy(j).start()

        return grow_s[pl.ds(j, 1), :] * state + got_s[j].astype(F32)

    lax.fori_loop(0, NS, latent_scan, state)
    start[rows(z * 16, 16), lanes(x * 256, 256)] = sent[s]

    def last_tables(k, none):
        at_k = rows(k * 128, 128)
        grown_c[at_k, :] = expand(cdec[at_k, :], spread[...])
        gates[at_k, :] = silu(pre_b[at_k, 256:768].astype(F32))
        return none

    sum_xy(gq, gxy, gxy_recv, gf)
    gather_z(gf, gmod, gg_send, gg_recv)
    project_second(slice(256, 768))
    lax.fori_loop(0, 4, last_tables, 0)

    got_all(got_s.at[pl.ds(0, NS - 1)], b_recv.at[0])

    half = w_out.shape[1] // 2

    def make_inner(slot):
        at_k = slice(slot * 128, (slot + 1) * 128)
        for g in range(2):
            r = reads[at_k, g * 128 : (g + 1) * 128]
            ch = slice(g * 256, (g + 1) * 256)
            gs = slice(g * 512, (g + 1) * 512)
            more = jnp.dot(r, start[:, gs], preferred_element_type=F32) * grown_c[at_k, gs]
            total = local[at_k, ch] + more[:, 0:256] + more[:, 256:512]
            gated = total * gates[at_k, ch]
            power = jnp.mean(gated * gated, -1, keepdims=True)
            gains = jnp.concatenate(
                [gain[pl.ds(y * 4 + g * 2, 1), :], gain[pl.ds(y * 4 + g * 2 + 1, 1), :]], axis=1
            )
            inner[:, ch] = (gated * lax.rsqrt(power + GATED_FLOOR) * gains).astype(BF16)

    def product(side):
        return jnp.dot(
            inner[...], w_out[:, side * half : (side + 1) * half], preferred_element_type=F32
        ).astype(BF16)

    make_inner(3)
    far[0] = product(0)
    far_r = remote(far.at[0], got_far.at[0], s1.at[0], r1.at[0], tp=right)
    far_r.start()
    far[1] = product(1)
    far_l = remote(far.at[1], got_far.at[1], s1.at[1], r1.at[1], tp=left)
    far_l.start()
    make_inner(2)
    near_r[1] = product(1)
    raw_r = remote(near_r.at[1], got_r.at[1], s2.at[0], r2.at[0], tp=right)
    raw_r.start()
    near_r[0] = product(0)
    make_inner(1)
    near_l[0] = product(0)
    raw_l = remote(near_l.at[0], got_l.at[0], s2.at[1], r2.at[1], tp=left)
    raw_l.start()
    near_l[1] = product(1)
    far_r.wait_recv()
    near_r[0] = (near_r[0].astype(F32) + got_far[0].astype(F32)).astype(BF16)
    sum_r = remote(near_r.at[0], got_r.at[0], s2.at[2], r2.at[2], tp=right)
    sum_r.start()
    far_l.wait_recv()
    near_l[1] = (near_l[1].astype(F32) + got_far[1].astype(F32)).astype(BF16)
    sum_l = remote(near_l.at[1], got_l.at[1], s2.at[3], r2.at[3], tp=left)
    sum_l.start()
    make_inner(0)
    mine[0] = product(0)
    mine[1] = product(1)

    got_all(gz, gg_recv.at[0])
    sent_all(zbuf, z_send.at[0])
    sent_all(xybuf.at[pl.ds(1, NX * NY - 1)], xy_send.at[0])
    sent_all(zbuf, g_send.at[0])
    sent_all(gz, gz_send.at[0])
    sent_all(gxy.at[pl.ds(1, NX * NY - 1)], gxy_send.at[0])
    sent_all(gz, gg_send.at[0])
    sent_all(gtot.at[pl.ds(0, NS - 1)], t_send.at[0])
    for sem in (c_send, s_send, b_send):
        sent_all(got_s.at[pl.ds(0, NS - 1)], sem.at[0])
    for copy in l_first + l_next + l_last:
        copy.wait_send()
    ahead.wait_send()
    back.wait_send()

    def close(side):
        cs = slice(side * half, (side + 1) * half)
        mixed = (
            mine[side].astype(F32) + got_r[side].astype(F32) + got_l[side].astype(F32)
        ).astype(BF16)
        own = gat[rows(y * 128, 128), cs]
        out[:, cs] = (own.astype(F32) + gmod[:, cs] * mixed.astype(F32)).astype(BF16)

    raw_r.wait_recv()
    raw_l.wait_recv()
    sum_r.wait_recv()
    close(0)
    sum_l.wait_recv()
    close(1)
    for copy in (far_r, far_l, raw_r, raw_l, sum_r, sum_l):
        copy.wait_send()


def mixer_call(*args):
    width = args[0].shape[1]
    tokens = NY * 128
    dma = pltpu.SemaphoreType.DMA
    vm = pltpu.VMEM
    same = [vm(args[k].shape, args[k].dtype) for k in range(19)]
    copied = same[2:7] + [vm((width, 896), BF16), vm((width, 768), BF16)] + same[11:19]
    piece = vm((2, 128, width // 2), BF16)
    return pl.pallas_call(
        mixer_kernel,
        out_shape=pltpu.VMEM((128, width), BF16),
        in_specs=[ANY] * 19,
        out_specs=VMEM,
        scratch_shapes=copied
        + [
            vm((4, width), F32), vm((NZ - 1, 4, 256), F32), vm((4, 256), F32),
            vm((NX * NY, 4, 256), F32), vm((4, 256), F32), vm((4, width), F32),
            vm((1, width), F32), vm((NZ - 1, 1, 256), F32), vm((1, 256), F32),
            vm((NX * NY, 1, 256), F32), vm((1, 256), F32), vm((1, width), F32),
            vm((tokens, width), BF16), vm((4 * HALO, width), BF16),
            vm((tokens + 4 * HALO, width), F32), vm((tokens + 4 * HALO, width), BF16),
            vm((tokens + 4 * HALO, 896), BF16), vm((tokens, 768), BF16),
            vm((tokens, 512), BF16), vm((tokens, 256), BF16), vm((tokens, 256), BF16),
            vm((tokens, 512), F32), vm((tokens, 512), F32),
            vm((tokens, 128), F32), vm((tokens, 128), F32), vm((tokens, 128), F32),
            vm((tokens, 128), F32), vm((tokens, 1024), F32),
            vm((256, 1024), BF16), vm((4, STATE, 1024), F32), vm((4, STATE, 1024), BF16),
            vm((8, 1024), F32), vm((8, 128), F32),
            vm((STATE, 1024), BF16), vm((STATE, 1024), BF16), vm((1, 128), F32),
            vm((NS, 16, 256), BF16), vm((NS, 16, 256), BF16), vm((NS, 1, 128), F32),
            vm((NS, 256), F32), vm((NS, 256), F32),
            vm((NS, 16, 256), BF16), vm((STATE, 1024), BF16),
            vm((128, 512), BF16), piece, piece, piece, piece, piece, piece, piece,
            dma((19,)),
        ]
        + [dma((1,))] * 12
        + [dma((6,))] * 2 + [dma((2,))] * 2 + [dma((2,))] * 2
        + [dma((1,))] * 8
        + [dma((2,)), dma((2,)), dma((4,)), dma((4,))],
        compiler_params=pltpu.CompilerParams(
            collective_id=0, has_side_effects=True, vmem_limit_bytes=56 << 20
        ),
        name="mixer",
    )(*args)


def per_device(
    latent, condition, context, context_cond, shift_matrix, scale_matrix, gate_matrix,
    value_proj, gate_proj, write_proj, read_proj, step_proj, decay_rate, pacing,
    value_taps, write_taps, read_taps, norm_gain, out_proj,
):
    width = latent.shape[2]
    updated = mixer_call(
        latent[0], context[0], condition.reshape(width // 128, 128),
        context_cond.reshape(width // 128, 128), shift_matrix, scale_matrix, gate_matrix,
        value_proj, gate_proj, write_proj, read_proj,
        step_proj.transpose(1, 2, 0).reshape(64, width), decay_rate, pacing.reshape(128, 128),
        value_taps, write_taps, read_taps, norm_gain.reshape(-1, 128), out_proj,
    )
    return updated[None]


def solution(mesh):
    torus = Mesh(
        mesh.devices.reshape(NZ, NX, mesh.shape["tp"], mesh.shape["dp"]),
        ("sp_0", "sp_1", "tp", "dp"),
    )
    placed = (
        P("dp", SP_TP, None), P("dp", None), P("dp", SP, None), P(),
        P(SP_TP, None), P(SP_TP, None), P(SP_TP, None),
        P(None, "tp"), P(None, "tp"), P(None, "tp"), P(None, "tp"),
        P(), P(), P("dp", None), P(), P(), P(), P(), P("tp", None),
    )
    return jax.shard_map(
        per_device, mesh=torus, in_specs=placed, out_specs=P("dp", SP_TP, None), check_vma=False
    )
```

```python
import jax
import jax.numpy as jnp
from jax import lax
from jax.experimental import pallas as pl
from jax.experimental.pallas import tpu as pltpu
from jax.sharding import Mesh
from jax.sharding import PartitionSpec as P

HEAD = 64
STATE = 128
ROW = 64
BLOCK = 128
HALO = 16
SP = ("sp_0", "sp_1")
SP_TP = ("sp_0", "sp_1", "tp")
NZ, NX, NY = 8, 4, 4
NS = NZ * NX

NORM_FLOOR = 1e-05
GATED_FLOOR = 1e-06
MESH = pl.DeviceIdType.MESH
F32 = jnp.float32
BF16 = jnp.bfloat16
HIGHEST = lax.Precision.HIGHEST
VMEM = pl.BlockSpec(memory_space=pltpu.VMEM)
ANY = pl.BlockSpec(memory_space=pl.ANY)


def silu(v):
    return v / (1.0 + jnp.exp(-v))


def remote(src, dst, send, recv, **where):
    return pltpu.make_async_remote_copy(
        src_ref=src, dst_ref=dst, send_sem=send, recv_sem=recv, device_id=where, device_id_type=MESH
    )


def position():
    return lax.axis_index("sp_0"), lax.axis_index("sp_1"), lax.axis_index("tp")


def lanes(start, size):
    return pl.ds(pl.multiple_of(start, 128), size)


def rows(start, size):
    return pl.ds(pl.multiple_of(start, 16), size)


def normed_rows(block):
    values = block.astype(F32)
    center = jnp.mean(values, -1, keepdims=True)
    off = values - center
    spread = jnp.mean(off * off, -1, keepdims=True)
    return off * lax.rsqrt(spread + NORM_FLOOR)


def conv_rows(pre, taps, run):
    length = pre.shape[0]
    at = lax.rem(lax.broadcasted_iota(jnp.int32, pre.shape, 0), run)
    total = pre * taps[2:3]
    for k in (0, 1, 3, 4):
        moved = pltpu.roll(pre, (2 - k) % length, 0)
        inside = (at + (k - 2) >= 0) & (at + (k - 2) < run)
        total = total + jnp.where(inside, moved, 0.0) * taps[k : k + 1]
    return silu(total)


def expand(v, spread):
    high = v.astype(BF16)
    low = (v - high.astype(F32)).astype(BF16)
    return jnp.dot(
        jnp.concatenate([high, low], axis=1), spread, preferred_element_type=F32
    )


def three_parts(v):
    high = v.astype(BF16)
    rest = v - high.astype(F32)
    mid = rest.astype(BF16)
    return high, mid, (rest - mid.astype(F32)).astype(BF16)


def softplus(v):
    return jnp.maximum(v, 0.0) + jnp.log1p(jnp.exp(-jnp.abs(v)))


def spread_matrix(spread):
    shape = spread.shape
    row = lax.rem(lax.broadcasted_iota(jnp.int32, shape, 0), 128)
    col = lax.broadcasted_iota(jnp.int32, shape, 1)
    head = lax.rem(col // 256, 2) * 8 + (col // 512) * 4 + lax.rem(col, 256) // HEAD
    spread[...] = jnp.where(row == head, 1.0, 0.0).astype(BF16)


def both_ways(v):
    return jnp.concatenate([v[:, 0:256], v[:, 0:256], v[:, 256:512], v[:, 256:512]], axis=1)


def dot_on(a, b, ca, cb):
    return lax.dot_general(a, b, (((ca,), (cb,)), ((), ())), preferred_element_type=F32)


def mixer_kernel(
    lat_h, ctx_h, cond_h, ccond_h, shift_h, scale_h, gatem_h,
    wv_h, wg_h, ww_h, wr_h, ws_h, rate_h, pace_h, tv_h, tw_h, tr_h, gain_h, wo_h,
    out,
    cond, ccond, shift_m, scale_m, gate_m,
    w_first, w_second, w_step, rates, pace, t_value, t_write, t_read, gain, w_out,
    part, zbuf, qbuf, xybuf, fbuf, mod,
    gpart, gz, gq, gxy, gf, gmod,
    gat, ctx_ext, nrm, hid, pre_a, pre_b, val, wri, reads, gates, local,
    cum, stp, cdec, pcol, grown_c, spread, inc, before, etot, tot,
    ends_s, ends_c, tot_b, got_s, got_c, gtot, grow_s, grow_c, sent, start,
    inner, far, near_r, near_l, mine, got_far, got_r, got_l,
    in_sem, z_send, z_recv, xy_send, xy_recv, g_send, g_recv,
    gz_send, gz_recv, gxy_send, gxy_recv, gg_send, gg_recv,
    l_send, l_recv, f_send, f_recv, h_send, h_recv,
    s_send, s_recv, t_send, t_recv, c_send, c_recv, b_send, b_recv,
    s1, r1, s2, r2,
):
    z, x, y = position()
    s = z * NX + x
    rank = s * NY + y
    right, left = lax.rem(y + 1, NY), lax.rem(y + NY - 1, NY)
    opposite = lax.rem(y + 2, NY)
    heads = 8

    def at(t):
        return {"sp_0": t // NX, "sp_1": lax.rem(t, NX)}

    def at_xy(q, sign):
        return {
            "sp_1": lax.rem(x + NX + sign * (q // NY), NX),
            "tp": lax.rem(y + NY + sign * lax.rem(q, NY), NY),
        }

    own_rows = gat.at[rows(y * 128, 128)]
    pairs = [
        (cond_h, cond), (ccond_h, ccond), (shift_h, shift_m), (scale_h, scale_m),
        (gatem_h, gate_m), (lat_h, own_rows), (ctx_h, ctx_ext.at[pl.ds(HALO, 2 * HALO)]),
        (ws_h, w_step), (rate_h, rates), (pace_h, pace),
        (wv_h, w_first.at[:, pl.ds(0, 512)]), (ww_h, w_first.at[:, pl.ds(512, 256)]),
        (tv_h, t_value), (tw_h, t_write), (wr_h, w_second.at[:, pl.ds(0, 256)]),
        (wg_h, w_second.at[:, pl.ds(256, 512)]), (tr_h, t_read),
        (gain_h, gain), (wo_h, w_out),
    ]
    fetch = [pltpu.make_async_copy(a, b, in_sem.at[k]) for k, (a, b) in enumerate(pairs)]
    for copy in fetch[:7]:
        copy.start()

    xts = [x] + [lax.rem(x + dx, NX) for dx in range(1, NX)]

    def each_other(start):
        def line(k, none):
            zt = lax.rem(z + NZ // 2 + ((k + 1) // 2) * (1 - 2 * lax.rem(k, 2)), NZ)
            for xt in (xts[2], xts[1], xts[3], xts[0]):
                start(zt, xt)
            return none

        lax.fori_loop(0, NZ - 1, line, 0)
        for xt in (xts[2], xts[1], xts[3]):
            start(z, xt)

    barrier = pltpu.get_barrier_semaphore()
    nxt, prv = lax.rem(s + 1, NS), lax.rem(s + NS - 1, NS)

    def greet(**where):
        pl.semaphore_signal(barrier, inc=1, device_id=where, device_id_type=MESH)

    for d in (4, 3, 5, 2, 6, 1, 7):
        greet(sp_0=lax.rem(z + d, NZ))
    for dy in (2, 1, 3):
        for xt in xts:
            greet(sp_1=xt, tp=lax.rem(y + dy, NY))
    for xt in xts[1:]:
        greet(sp_1=xt)
    greet(**at(nxt))
    greet(**at(prv))

    for copy in fetch[:5]:
        copy.wait()
    vec_row, vec_off = rank // 8, lax.rem(rank, 8) * 16
    lane = lax.broadcasted_iota(jnp.int32, (8, 128), 1)
    line = lax.broadcasted_iota(jnp.int32, (8, 128), 0)
    window = (lane >= vec_off) & (lane < vec_off + 16)
    both = jnp.where(
        line == 0,
        jnp.broadcast_to(cond[pl.ds(vec_row, 1), :], (8, 128)),
        jnp.broadcast_to(ccond[pl.ds(vec_row, 1), :], (8, 128)),
    )
    acts = jnp.where(window, silu(both), 0.0).astype(BF16)

    def product_of(matrix):
        tall = jnp.concatenate([matrix[...]] * 8, axis=0)
        return jnp.dot(acts, tall, preferred_element_type=F32)

    part[0:2, :] = product_of(shift_m)[0:2]
    part[2:4, :] = product_of(scale_m)[0:2]
    gpart[...] = product_of(gate_m)[0:1]
    def norm_at(base, count):
        for k in range(count // 64):
            rs = rows(base + k * 64, 64)
            nrm[rs, :] = normed_rows(gat[rs, :])

    def norm_ctx(base):
        nrm[pl.ds(512 + base, HALO), :] = normed_rows(ctx_ext[pl.ds(base, HALO), :])

    pl.semaphore_wait(barrier, NZ - 1 + NX * NY - 1 + 2)

    def got_all(ref, recv):
        remote(ref, ref, recv, recv, **at(nxt)).wait_recv()

    def sent_all(ref, send):
        remote(ref, ref, send, send, **at(nxt)).wait_send()

    def scatter_z(whole, buf, send, recv):
        for d in (4, 3, 5, 2, 6, 1, 7):
            to = lax.rem(z + d, NZ)
            remote(
                whole.at[:, lanes(to * 256, 256)], buf.at[d - 1], send.at[0], recv.at[0], sp_0=to
            ).start()

    def sum_z(whole, buf, recv, piece):
        got_all(buf, recv.at[0])
        total = whole[:, lanes(z * 256, 256)]
        for d in range(1, NZ):
            total = total + buf[d - 1]
        piece[...] = total

    def send_xy(piece, buf, send, recv):
        def one(k, none):
            q = NX * NY - 1 - k
            remote(piece, buf.at[q], send.at[0], recv.at[0], **at_xy(q, 1)).start()
            return none

        lax.fori_loop(0, NX * NY - 1, one, 0)

    def sum_xy(piece, buf, recv, last):
        got_all(buf.at[pl.ds(1, NX * NY - 1)], recv.at[0])
        total = piece[...]
        for q in range(1, NX * NY):
            total = total + buf[q]
        last[...] = total

    def gather_z(last, whole, send, recv):
        for d in (4, 3, 5, 2, 6, 1, 7):
            remote(
                last, whole.at[:, lanes(z * 256, 256)], send.at[0], recv.at[0],
                sp_0=lax.rem(z + d, NZ),
            ).start()
        whole[:, lanes(z * 256, 256)] = last[...]

    scatter_z(part, zbuf, z_send, z_recv)

    def latent_piece(side, first_row, count, k):
        piece = gat.at[rows(y * 128 + first_row, count)]
        return remote(
            piece, piece, l_send.at[k], l_recv.at[k], tp=right if side == 0 else left
        )

    def latent_ahead(side):
        owner = left if side == 0 else right
        piece = gat.at[rows(owner * 128 + side * 64, 64)]
        return remote(
            piece, piece, f_send.at[side], f_recv.at[side], tp=right if side == 0 else left
        )

    l_first = [latent_piece(0, 0, 64, 0), latent_piece(1, 64, 64, 1)]
    l_next = [latent_piece(0, 64, 32, 2), latent_piece(1, 0, 32, 3)]
    l_last = [latent_piece(0, 96, 32, 4), latent_piece(1, 32, 32, 5)]
    ahead, back = latent_ahead(0), latent_ahead(1)

    def start_all(copies):
        for copy in copies:
            copy.start()

    def start_ahead():
        l_first[0].wait_recv()
        ahead.start()
        l_first[1].wait_recv()
        back.start()

    early = lax.axis_index("dp") == 1
    late = lax.axis_index("dp") == 0
    fetch[5].wait()
    fetch[6].wait()
    pl.when(early)(lambda: start_all(l_first + l_next))
    halo_next = remote(
        ctx_ext.at[pl.ds(2 * HALO, HALO)], ctx_ext.at[pl.ds(0, HALO)],
        h_send.at[0], h_recv.at[0], **at(nxt),
    )
    halo_prev = remote(
        ctx_ext.at[pl.ds(HALO, HALO)], ctx_ext.at[pl.ds(3 * HALO, HALO)],
        h_send.at[1], h_recv.at[1], **at(prv),
    )
    halo_next.start()
    halo_prev.start()

    scatter_z(gpart, gz, gz_send, gz_recv)
    for copy in fetch[7:]:
        copy.start()
    norm_at(y * 128, 128)
    norm_ctx(HALO)
    norm_ctx(2 * HALO)
    spread_matrix(spread)
    row64 = lax.broadcasted_iota(jnp.int32, (64, 128), 0)
    col64 = lax.broadcasted_iota(jnp.int32, (64, 128), 1)
    wanted = jnp.where(col64 < heads, y * heads + col64, 32 + y * heads + col64 - heads)
    pick = jnp.where((row64 == wanted) & (col64 < 2 * heads), 1.0, 0.0)
    row = lax.broadcasted_iota(jnp.int32, (BLOCK, BLOCK), 0)
    col = lax.broadcasted_iota(jnp.int32, (BLOCK, BLOCK), 1)
    lower = jnp.where(col <= row, 1.0, 0.0).astype(BF16)
    upper = jnp.where(col >= row, 1.0, 0.0).astype(BF16)
    forward_lane = col < heads
    fl = forward_lane[0:1]
    for copy in fetch[7:10]:
        copy.wait()
    w_first[:, 768:896] = dot_on(w_step[...], pick.astype(BF16), 0, 0).astype(BF16)
    for b in range(4):
        pace_row = pace[pl.ds(s * 4 + b, 1), :]
        pcol[b * 128 : (b + 1) * 128, :] = jnp.transpose(
            jnp.broadcast_to(pace_row, (128, 128))
        )

    sum_z(part, zbuf, z_recv, qbuf)
    send_xy(qbuf, xybuf, xy_send, xy_recv)

    @pl.when(early)
    def _():
        start_all(l_last)
        start_ahead()
        norm_at(left * 128, 64)
        norm_at(right * 128 + 64, 64)

    pl.when(late)(lambda: start_all(l_first + l_next + l_last))

    sum_xy(qbuf, xybuf, xy_recv, fbuf)
    gather_z(fbuf, mod, g_send, g_recv)

    halo_next.wait()
    halo_prev.wait()
    norm_ctx(0)
    norm_ctx(3 * HALO)
    def second_halves():
        for copy in l_next + l_last:
            copy.wait_recv()
        norm_at(left * 128 + 64, 64)
        norm_at(right * 128, 64)

    pl.when(early)(second_halves)

    @pl.when(late)
    def _():
        start_ahead()
        norm_at(left * 128, 64)
        norm_at(right * 128 + 64, 64)

    for copy in fetch[10:]:
        copy.wait()
    rate_row = (
        jnp.dot(
            jnp.broadcast_to(rates[0:1, :], (8, 32)), pick[0:32], precision=HIGHEST,
            preferred_element_type=F32,
        )
        + jnp.dot(
            jnp.broadcast_to(rates[1:2, :], (8, 32)), pick[32:64], precision=HIGHEST,
            preferred_element_type=F32,
        )
    )[0:1]
    value_taps = t_value[:, lanes(y * 512, 512)]
    write_taps = t_write[:, lanes(y * 256, 256)]
    read_taps = t_read[:, lanes(y * 256, 256)]

    got_all(zbuf, g_recv.at[0])

    def block_of(k):
        return lax.rem(y + (lax.rem(k + 1, 3) + 1) * ((k + 3) // 4), NY)

    def modulate(k, none):
        b = block_of(k)

        for i in range(2):
            rs = rows(b * 128 + i * 64, 64)
            hid[rows(64 + k * 128 + i * 64, 64), :] = (
                nrm[rs, :] * (1.0 + mod[2:3, :]) + mod[0:1, :]
            ).astype(BF16)
        return none

    def project(lo, count):
        for cs in (slice(0, 512), slice(512, 896)):
            pre_a[lo : lo + count, cs] = jnp.dot(
                hid[lo : lo + count, :], w_first[:, cs], preferred_element_type=F32
            ).astype(BF16)

    for k in range(2):
        hid[pl.ds(k * 32, 32), :] = (
            nrm[pl.ds(512 + k * 32, 32), :] * (1.0 + mod[3:4, :]) + mod[1:2, :]
        ).astype(BF16)
    modulate(0, 0)
    project(0, 192)

    line_c = lax.broadcasted_iota(jnp.int32, (4 * HALO, 1), 0)
    first = jnp.where(s == 0, HALO, 0)
    last = jnp.where(s == NS - 1, 3 * HALO, 4 * HALO)
    present = (line_c >= first) & (line_c < last)
    own_c = slice(HALO, 3 * HALO)
    cv = pre_a[0:64, 0:512].astype(F32)
    cw = pre_a[0:64, 512:768].astype(F32)
    cv = conv_rows(jnp.where(present, cv, 0.0), value_taps, 4 * HALO)[own_c].astype(BF16)
    cw = conv_rows(jnp.where(present, cw, 0.0), write_taps, 4 * HALO)[own_c].astype(BF16)
    cstep = softplus(pre_a[HALO : 3 * HALO, 768:896].astype(F32))
    cdecay = -rate_row * cstep
    r32 = lax.broadcasted_iota(jnp.int32, (2 * HALO, 2 * HALO), 0)
    c32 = lax.broadcasted_iota(jnp.int32, (2 * HALO, 2 * HALO), 1)
    cparts = jnp.concatenate(three_parts(cdecay), axis=1)

    def ctx_sum(allowed):
        got = jnp.dot(
            jnp.where(allowed, 1.0, 0.0).astype(BF16), cparts, preferred_element_type=F32
        )
        return got[:, 0:128] + got[:, 128:256] + got[:, 256:384]

    later, earlier = ctx_sum(c32 > r32), ctx_sum(c32 < r32)
    cweight = jnp.exp(jnp.where(forward_lane[0 : 2 * HALO], later, earlier)) * cstep
    cvf = cv.astype(F32)
    cscaled = (both_ways(cvf) * expand(cweight, spread[...])).astype(BF16)
    for g in range(2):
        gs = slice(g * 512, (g + 1) * 512)
        ends_c[:, gs] = dot_on(
            cw[:, g * 128 : (g + 1) * 128], cscaled[:, gs], 0, 0
        ).astype(BF16)

    ctotal = jnp.exp(jnp.sum(cdecay, axis=0, keepdims=True))

    def state_copies(states, got, a_send, a_recv):
        def outgoing(zt, xt):
            return remote(
                states.at[rows(zt * 16, 16), lanes(xt * 256, 256)],
                got.at[s], a_send.at[0], a_recv.at[0], sp_0=zt, sp_1=xt,
            )

        return outgoing

    out_c = state_copies(ends_c, got_c, c_send, c_recv)
    each_other(lambda zt, xt: out_c(zt, xt).start())
    got_c[s] = ends_c[rows(z * 16, 16), lanes(x * 256, 256)]

    def block_states(k, none):
        b = block_of(k)
        at_k = rows(k * 128, 128)
        at_a = rows(64 + k * 128, 128)
        vb = conv_rows(pre_a[at_a, 0:512].astype(F32), value_taps, ROW).astype(BF16)
        val[at_k, :] = vb
        w = conv_rows(pre_a[at_a, 512:768].astype(F32), write_taps, ROW).astype(BF16)
        wri[at_k, :] = w
        step = softplus(pre_a[at_a, 768:896].astype(F32)) * pcol[rows(b * 128, 128), :]
        decay = -rate_row * step
        parts = jnp.concatenate(three_parts(decay), axis=1)
        down = jnp.dot(lower, parts, preferred_element_type=F32)
        up = jnp.dot(upper, parts, preferred_element_type=F32)
        both = jnp.where(jnp.concatenate([forward_lane] * 3, axis=1), down, up)
        cums = both[:, 0:128] + both[:, 128:256] + both[:, 256:384]
        total = jnp.where(fl, cums[127:128], cums[0:1])
        cum[at_k, :] = cums
        stp[at_k, :] = step
        weight = jnp.exp(total - cums) * step
        vf = vb.astype(F32)
        wide = expand(
            jnp.concatenate([weight, jnp.broadcast_to(jnp.exp(total), (8, 128))], axis=0),
            spread[...],
        )
        etot[pl.ds(b, 1), :] = wide[128:129]
        scaled = (both_ways(vf) * wide[0:128]).astype(BF16)
        for g in range(2):
            gs = slice(g * 512, (g + 1) * 512)
            inc[b, :, gs] = dot_on(w[:, g * 128 : (g + 1) * 128], scaled[:, gs], 0, 0)
        tot[pl.ds(b, 1), :] = total
        return none

    block_states(0, 0)

    pl.when(late)(second_halves)
    modulate(1, 0)
    modulate(2, 0)
    pl.when(late)(lambda: project(192, 256))
    ahead.wait_recv()
    back.wait_recv()
    norm_at(opposite * 128, 128)
    modulate(3, 0)
    pl.when(early)(lambda: project(192, 384))
    pl.when(late)(lambda: project(448, 128))
    for k in (1, 2, 3):
        block_states(k, 0)

    t0, t1, t2, t3 = (tot[b : b + 1, :] for b in range(4))
    zero = jnp.zeros_like(t0)
    lane1 = lane[0:1]
    tot_b[...] = jnp.where(
        lane1 < 2 * heads, jnp.exp(t0 + t1 + t2 + t3),
        jnp.where(lane1 < 4 * heads, pltpu.roll(ctotal, 2 * heads, 1), 0.0),
    )
    tot[0:1, :] = jnp.where(fl, zero, t1 + t2 + t3)
    tot[1:2, :] = jnp.where(fl, t0, t2 + t3)
    tot[2:3, :] = jnp.where(fl, t0 + t1, t3)
    tot[3:4, :] = jnp.where(fl, t0 + t1 + t2, zero)
    each_other(
        lambda zt, xt: remote(
            tot_b, gtot.at[s], t_send.at[0], t_recv.at[0], sp_0=zt, sp_1=xt
        ).start()
    )
    gtot[s] = tot_b[...]
    out_s = state_copies(ends_s, got_s, s_send, s_recv)
    for g in range(2):
        for d, order in ((0, (0, 1, 2, 3)), (1, (3, 2, 1, 0))):
            lg = g * 2 + d
            ls = slice(lg * 256, (lg + 1) * 256)
            state = jnp.zeros((STATE, 256), F32)
            for b in order:
                before[b, :, ls] = state.astype(BF16)
                state = etot[b : b + 1, ls] * state + inc[b, :, ls]
            ends_s[:, ls] = state.astype(BF16)

            def send_line(k, none, lg=lg):
                turn = NZ // 2 + ((k + 1) // 2) * (1 - 2 * lax.rem(k, 2))
                out_s(lax.rem(z + turn, NZ), lg).start()
                return none

            lax.fori_loop(0, NZ - 1, send_line, 0)

            @pl.when(x != lg)
            def _(lg=lg):
                out_s(z, lg).start()

    got_s[s] = ends_s[rows(z * 16, 16), lanes(x * 256, 256)]

    sum_z(gpart, gz, gz_recv, gq)
    send_xy(gq, gxy, gxy_send, gxy_recv)
    def project_second(c):
        pre_b[:, c] = jnp.dot(
            hid[64:576, :], w_second[:, c], preferred_element_type=F32
        ).astype(BF16)

    project_second(slice(0, 256))

    def within(k, none):
        b = block_of(k)
        at_k = rows(k * 128, 128)
        rb = conv_rows(pre_b[at_k, 0:256].astype(F32), read_taps, ROW).astype(BF16)
        reads[at_k, :] = rb
        cums = cum[at_k, :]
        step = stp[at_k, :]
        cums_t = jnp.transpose(cums)
        step_t = jnp.transpose(step)
        cdec[at_k, :] = jnp.exp(cums + tot[pl.ds(b, 1), :])
        grown = expand(jnp.exp(cums), spread[...])
        for g in range(2):
            r = rb[:, g * 128 : (g + 1) * 128]
            affinity = dot_on(r, wri[at_k, g * 128 : (g + 1) * 128], 1, 1)
            gs = slice(g * 512, (g + 1) * 512)
            carried = jnp.dot(r, before[b, :, gs], preferred_element_type=F32) * grown[:, gs]
            carried = carried[:, 0:256] + carried[:, 256:512]
            for q in range(2):
                mixes = []
                for h in (g * 4 + q * 2, g * 4 + q * 2 + 1):
                    exponent = jnp.where(
                        col <= row,
                        cums[:, h : h + 1] - cums_t[h : h + 1, :],
                        cums[:, 8 + h : 9 + h] - cums_t[8 + h : 9 + h, :],
                    )
                    sf, sb = step_t[h : h + 1, :], step_t[8 + h : 9 + h, :]
                    amount = jnp.where(col < row, sf, jnp.where(col > row, sb, sf + sb))
                    mixes.append((affinity * jnp.exp(exponent) * amount).astype(BF16))
                ls = slice((g * 2 + q) * 128, (g * 2 + q + 1) * 128)
                pair = val[at_k, ls]
                none16 = jnp.zeros_like(pair)
                tall = jnp.concatenate(
                    [jnp.where(col < HEAD, pair, none16), jnp.where(col >= HEAD, pair, none16)],
                    axis=0,
                )
                got = jnp.dot(jnp.concatenate(mixes, axis=1), tall, preferred_element_type=F32)
                local[at_k, ls] = got + carried[:, q * 128 : (q + 1) * 128]
        return none

    lax.fori_loop(0, 4, within, 0)

    turned = lax.rem(x, 2)

    def order_of(k):
        return k + turned * (NS - 1 - 2 * k)

    got_all(gtot.at[pl.ds(0, NS - 1)], t_recv.at[0])

    def spread_own(v):
        high, mid, low = three_parts(v)
        own = lanes(x * 256, 256)
        return jnp.dot(high, spread[0:128, own], preferred_element_type=F32) + jnp.dot(
            jnp.concatenate([mid, low], axis=1), spread[:, own], preferred_element_type=F32
        )

    ranges = gtot[...].reshape(NS, 128)
    grow_s[...] = spread_own(ranges)
    grow_c[...] = spread_own(pltpu.roll(ranges, 128 - 2 * heads, 1))
    got_all(got_c.at[pl.ds(0, NS - 1)], c_recv.at[0])

    def context_scan(k, state):
        j = order_of(k)
        return grow_c[pl.ds(j, 1), :] * state + got_c[j].astype(F32)

    state = lax.fori_loop(0, NS, context_scan, jnp.zeros((16, 256), F32))
    got_all(got_s.at[pl.ds(0, NS - 1)], s_recv.at[0])

    def back_copy(j):
        return remote(
            sent.at[j], start.at[rows(z * 16, 16), lanes(x * 256, 256)],
            b_send.at[0], b_recv.at[0], **at(j),
        )

    def latent_scan(k, state):
        j = order_of(k)
        sent[j] = state.astype(BF16)

        @pl.when(j != s)
        def _():
            back_copy(j).start()

        return grow_s[pl.ds(j, 1), :] * state + got_s[j].astype(F32)

    lax.fori_loop(0, NS, latent_scan, state)
    start[rows(z * 16, 16), lanes(x * 256, 256)] = sent[s]

    def last_tables(k, none):
        at_k = rows(k * 128, 128)
        grown_c[at_k, :] = expand(cdec[at_k, :], spread[...])
        gates[at_k, :] = silu(pre_b[at_k, 256:768].astype(F32))
        return none

    sum_xy(gq, gxy, gxy_recv, gf)
    gather_z(gf, gmod, gg_send, gg_recv)
    project_second(slice(256, 768))
    lax.fori_loop(0, 4, last_tables, 0)

    got_all(got_s.at[pl.ds(0, NS - 1)], b_recv.at[0])

    half = w_out.shape[1] // 2

    def make_inner(slot):
        at_k = slice(slot * 128, (slot + 1) * 128)
        for g in range(2):
            r = reads[at_k, g * 128 : (g + 1) * 128]
            ch = slice(g * 256, (g + 1) * 256)
            gs = slice(g * 512, (g + 1) * 512)
            more = jnp.dot(r, start[:, gs], preferred_element_type=F32) * grown_c[at_k, gs]
            total = local[at_k, ch] + more[:, 0:256] + more[:, 256:512]
            gated = total * gates[at_k, ch]
            power = jnp.mean(gated * gated, -1, keepdims=True)
            gains = jnp.concatenate(
                [gain[pl.ds(y * 4 + g * 2, 1), :], gain[pl.ds(y * 4 + g * 2 + 1, 1), :]], axis=1
            )
            inner[:, ch] = (gated * lax.rsqrt(power + GATED_FLOOR) * gains).astype(BF16)

    def product(side):
        return jnp.dot(
            inner[...], w_out[:, side * half : (side + 1) * half], preferred_element_type=F32
        ).astype(BF16)

    make_inner(3)
    quarter = half // 2
    far_copies = []
    for part in range(2):
        for side in range(2):
            cs = slice(part * quarter, (part + 1) * quarter)
            far[side, :, cs] = jnp.dot(
                inner[...],
                w_out[:, side * half + part * quarter : side * half + (part + 1) * quarter],
                preferred_element_type=F32,
            ).astype(BF16)
            piece = (side, slice(None), pl.ds(part * quarter, quarter))
            far_copies.append(
                remote(
                    far.at[piece], got_far.at[piece], s1.at[part * 2 + side],
                    r1.at[part * 2 + side], tp=right if side == 0 else left,
                )
            )
            far_copies[-1].start()
    make_inner(2)
    near_r[1] = product(1)
    raw_r = remote(near_r.at[1], got_r.at[1], s2.at[0], r2.at[0], tp=right)
    raw_r.start()
    near_r[0] = product(0)
    make_inner(1)
    near_l[0] = product(0)
    raw_l = remote(near_l.at[0], got_l.at[0], s2.at[1], r2.at[1], tp=left)
    raw_l.start()
    near_l[1] = product(1)
    far_copies[0].wait_recv()
    far_copies[2].wait_recv()
    near_r[0] = (near_r[0].astype(F32) + got_far[0].astype(F32)).astype(BF16)
    sum_r = remote(near_r.at[0], got_r.at[0], s2.at[2], r2.at[2], tp=right)
    sum_r.start()
    far_copies[1].wait_recv()
    far_copies[3].wait_recv()
    near_l[1] = (near_l[1].astype(F32) + got_far[1].astype(F32)).astype(BF16)
    sum_l = remote(near_l.at[1], got_l.at[1], s2.at[3], r2.at[3], tp=left)
    sum_l.start()
    make_inner(0)
    mine[0] = product(0)
    mine[1] = product(1)

    got_all(gz, gg_recv.at[0])
    sent_all(zbuf, z_send.at[0])
    sent_all(xybuf.at[pl.ds(1, NX * NY - 1)], xy_send.at[0])
    sent_all(zbuf, g_send.at[0])
    sent_all(gz, gz_send.at[0])
    sent_all(gxy.at[pl.ds(1, NX * NY - 1)], gxy_send.at[0])
    sent_all(gz, gg_send.at[0])
    sent_all(gtot.at[pl.ds(0, NS - 1)], t_send.at[0])
    for sem in (c_send, s_send, b_send):
        sent_all(got_s.at[pl.ds(0, NS - 1)], sem.at[0])
    for copy in l_first + l_next + l_last:
        copy.wait_send()
    ahead.wait_send()
    back.wait_send()

    def close(side):
        cs = slice(side * half, (side + 1) * half)
        mixed = (
            mine[side].astype(F32) + got_r[side].astype(F32) + got_l[side].astype(F32)
        ).astype(BF16)
        own = gat[rows(y * 128, 128), cs]
        out[:, cs] = (own.astype(F32) + gmod[:, cs] * mixed.astype(F32)).astype(BF16)

    raw_r.wait_recv()
    raw_l.wait_recv()
    sum_r.wait_recv()
    close(0)
    sum_l.wait_recv()
    close(1)
    for copy in (*far_copies, raw_r, raw_l, sum_r, sum_l):
        copy.wait_send()


def mixer_call(*args):
    width = args[0].shape[1]
    tokens = NY * 128
    dma = pltpu.SemaphoreType.DMA
    vm = pltpu.VMEM
    same = [vm(args[k].shape, args[k].dtype) for k in range(19)]
    copied = same[2:7] + [vm((width, 896), BF16), vm((width, 768), BF16)] + same[11:19]
    piece = vm((2, 128, width // 2), BF16)
    return pl.pallas_call(
        mixer_kernel,
        out_shape=pltpu.VMEM((128, width), BF16),
        in_specs=[ANY] * 19,
        out_specs=VMEM,
        scratch_shapes=copied
        + [
            vm((4, width), F32), vm((NZ - 1, 4, 256), F32), vm((4, 256), F32),
            vm((NX * NY, 4, 256), F32), vm((4, 256), F32), vm((4, width), F32),
            vm((1, width), F32), vm((NZ - 1, 1, 256), F32), vm((1, 256), F32),
            vm((NX * NY, 1, 256), F32), vm((1, 256), F32), vm((1, width), F32),
            vm((tokens, width), BF16), vm((4 * HALO, width), BF16),
            vm((tokens + 4 * HALO, width), F32), vm((tokens + 4 * HALO, width), BF16),
            vm((tokens + 4 * HALO, 896), BF16), vm((tokens, 768), BF16),
            vm((tokens, 512), BF16), vm((tokens, 256), BF16), vm((tokens, 256), BF16),
            vm((tokens, 512), F32), vm((tokens, 512), F32),
            vm((tokens, 128), F32), vm((tokens, 128), F32), vm((tokens, 128), F32),
            vm((tokens, 128), F32), vm((tokens, 1024), F32),
            vm((256, 1024), BF16), vm((4, STATE, 1024), F32), vm((4, STATE, 1024), BF16),
            vm((8, 1024), F32), vm((8, 128), F32),
            vm((STATE, 1024), BF16), vm((STATE, 1024), BF16), vm((1, 128), F32),
            vm((NS, 16, 256), BF16), vm((NS, 16, 256), BF16), vm((NS, 1, 128), F32),
            vm((NS, 256), F32), vm((NS, 256), F32),
            vm((NS, 16, 256), BF16), vm((STATE, 1024), BF16),
            vm((128, 512), BF16), piece, piece, piece, piece, piece, piece, piece,
            dma((19,)),
        ]
        + [dma((1,))] * 12
        + [dma((6,))] * 2 + [dma((2,))] * 2 + [dma((2,))] * 2
        + [dma((1,))] * 8
        + [dma((4,)), dma((4,)), dma((4,)), dma((4,))],
        compiler_params=pltpu.CompilerParams(
            collective_id=0, has_side_effects=True, vmem_limit_bytes=56 << 20
        ),
        name="mixer",
    )(*args)


def per_device(
    latent, condition, context, context_cond, shift_matrix, scale_matrix, gate_matrix,
    value_proj, gate_proj, write_proj, read_proj, step_proj, decay_rate, pacing,
    value_taps, write_taps, read_taps, norm_gain, out_proj,
):
    width = latent.shape[2]
    updated = mixer_call(
        latent[0], context[0], condition.reshape(width // 128, 128),
        context_cond.reshape(width // 128, 128), shift_matrix, scale_matrix, gate_matrix,
        value_proj, gate_proj, write_proj, read_proj,
        step_proj.transpose(1, 2, 0).reshape(64, width), decay_rate, pacing.reshape(128, 128),
        value_taps, write_taps, read_taps, norm_gain.reshape(-1, 128), out_proj,
    )
    return updated[None]


def solution(mesh):
    torus = Mesh(
        mesh.devices.reshape(NZ, NX, mesh.shape["tp"], mesh.shape["dp"]),
        ("sp_0", "sp_1", "tp", "dp"),
    )
    placed = (
        P("dp", SP_TP, None), P("dp", None), P("dp", SP, None), P(),
        P(SP_TP, None), P(SP_TP, None), P(SP_TP, None),
        P(None, "tp"), P(None, "tp"), P(None, "tp"), P(None, "tp"),
        P(), P(), P("dp", None), P(), P(), P(), P(), P("tp", None),
    )
    return jax.shard_map(
        per_device, mesh=torus, in_specs=placed, out_specs=P("dp", SP_TP, None), check_vma=False
    )
```
